32 devices in a mesh: dp: 4 (over y, x), kv: 4 (over z), tp: 2 (over core).
Axes of the slice: x: 2, y: 2, z: 4, core: 2. Of those that a mesh axis runs over, the one named last changes fastest.
Arguments:
- piece_tokens: bfloat16 [2048, 2048], P(('dp', 'kv')), parts along dimension 0, may hold values from -6 to 6
- step_tokens: bfloat16 [16, 2048], P(('dp', 'kv')), parts along dimension 0, may hold values from -6 to 6
- norm_gain: float32 [2048], replicated, may hold values from 0.1 to 1.9
- query_weight: bfloat16 [2048, 1024], P(None, 'tp'), may hold values from -0.125 to 0.125
- key_weight: bfloat16 [2048, 1024], P(None, 'tp'), may hold values from -0.125 to 0.125
- value_weight: bfloat16 [2048, 1024], P(None, 'tp'), may hold values from -0.125 to 0.125
- gate_weight: bfloat16 [2048, 16], replicated, may hold values from -0.125 to 0.125
- gate_bias: float32 [16], replicated, may hold values from 3 to 10.5
- out_weight: bfloat16 [1024, 2048], P(None, 'tp'), may hold values from -0.1875 to 0.1875
- cache_keys: bfloat16 [8192, 1024], P(('dp', 'kv'), 'tp'), parts along dimension 0, may hold values from -320 to 320
- cache_values: bfloat16 [8192, 1024], P(('dp', 'kv'), 'tp'), parts along dimension 0, may hold values from -10 to 10
- cache_decay: float32 [16, 8192], P('tp', ('dp', 'kv')), parts along dimension 1, may hold values from -696.32 to 0, as said below
- decay_total: float32 [64], P('dp'), parts along dimension 0, may hold values from -696.32 to 0, as said below
- step_keys: bfloat16 [16, 1024, 1024], P(('dp', 'kv'), None, 'tp'), parts along dimension 0, may hold values from -6 to 6
- step_values: bfloat16 [16, 1024, 1024], P(('dp', 'kv'), None, 'tp'), parts along dimension 0, may hold values from -6 to 6
- step_gates: float32 [16, 16, 1024], P(('dp', 'kv'), 'tp'), parts along dimension 0, may hold values from -0.34 to 0
- step_lengths: int32 [16], P(('dp', 'kv')), parts along dimension 0, may hold values from 1 to 1024, 2048 in all
Outputs:
- piece_out: bfloat16 [2048, 2048], P(('dp', 'kv'), 'tp'), parts along dimension 0
- step_out: bfloat16 [16, 2048], P(('dp', 'kv'), 'tp'), parts along dimension 0
The draws below stay inside these ranges and needn't reach their ends.
There are 4 independent parts, one for each index of `dp`. The reference program is written for one: setup_inputs(seed, part) draws one part's arguments, and reference() takes and returns one part's arrays. A program takes and returns all parts, laid end to end along the dimension named above; an argument that names none is the same for every part. Nothing has to cross between parts.
Inputs may be any that keep to these rules, and one draw needn't show every extreme that they name: `cache_decay`: cumulative values never rise along the positions and start at one gate below zero. `decay_total`: equal to the cumulative value of the last cached position. `step_lengths`: each length is 1 to 1024; the largest is exactly 1024; positions at or past a length are unused.
All inputs are finite; a program needn't handle non-finite values.
Results may differ from the reference program's by a relative error of at most 0.0095.
The reference program's roundings to bfloat16 on the way count: a program that leaves them out, or rounds other values in their place, can miss the bound.
Values may be sent and summed in bfloat16 or wider, within the bound.
A program may use at most 128 MiB of HBM per device.

```python
import math
import jax
import jax.numpy as jnp
import numpy as np
from jax import lax

D = 2048
HEADS = 16
HEAD = 64
PIECE_DEV = 128
DEC_LEN = 1024
CACHE_DEV = 512
PIECE = 512
CACHE = 2048
DEC = 4
N_KV = 4


def fast_heads(key):
    ranking = jax.random.permutation(jax.random.fold_in(key, 13), HEADS)
    fast_count = HEADS // 2
    return ranking < fast_count


def gate_values(key, leading, span, block):
    fast_mask = fast_heads(key)
    base_rate = jnp.where(fast_mask, 0.03, 5e-05).astype(jnp.float32)
    factor = 0.5 + jax.random.uniform(jax.random.fold_in(key, 12), (leading, 1, span // block), jnp.float32)
    factor = jnp.repeat(factor, block, axis=2)
    noise_key = jax.random.fold_in(key, 11)
    spread = jnp.clip(jax.random.normal(noise_key, (leading, HEADS, span), jnp.float32), -4.0, 4.0) * 0.5
    return -base_rate[None, :, None] * factor * jnp.exp(spread)


def prompt_decay(key):
    gates_drawn = gate_values(jax.random.fold_in(key, 5), 1, CACHE, CACHE_DEV)[0]
    return jnp.cumsum(gates_drawn, axis=1)


def draw_gate_bias(key, part):
    offsets = jax.random.uniform(jax.random.fold_in(key, 3), (HEADS,), jnp.float32)
    fast_mask = fast_heads(jax.random.fold_in(key, 4))
    return jnp.where(fast_mask, 3.0 + offsets, 9.5 + offsets)


def draw_cache_keys(key, part):
    base_keys = jnp.clip(jax.random.normal(jax.random.fold_in(key, 21), (CACHE, HEADS * HEAD), jnp.float32), -4.0, 4.0)
    return base_keys.astype(jnp.bfloat16)


def draw_cache_values(key, part):
    noise_key = jax.random.fold_in(key, 31)
    noise = jnp.clip(jax.random.normal(noise_key, (CACHE, HEADS * HEAD), jnp.float32), -4.0, 4.0)
    block_means = jnp.clip(jax.random.normal(jax.random.fold_in(key, 32), (CACHE // CACHE_DEV, HEADS * HEAD), jnp.float32), -4.0, 4.0) * 1.5
    return (noise + jnp.repeat(block_means, CACHE_DEV, axis=0)).astype(jnp.bfloat16)


def draw_cache_decay(key, part):
    return prompt_decay(key)


def draw_decay_total(key, part):
    return prompt_decay(key)[:, -1]


def draw_step_gates(key, part):
    return gate_values(jax.random.fold_in(key, 9), DEC, DEC_LEN, DEC_LEN)


def steps_of(rng, shape, pieces, smallest, high):
    level = 1.0
    for position, blocks in pieces:
        heights = jax.random.uniform(jax.random.fold_in(jax.random.fold_in(rng, 6), position), (blocks,), jnp.float32, smallest / len(pieces), high / len(pieces))
        level = level * jnp.repeat(jnp.exp(heights), shape[position] // blocks).reshape((-1,) + (1,) * (len(shape) - 1 - position))
    return level


def length_profile(count, total, limit, skew):
    portions = [(1 << 20) // math.isqrt(rank ** skew) + 1 for rank in range(2, count + 1)]
    spare, counts = total - limit - (count - 1), [1] * (count - 1)
    while spare > 0:
        free = [i for i in range(count - 1) if counts[i] < limit]
        pool, left = sum([portions[i] for i in free]), spare
        for i in free:
            addition = min(limit - counts[i], max(1, left * portions[i] // pool), spare)
            counts[i] = counts[i] + addition
            spare = spare - addition
    return np.array([limit] + counts)


def ragged(rng, amount, total, bound, lean):
    if amount == 2:
        one = jax.random.randint(rng, (), max(1, total - bound), min(bound, total - 1) + 1)
        return jnp.stack([one, total - one])
    sizes = jnp.asarray(length_profile(amount, total, bound, lean), jnp.int32)
    couples = (amount - 1) // 2
    donor, taker = sizes[1:1 + 2 * couples:2], sizes[2:2 + 2 * couples:2]
    room = jnp.minimum(donor - 1, bound - taker)
    shifted = jax.random.randint(jax.random.fold_in(rng, 1), (couples,), 0, 1 << 20) % (room + 1)
    sizes = sizes.at[1:1 + 2 * couples:2].set(donor - shifted).at[2:2 + 2 * couples:2].set(taker + shifted)
    return sizes[jax.random.permutation(jax.random.fold_in(rng, 2), amount)]


def normal_values(own_key, extent, deviation, limit, pieces=(), kind=jnp.bfloat16):
    gain = steps_of(own_key, extent, pieces, -0.22, 0.18) if pieces else 1.0
    drawn = jax.random.normal(own_key, extent, jnp.float32) * deviation * gain
    return jnp.minimum(jnp.maximum(drawn, -limit), limit).astype(kind)


def setup_inputs(seed: int = 0, part: int = 0) -> dict:
    arg_keys = jax.random.split(jax.random.key(seed), 18)
    part_keys = jax.random.split(jax.random.fold_in(arg_keys[17], part), 18)
    return {
        "piece_tokens": normal_values(part_keys[0], (PIECE, D), 1.0, 6.0, ((0, 4),)),
        "step_tokens": normal_values(part_keys[1], (DEC, D), 1.0, 6.0, ((0, 4),)),
        "norm_gain": jnp.clip(1.0 + 0.18 * jax.random.normal(arg_keys[2], (D,), jnp.float32), 0.1, 1.9),
        "query_weight": normal_values(arg_keys[3], (D, HEADS * HEAD), D ** -0.5, 0.125, ((1, 2),)),
        "key_weight": normal_values(arg_keys[4], (D, HEADS * HEAD), D ** -0.5, 0.125, ((1, 2),)),
        "value_weight": normal_values(arg_keys[5], (D, HEADS * HEAD), D ** -0.5, 0.125, ((1, 2),)),
        "gate_weight": normal_values(arg_keys[6], (D, HEADS), D ** -0.5, 0.125),
        "gate_bias": draw_gate_bias(jax.random.fold_in(arg_keys[17], 71), part),
        "out_weight": normal_values(arg_keys[8], (HEADS * HEAD, D), (HEADS * HEAD) ** -0.5, 0.1875, ((1, 2),)),
        "cache_keys": draw_cache_keys(jax.random.fold_in(jax.random.fold_in(arg_keys[17], part), 71), part),
        "cache_values": draw_cache_values(jax.random.fold_in(jax.random.fold_in(arg_keys[17], part), 71), part),
        "cache_decay": draw_cache_decay(jax.random.fold_in(jax.random.fold_in(arg_keys[17], part), 71), part),
        "decay_total": draw_decay_total(jax.random.fold_in(jax.random.fold_in(arg_keys[17], part), 71), part),
        "step_keys": normal_values(part_keys[13], (DEC, DEC_LEN, HEADS * HEAD), 1.0, 6.0, ((0, 4), (2, 2))),
        "step_values": normal_values(part_keys[14], (DEC, DEC_LEN, HEADS * HEAD), 1.0, 6.0, ((0, 4), (2, 2))),
        "step_gates": draw_step_gates(jax.random.fold_in(jax.random.fold_in(arg_keys[17], part), 71), part),
        "step_lengths": ragged(part_keys[16], DEC, DEC * DEC_LEN // 2, DEC_LEN, 2).astype(jnp.int32),
    }


norm_eps = 1e-06
negative = -1e+30

def normalize(token_rows, norm_gain):
    wide = token_rows.astype(jnp.float32)
    factor = lax.rsqrt(lax.optimization_barrier(jnp.mean(wide * wide, axis=-1, keepdims=True)) + norm_eps)
    return (wide * factor * norm_gain).astype(jnp.bfloat16)

def reference(piece_tokens, step_tokens, norm_gain, query_weight, key_weight, value_weight, gate_weight, gate_bias, out_weight, cache_keys, cache_values, cache_decay, decay_total, step_keys, step_values, step_gates, step_lengths):
    score_scale = HEAD ** (-0.5)
    token_rows = jnp.concatenate([piece_tokens, step_tokens], axis=0)
    normed = normalize(token_rows, norm_gain)
    queries = jnp.dot(normed, query_weight, preferred_element_type=jnp.float32).astype(jnp.bfloat16)
    new_keys = jnp.dot(normed, key_weight, preferred_element_type=jnp.float32).astype(jnp.bfloat16)
    new_values = jnp.dot(normed, value_weight, preferred_element_type=jnp.float32).astype(jnp.bfloat16)
    log_gates = jax.nn.log_sigmoid(jnp.dot(normed, gate_weight, preferred_element_type=jnp.float32) + gate_bias)
    piece_q = queries[:PIECE].reshape(PIECE, HEADS, HEAD).astype(jnp.float32)
    piece_k = new_keys[:PIECE].reshape(PIECE, HEADS, HEAD)
    piece_v = new_values[:PIECE].reshape(PIECE, HEADS, HEAD)
    piece_decay = decay_total[None, :] + jnp.cumsum(log_gates[:PIECE], axis=0)
    query_pos = jnp.arange(PIECE, dtype=jnp.int32)
    key_local = jnp.arange(PIECE_DEV, dtype=jnp.int32)

    def visit_block(carry_in, block_id):
        best_high, mass_sum, weighted = carry_in
        cache_start = (block_id * CACHE_DEV).astype(jnp.int32)
        piece_start = (block_id * PIECE_DEV).astype(jnp.int32)
        own_keys = lax.dynamic_slice_in_dim(cache_keys, cache_start, CACHE_DEV, 0).reshape(CACHE_DEV, HEADS, HEAD)
        own_values = lax.dynamic_slice_in_dim(cache_values, cache_start, CACHE_DEV, 0).reshape(CACHE_DEV, HEADS, HEAD)
        own_decay = lax.dynamic_slice_in_dim(cache_decay, cache_start, CACHE_DEV, 1)
        block_keys = lax.dynamic_slice_in_dim(piece_k, piece_start, PIECE_DEV, 0)
        block_values = lax.dynamic_slice_in_dim(piece_v, piece_start, PIECE_DEV, 0)
        block_decay = lax.dynamic_slice_in_dim(piece_decay, piece_start, PIECE_DEV, 0).T
        join_keys = jnp.concatenate([own_keys, block_keys], axis=0).astype(jnp.float32)
        join_values = jnp.concatenate([own_values, block_values], axis=0).astype(jnp.float32)
        join_decay = jnp.concatenate([own_decay, block_decay], axis=1)
        scores = jnp.einsum('qhd,khd->hqk', piece_q, join_keys) * score_scale
        scores = scores + piece_decay.T[:, :, None] - join_decay[:, None, :]
        visible = jnp.concatenate([jnp.ones((PIECE, CACHE_DEV), jnp.bool_), query_pos[:, None] >= (piece_start + key_local)[None, :]], axis=1)
        scores = jnp.where(visible[None], scores, negative)
        row_high = lax.optimization_barrier(jnp.max(scores, axis=-1))
        exp_scores = jnp.exp(scores - row_high[..., None])
        row_mass = lax.optimization_barrier(jnp.sum(exp_scores, axis=-1))
        block_weights = lax.optimization_barrier(exp_scores.astype(jnp.bfloat16)).astype(jnp.float32)
        block_means = (jnp.einsum('hqk,khd->hqd', block_weights, join_values) / row_mass[..., None]).astype(jnp.bfloat16)
        block_means = lax.optimization_barrier(block_means).astype(jnp.float32)
        new_best = jnp.maximum(best_high, row_high)
        keep_old = jnp.exp(best_high - new_best)
        add_new = row_mass * jnp.exp(row_high - new_best)
        mass_sum = mass_sum * keep_old + add_new
        weighted = weighted * keep_old[..., None] + add_new[..., None] * block_means
        return ((new_best, mass_sum, weighted), None)
    start_state = (jnp.full((HEADS, PIECE), negative, jnp.float32), jnp.zeros((HEADS, PIECE), jnp.float32), jnp.zeros((HEADS, PIECE, HEAD), jnp.float32))
    (best_high, mass_sum, weighted), unused = lax.scan(visit_block, start_state, jnp.arange(N_KV, dtype=jnp.int32))
    piece_att = (weighted / mass_sum[..., None]).astype(jnp.bfloat16).transpose(1, 0, 2).reshape(PIECE, HEADS * HEAD)
    step_q = queries[PIECE:].reshape(DEC, HEADS, HEAD).astype(jnp.float32)
    step_k = new_keys[PIECE:].reshape(DEC, HEADS, HEAD).astype(jnp.float32)
    step_v = new_values[PIECE:].reshape(DEC, HEADS, HEAD).astype(jnp.float32)
    step_lg = log_gates[PIECE:]
    in_cache = jnp.arange(DEC_LEN, dtype=jnp.int32)[None, :] < step_lengths[:, None]
    kept_gates = jnp.where(in_cache[:, None, :], step_gates, 0.0)
    after_sum = lax.cumsum(kept_gates, axis=2, reverse=True) - kept_gates
    cache_scores = jnp.einsum('bhd,blhd->bhl', step_q, step_keys.reshape(DEC, DEC_LEN, HEADS, HEAD).astype(jnp.float32)) * score_scale
    cache_scores = cache_scores + step_lg[:, :, None] + after_sum
    cache_scores = jnp.where(in_cache[:, None, :], cache_scores, negative)
    self_scores = lax.optimization_barrier(jnp.sum(step_q * step_k, axis=-1)) * score_scale
    step_high = jnp.maximum(lax.optimization_barrier(jnp.max(cache_scores, axis=-1)), self_scores)
    cache_exp = jnp.exp(cache_scores - step_high[..., None])
    self_exp = jnp.exp(self_scores - step_high)
    step_mass = lax.optimization_barrier(jnp.sum(cache_exp, axis=-1)) + self_exp
    cache_weights = lax.optimization_barrier(cache_exp.astype(jnp.bfloat16)).astype(jnp.float32)
    self_weights = lax.optimization_barrier(self_exp.astype(jnp.bfloat16)).astype(jnp.float32)
    step_mix = jnp.einsum('bhl,blhd->bhd', cache_weights, step_values.reshape(DEC, DEC_LEN, HEADS, HEAD).astype(jnp.float32))
    step_mix = step_mix + self_weights[..., None] * step_v
    step_att = (step_mix / step_mass[..., None]).astype(jnp.bfloat16).reshape(DEC, HEADS * HEAD)
    piece_out = jnp.dot(piece_att, out_weight, preferred_element_type=jnp.float32).astype(jnp.bfloat16)
    step_out = jnp.dot(step_att, out_weight, preferred_element_type=jnp.float32).astype(jnp.bfloat16)
    return (piece_out, step_out)
```

```python
import functools
import math

import jax
import jax.numpy as jnp
from jax import lax
from jax.experimental import pallas as pl
from jax.experimental.pallas import tpu as pltpu
from jax.sharding import PartitionSpec as P

norm_eps = 1e-06
negative = -1e30
log2e = math.log2(math.e)
MESH = pl.DeviceIdType.MESH
F32 = jnp.float32
BF16 = jnp.bfloat16
NT = (((1,), (1,)), ((), ()))


def iota(shape, dim):
    return lax.broadcasted_iota(jnp.int32, shape, dim)


def normalize(rows, gain):
    wide = rows.astype(F32)
    factor = lax.rsqrt(jnp.mean(wide * wide, axis=-1, keepdims=True) + norm_eps)
    return (wide * factor * gain).astype(BF16)


def to_column(row, count):
    eye = iota((count, count), 0) == iota((count, count), 1)
    return jnp.sum(jnp.where(eye, row, 0.0), axis=1, keepdims=True)


def kernel(
    n, heads, width,
    tok_h, stok_h, gain_h, gate_w_h, gate_b_h, total_h, cache_decay_h, step_gates_h, step_len_h,
    wq, wk, wv, cache_k, cache_v, step_k, step_v, w_out,
    out_piece, out_step,
    tok, stok, gain, gate_w, gate_b, total_decay, cache_decay, step_gates, step_len,
    nrm, wq_v, wk_v, wv_v, k_all, cv_v, v_turned, sk_v, sv_v, wo_v,
    q_all, lg, gate_in, gate_out, bias_rows, bias_lanes, picks,
    own_mean, own_stat, to_r, to_l, stat_r, stat_l, own_final, own_final_stat, att,
    local_sem, q_right, q_left, q_recv, g_send, g_recv,
    m_send, m_recv, s_send, s_recv, x_send, x_recv,
):
    me = lax.axis_index("kv")
    tp = lax.axis_index("tp")
    rows = tok.shape[0]
    steps = stok.shape[0]
    cache_len = cache_k.shape[0]
    span = step_k.shape[0] // steps
    local = heads * width
    pair_lanes = 2 * width
    pairs = heads // 2
    keys = cache_len + rows
    root = math.sqrt(width)
    scale = log2e / root

    count = [0]

    def fetch(src, dst):
        copy = pltpu.make_async_copy(src, dst, local_sem.at[count[0]])
        count[0] += 1
        copy.start()
        return copy

    halves = 2 if local % 256 == 0 else 1
    part = local // halves
    c_tok = fetch(tok_h, tok)
    c_gain = fetch(gain_h, gain)
    c_stok = fetch(stok_h, stok)
    c_wq = [
        fetch(wq.at[:, pl.ds(c * part, part)], wq_v.at[:, pl.ds(c * part, part)])
        for c in range(halves)
    ]
    c_gw = fetch(gate_w_h, gate_w)
    c_gb = fetch(gate_b_h, gate_b)
    c_wk = fetch(wk, wk_v)
    c_wv = fetch(wv, wv_v)
    c_ck = fetch(cache_k, k_all.at[pl.ds(0, cache_len)])
    c_cv = fetch(cache_v, cv_v)
    c_td = fetch(total_h, total_decay)
    c_cd = fetch(cache_decay_h, cache_decay)
    c_sk = fetch(step_k, sk_v)
    c_sv = fetch(step_v, sv_v)
    c_sg = fetch(step_gates_h, step_gates)
    c_sl = fetch(step_len_h, step_len)
    c_wo = fetch(w_out, wo_v)

    has_right = me < n - 1
    has_left = me > 0
    right = lax.rem(me + 1, n)
    left = lax.rem(me + n - 1, n)

    barrier = pltpu.get_barrier_semaphore()

    @pl.when(has_right)
    def _():
        pl.semaphore_signal(barrier, inc=1, device_id={"kv": right}, device_id_type=MESH)

    @pl.when(has_left)
    def _():
        pl.semaphore_signal(barrier, inc=1, device_id={"kv": left}, device_id_type=MESH)

    pl.semaphore_signal(barrier, inc=1, device_id={"tp": 1 - tp}, device_id_type=MESH)

    def q_copy(source, p, sems, target):
        return pltpu.make_async_remote_copy(
            src_ref=q_all.at[source, p], dst_ref=q_all.at[source, p],
            send_sem=sems.at[source, p], recv_sem=q_recv.at[source, p],
            device_id={"kv": target}, device_id_type=MESH,
        )

    def q_to_right(source, p):
        return q_copy(source, p, q_right, right)

    def q_to_left(source, p):
        return q_copy(source, p, q_left, left)

    def part_copies(side, owner, p):
        means, stats, target = (to_r, stat_r, right) if side == 0 else (to_l, stat_l, left)
        return [
            pltpu.make_async_remote_copy(
                src_ref=ref.at[owner, p], dst_ref=ref.at[owner, p],
                send_sem=send.at[side, owner, p], recv_sem=recv.at[side, owner, p],
                device_id={"kv": target}, device_id_type=MESH,
            )
            for ref, send, recv in ((means, m_send, m_recv), (stats, s_send, s_recv))
        ]

    def send_part(side, owner, p):
        for copy in part_copies(side, owner, p):
            copy.start()

    def wait_part(side, owner, p):
        for copy in part_copies(side, owner, p):
            copy.wait_recv()

    c_tok.wait()
    c_gain.wait()
    c_stok.wait()
    nrm[pl.ds(0, rows)] = normalize(tok[...], gain[...])
    pad = nrm.shape[0] - rows
    step_norm = normalize(stok[...], gain[...]).astype(F32)
    step_rows = jnp.zeros((pad, nrm.shape[1]), F32)
    for b in range(steps):
        step_rows = jnp.where(iota((pad, nrm.shape[1]), 0) == b, step_norm[b : b + 1], step_rows)
    nrm[pl.ds(rows, pad)] = step_rows.astype(BF16)

    pairs_in_part = part // pair_lanes
    step_q_parts = []
    for c in range(halves):
        c_wq[c].wait()
        q_new = jnp.dot(
            nrm[...], wq_v[:, c * part : (c + 1) * part], preferred_element_type=F32
        ).astype(BF16)
        turned = q_new[:rows].T
        for i in range(pairs_in_part):
            q_all[me, c * pairs_in_part + i] = turned[i * pair_lanes : (i + 1) * pair_lanes]
        step_q_parts.append(q_new[rows:].astype(F32))
        if c == 0:
            pl.semaphore_wait(
                barrier, 1 + has_right.astype(jnp.int32) + has_left.astype(jnp.int32)
            )
        for i in range(pairs_in_part):
            p = c * pairs_in_part + i

            @pl.when(has_right)
            def _():
                q_to_right(me, p).start()

            @pl.when(has_left)
            def _():
                q_to_left(me, p).start()

    step_q = jnp.concatenate(step_q_parts, axis=1)

    c_gw.wait()
    c_gb.wait()
    logits = lax.dot_general(gate_w[...], nrm[...], NT, preferred_element_type=F32)
    logits = logits + to_column(gate_b[...], gate_w.shape[0])
    lg[...] = jnp.minimum(logits, 0.0) - jnp.log1p(jnp.exp(-jnp.abs(logits)))
    own_lg = lg[pl.ds(pl.multiple_of(tp * heads, heads), heads), :]
    piece_lg = own_lg[:, :rows]
    own_sum = jnp.broadcast_to(jnp.sum(piece_lg, axis=1, keepdims=True), gate_out.shape)

    g_copy = pltpu.make_async_remote_copy(
        src_ref=gate_out, dst_ref=gate_in, send_sem=g_send, recv_sem=g_recv,
        device_id={"kv": right}, device_id_type=MESH,
    )

    @pl.when(jnp.logical_not(has_left))
    def _():
        gate_in[...] = jnp.zeros(gate_in.shape, F32)
        gate_out[...] = own_sum

        @pl.when(has_right)
        def _():
            g_copy.start()

    c_wk.wait()
    k_new = jnp.dot(nrm[...], wk_v[...], preferred_element_type=F32).astype(BF16)
    k_all[pl.ds(cache_len, rows)] = k_new[:rows]
    step_nk = k_new[rows:].astype(F32)
    c_wv.wait()
    v_new = jnp.dot(nrm[...], wv_v[...], preferred_element_type=F32).astype(BF16)
    v_turned[:, pl.ds(cache_len, rows)] = v_new[:rows].T
    step_nv = v_new[rows:].astype(F32)
    c_cv.wait()
    v_turned[:, pl.ds(0, cache_len)] = cv_v[...].T

    upto = (iota((rows, rows), 0) <= iota((rows, rows), 1)).astype(F32)
    running = jnp.dot(
        piece_lg, upto, preferred_element_type=F32, precision=lax.Precision.HIGHEST
    )

    def bias_terms(bias):
        high = bias.astype(BF16).astype(F32)
        rest = bias - high
        middle = rest.astype(BF16).astype(F32)
        low = rest - middle
        blank = jnp.zeros((128 - 3 * heads, bias.shape[1]), F32)
        return jnp.concatenate([high, middle, low, blank], axis=0).T.astype(BF16)

    c_td.wait()
    c_cd.wait()
    lg_start = to_column(total_decay[...], gate_w.shape[0])
    start_rows = jnp.where(tp == 0, lg_start[:heads], lg_start[heads : 2 * heads])
    bias_lanes[pl.ds(0, cache_len)] = bias_terms((start_rows - cache_decay[...]) * root)
    bias_rows[...] = running

    head_of_column = lax.div(iota((128, 2 * rows), 1), rows)
    lane_of_term = iota((128, 2 * rows), 0)
    for p in range(pairs):
        hit = jnp.logical_and(
            lax.rem(lane_of_term, heads) == 2 * p + head_of_column, lane_of_term < 3 * heads
        )
        picks[p] = hit.astype(F32).astype(BF16)

    def finish_bias():
        @pl.when(has_left)
        def _():
            g_copy.wait_recv()

            @pl.when(has_right)
            def _():
                gate_out[...] = gate_in[...] + own_sum
                g_copy.start()

        fresh = -(gate_in[:, :1] + bias_rows[...]) * root
        bias_lanes[pl.ds(cache_len, rows)] = bias_terms(fresh)

    @pl.when(has_right)
    def _():
        finish_bias()

    c_ck.wait()

    first_rows = iota((pair_lanes, rows), 0) < width
    causal = lax.rem(iota((rows, 2 * rows), 1), rows) >= iota((rows, 2 * rows), 0)

    def spread(two):
        return jnp.concatenate(
            [
                jnp.broadcast_to(two[0:1], (width, rows)),
                jnp.broadcast_to(two[1:2], (width, rows)),
            ],
            axis=0,
        )

    def attend(source, p, used, masked):
        q_pair = q_all[source, p]
        zero = jnp.zeros_like(q_pair)
        rhs = jnp.concatenate(
            [
                jnp.concatenate(
                    [jnp.where(first_rows, q_pair, zero), jnp.where(first_rows, zero, q_pair)],
                    axis=1,
                ),
                picks[p],
            ],
            axis=0,
        )
        lanes = pl.ds(p * pair_lanes, pair_lanes)
        lhs = jnp.concatenate([k_all[pl.ds(0, used), lanes], bias_lanes[pl.ds(0, used)]], axis=1)
        raw = jnp.dot(lhs, rhs, preferred_element_type=F32)
        if masked:
            fresh = jnp.where(causal, raw[cache_len:], negative)
            raw = jnp.concatenate([raw[:cache_len], fresh], axis=0)
        high = jnp.max(raw, axis=0, keepdims=True)
        weight = jnp.exp2((raw - high) * scale)
        mass = jnp.sum(weight, axis=0, keepdims=True)
        mix = jnp.dot(
            v_turned[lanes, pl.ds(0, used)], weight.astype(BF16), preferred_element_type=F32
        )
        mix = mix * (1.0 / mass)
        mean = jnp.concatenate([mix[:width, :rows], mix[width:, rows:]], axis=0)
        level = high * scale + jnp.log2(mass)
        return mean, jnp.concatenate([level[:, :rows], level[:, rows:]], axis=0)

    def merge(pieces):
        best = functools.reduce(jnp.maximum, [level for _, level in pieces])
        shares = [jnp.exp2(level - best) for _, level in pieces]
        total = functools.reduce(jnp.add, shares)
        inverse = 1.0 / total
        mean = functools.reduce(
            jnp.add,
            [spread(share * inverse) * mean for share, (mean, _) in zip(shares, pieces)],
        )
        return mean, best + jnp.log2(total)

    def attend_left(k, p):
        source = me - k
        q_to_right(source, p).wait_recv()

        @pl.when(has_right)
        def _():
            q_to_right(source, p).start()

        mean, level = attend(source, p, cache_len, False)

        @pl.when(has_right)
        def _():
            own_mean[source, p] = mean
            own_stat[source, p] = level

        @pl.when(jnp.logical_not(has_right))
        def _():
            to_l[source, p] = mean.astype(BF16)
            stat_l[source, p] = level
            send_part(1, source, p)

    def attend_right(k, p):
        source = me + k
        q_to_left(source, p).wait_recv()

        @pl.when(has_left)
        def _():
            q_to_left(source, p).start()

        mean, level = attend(source, p, keys, False)

        @pl.when(has_left)
        def _():
            own_mean[source, p] = mean
            own_stat[source, p] = level

        @pl.when(jnp.logical_not(has_left))
        def _():
            to_r[source, p] = mean.astype(BF16)
            stat_r[source, p] = level
            send_part(0, source, p)

    def attend_own():
        @pl.when(jnp.logical_not(has_right))
        def _():
            finish_bias()

        for p in range(pairs):
            mean, level = attend(me, p, keys, True)
            own_final[p] = mean
            own_final_stat[p] = level

    def decode():
        head_mask = lax.div(iota((heads, local), 1), width) == iota((heads, local), 0)
        chunk = 128
        chunks = span // chunk
        later = (iota((chunk, chunk), 0) > iota((chunk, chunk), 1)).astype(F32)
        c_sk.wait()
        c_sv.wait()
        c_sg.wait()
        c_sl.wait()
        step_att = jnp.zeros((pad, local), F32)
        for b in range(steps):
            length = step_len[b]
            in_cache = iota((heads, span), 1) < length
            kept = jnp.where(in_cache, step_gates[b], 0.0)
            tail = jnp.zeros((heads, 1), F32)
            parts = [None] * chunks
            for c in reversed(range(chunks)):
                piece = kept[:, c * chunk : (c + 1) * chunk]
                inner = jnp.dot(
                    piece, later, preferred_element_type=F32, precision=lax.Precision.HIGHEST
                )
                parts[c] = inner + tail
                tail = tail + jnp.sum(piece, axis=1, keepdims=True)
            after = jnp.concatenate(parts, axis=1)
            q_row = jnp.where(head_mask, step_q[b : b + 1], 0.0)
            scores = lax.dot_general(
                q_row.astype(BF16), sk_v[pl.ds(b * span, span)], NT, preferred_element_type=F32
            )
            new_lg = own_lg[:, rows + b : rows + b + 1]
            scores = scores * scale + (new_lg + after) * log2e
            scores = jnp.where(in_cache, scores, negative)
            self_score = jnp.sum(q_row * step_nk[b : b + 1], axis=1, keepdims=True) * scale
            high = jnp.maximum(jnp.max(scores, axis=1, keepdims=True), self_score)
            weight = jnp.exp2(scores - high)
            self_weight = jnp.exp2(self_score - high)
            mass = jnp.sum(weight, axis=1, keepdims=True) + self_weight
            mix = jnp.dot(
                weight.astype(BF16), sv_v[pl.ds(b * span, span)], preferred_element_type=F32
            )
            mix = mix + self_weight.astype(BF16).astype(F32) * step_nv[b : b + 1]
            one = jnp.sum(jnp.where(head_mask, mix / mass, 0.0), axis=0, keepdims=True)
            step_att = jnp.where(iota((pad, local), 0) == b, one, step_att)
        done = step_att.astype(BF16)
        for p in range(pairs):
            att[tp * pairs + p, pl.ds(rows, pad)] = done[:, p * pair_lanes : (p + 1) * pair_lanes]

    def step(k, carry):
        for p in range(pairs):
            @pl.when(me >= k)
            def _():
                attend_left(k, p)

            @pl.when(me + k < n)
            def _():
                attend_right(k, p)

        @pl.when(k == 1)
        def _():
            decode()

        @pl.when(k == min(2, n - 1))
        def _():
            attend_own()

        return carry

    lax.fori_loop(1, n, step, 0)

    def forward(side, owner, p):
        wait_part(side, owner, p)
        means, stats = (to_r, stat_r) if side == 0 else (to_l, stat_l)
        mean, level = merge(
            [
                (means[owner, p].astype(F32), stats[owner, p]),
                (own_mean[owner, p], own_stat[owner, p]),
            ]
        )
        means[owner, p] = mean.astype(BF16)
        stats[owner, p] = level
        send_part(side, owner, p)

    def pass_right(r):
        @pl.when(jnp.logical_and(has_left, r > me))
        def _():
            for p in range(pairs):
                forward(0, r, p)

    def pass_left(r):
        owner = n - 1 - r

        @pl.when(jnp.logical_and(has_right, owner < me))
        def _():
            for p in range(pairs):
                forward(1, owner, p)

    def turn(r, carry):
        @pl.when(2 * me < n)
        def _():
            pass_right(r)
            pass_left(r)

        @pl.when(2 * me >= n)
        def _():
            pass_left(r)
            pass_right(r)

        return carry

    lax.fori_loop(1, n, turn, 0)

    def swap(p):
        slot = tp * pairs + p
        return pltpu.make_async_remote_copy(
            src_ref=att.at[slot], dst_ref=att.at[slot],
            send_sem=x_send.at[p], recv_sem=x_recv.at[p],
            device_id={"tp": 1 - tp}, device_id_type=MESH,
        )

    def swap_in(p):
        slot = (1 - tp) * pairs + p
        return pltpu.make_async_remote_copy(
            src_ref=att.at[slot], dst_ref=att.at[slot],
            send_sem=x_send.at[p], recv_sem=x_recv.at[p],
            device_id={"tp": 1 - tp}, device_id_type=MESH,
        )

    def finish(p, sides):
        pieces = [(own_final[p], own_final_stat[p])]
        for side in sides:
            wait_part(side, me, p)
            means, stats = (to_r, stat_r) if side == 0 else (to_l, stat_l)
            pieces.append((means[me, p].astype(F32), stats[me, p]))
        mean, _ = merge(pieces)
        att[tp * pairs + p, pl.ds(0, rows)] = mean.T.astype(BF16)
        swap(p).start()

    @pl.when(jnp.logical_and(has_left, has_right))
    def _():
        for p in range(pairs):
            finish(p, (0, 1))

    @pl.when(jnp.logical_and(has_left, jnp.logical_not(has_right)))
    def _():
        for p in range(pairs):
            finish(p, (0,))

    @pl.when(jnp.logical_and(has_right, jnp.logical_not(has_left)))
    def _():
        for p in range(pairs):
            finish(p, (1,))

    c_wo.wait()
    for p in range(pairs):
        swap_in(p).wait_recv()
    whole = jnp.concatenate([att[i] for i in range(2 * pairs)], axis=1)
    projected = jnp.dot(whole, wo_v[...], preferred_element_type=F32)
    out_piece[...] = projected[:rows].astype(BF16)
    out_step[...] = projected[rows : rows + steps].astype(BF16)

    for p in range(pairs):
        swap(p).wait_send()

    @pl.when(has_right)
    def _():
        g_copy.wait_send()

    def sent(owner, carry):
        for p in range(pairs):
            @pl.when(jnp.logical_and(has_right, owner <= me))
            def _():
                q_to_right(owner, p).wait_send()

            @pl.when(jnp.logical_and(has_left, owner >= me))
            def _():
                q_to_left(owner, p).wait_send()

            @pl.when(owner > me)
            def _():
                for copy in part_copies(0, owner, p):
                    copy.wait_send()

            @pl.when(owner < me)
            def _():
                for copy in part_copies(1, owner, p):
                    copy.wait_send()

        return carry

    lax.fori_loop(0, n, sent, 0)


def per_device(
    piece_tokens, step_tokens, norm_gain, query_weight, key_weight, value_weight,
    gate_weight, gate_bias, out_weight, cache_keys, cache_values, cache_decay,
    decay_total, step_keys, step_values, step_gates, step_lengths,
):
    n = lax.axis_size("kv")
    rows, model = piece_tokens.shape
    steps = step_tokens.shape[0]
    heads = cache_decay.shape[0]
    local = query_weight.shape[1]
    width = local // heads
    pairs = heads // 2
    cache_len = cache_keys.shape[0]
    keys = cache_len + rows
    span = step_keys.shape[1]
    columns = out_weight.shape[1]
    padded = rows + 16 * (-(-steps // 16))
    all_heads = gate_weight.shape[1]
    vmem = pl.BlockSpec(memory_space=pltpu.VMEM)
    hbm = pl.BlockSpec(memory_space=pltpu.HBM)
    dma = pltpu.SemaphoreType.DMA
    return pl.pallas_call(
        functools.partial(kernel, n, heads, width),
        out_shape=(
            jax.ShapeDtypeStruct((rows, columns), BF16),
            jax.ShapeDtypeStruct((steps, columns), BF16),
        ),
        in_specs=[hbm] * 17,
        out_specs=(vmem, vmem),
        scratch_shapes=[
            pltpu.VMEM((rows, model), BF16),
            pltpu.VMEM((steps, model), BF16),
            pltpu.VMEM((1, model), F32),
            pltpu.VMEM((all_heads, model), BF16),
            pltpu.VMEM((1, all_heads), F32),
            pltpu.VMEM((1, all_heads), F32),
            pltpu.VMEM(cache_decay.shape, F32),
            pltpu.VMEM(step_gates.shape, F32),
            pltpu.SMEM((steps,), jnp.int32),
            pltpu.VMEM((padded, model), BF16),
            pltpu.VMEM(query_weight.shape, BF16),
            pltpu.VMEM(key_weight.shape, BF16),
            pltpu.VMEM(value_weight.shape, BF16),
            pltpu.VMEM((keys, local), BF16),
            pltpu.VMEM((cache_len, local), BF16),
            pltpu.VMEM((local, keys), BF16),
            pltpu.VMEM((steps * span, local), BF16),
            pltpu.VMEM((steps * span, local), BF16),
            pltpu.VMEM(out_weight.shape, BF16),
            pltpu.VMEM((n, pairs, 2 * width, rows), BF16),
            pltpu.VMEM((all_heads, padded), F32),
            pltpu.VMEM((heads, 128), F32),
            pltpu.VMEM((heads, 128), F32),
            pltpu.VMEM((heads, rows), F32),
            pltpu.VMEM((keys, 128), BF16),
            pltpu.VMEM((pairs, 128, 2 * rows), BF16),
            pltpu.VMEM((n, pairs, 2 * width, rows), F32),
            pltpu.VMEM((n, pairs, 2, rows), F32),
            pltpu.VMEM((n, pairs, 2 * width, rows), BF16),
            pltpu.VMEM((n, pairs, 2 * width, rows), BF16),
            pltpu.VMEM((n, pairs, 2, rows), F32),
            pltpu.VMEM((n, pairs, 2, rows), F32),
            pltpu.VMEM((pairs, 2 * width, rows), F32),
            pltpu.VMEM((pairs, 2, rows), F32),
            pltpu.VMEM((2 * pairs, padded, 2 * width), BF16),
            dma((20,)),
            dma((n, pairs)), dma((n, pairs)), dma((n, pairs)),
            dma(()), dma(()),
            dma((2, n, pairs)), dma((2, n, pairs)), dma((2, n, pairs)), dma((2, n, pairs)),
            dma((pairs,)), dma((pairs,)),
        ],
        compiler_params=pltpu.CompilerParams(
            collective_id=0, has_side_effects=True, vmem_limit_bytes=60 * 1024 * 1024
        ),
    )(
        piece_tokens, step_tokens, norm_gain.reshape(1, -1), gate_weight.T,
        gate_bias.reshape(1, -1), decay_total.reshape(1, -1), cache_decay, step_gates,
        step_lengths, query_weight, key_weight, value_weight,
        cache_keys, cache_values,
        step_keys.reshape(steps * span, local), step_values.reshape(steps * span, local),
        out_weight,
    )


def solution(mesh):
    rows = P(("dp", "kv"), None)
    both = P(("dp", "kv"), "tp")
    cols = P(None, "tp")
    in_specs = (
        rows, rows, P(), cols, cols, cols, P(), P(), cols, both, both,
        P("tp", ("dp", "kv")), P("dp"),
        P(("dp", "kv"), None, "tp"), P(("dp", "kv"), None, "tp"),
        P(("dp", "kv"), "tp", None), P(("dp", "kv")),
    )
    return jax.shard_map(
        per_device, mesh=mesh, in_specs=in_specs, out_specs=(both, both), check_vma=False
    )
```

```python
import functools
import math

import jax
import jax.numpy as jnp
from jax import lax
from jax.experimental import pallas as pl
from jax.experimental.pallas import tpu as pltpu
from jax.sharding import PartitionSpec as P

norm_eps = 1e-06
negative = -1e30
log2e = math.log2(math.e)
MESH = pl.DeviceIdType.MESH
F32 = jnp.float32
BF16 = jnp.bfloat16
NT = (((1,), (1,)), ((), ()))


def mark(name):
    return


def iota(shape, dim):
    return lax.broadcasted_iota(jnp.int32, shape, dim)


def normalize(rows, gain):
    wide = rows.astype(F32)
    factor = lax.rsqrt(jnp.mean(wide * wide, axis=-1, keepdims=True) + norm_eps)
    return (wide * factor * gain).astype(BF16)


def to_column(row, count):
    eye = iota((count, count), 0) == iota((count, count), 1)
    return jnp.sum(jnp.where(eye, row, 0.0), axis=1, keepdims=True)


def kernel(
    n, heads, width,
    tok_h, stok_h, gain_h, gate_w_h, gate_b_h, total_h, cache_decay_h, step_gates_h, step_len_h,
    wq, wk, wv, cache_k, cache_v, step_k, step_v,
    out_att,
    tok, stok, gain, gate_w, gate_b, total_decay, cache_decay, step_gates, step_len,
    nrm, wq_v, wk_v, wv_v, k_all, cv_v, v_turned, sk_v, sv_v,
    q_all, lg, gate_in, gate_out, bias_rows, bias_lanes, picks,
    own_mean, own_stat, to_r, to_l, stat_r, stat_l, near, near_stat, own_final, own_final_stat, att,
    local_sem, q_right, q_left, q_far, q_recv, g_send, g_recv, far_sem,
    m_send, m_recv, s_send, s_recv, x_send, x_recv,
):
    me = lax.axis_index("kv")
    tp = lax.axis_index("tp")
    rows = tok.shape[0]
    steps = stok.shape[0]
    cache_len = cache_k.shape[0]
    span = step_k.shape[0] // steps
    local = heads * width
    pair_lanes = 2 * width
    pairs = heads // 2
    keys = cache_len + rows
    root = math.sqrt(width)
    scale = log2e / root

    count = [0]

    def fetch(src, dst):
        copy = pltpu.make_async_copy(src, dst, local_sem.at[count[0]])
        count[0] += 1
        copy.start()
        return copy

    halves = 2 if local % 256 == 0 else 1
    part = local // halves
    c_tok = fetch(tok_h, tok)
    c_gain = fetch(gain_h, gain)
    c_stok = fetch(stok_h, stok)
    c_wq = [
        fetch(wq.at[:, pl.ds(c * part, part)], wq_v.at[:, pl.ds(c * part, part)])
        for c in range(halves)
    ]
    c_gw = fetch(gate_w_h, gate_w)
    c_gb = fetch(gate_b_h, gate_b)
    c_wk = fetch(wk, wk_v)
    c_wv = fetch(wv, wv_v)
    c_ck = fetch(cache_k, k_all.at[pl.ds(0, cache_len)])
    c_cv = fetch(cache_v, cv_v)
    c_td = fetch(total_h, total_decay)
    c_cd = fetch(cache_decay_h, cache_decay)
    c_sk = fetch(step_k, sk_v)
    c_sv = fetch(step_v, sv_v)
    c_sg = fetch(step_gates_h, step_gates)
    c_sl = fetch(step_len_h, step_len)

    has_right = me < n - 1
    has_left = me > 0
    right = lax.rem(me + 1, n)
    left = lax.rem(me + n - 1, n)

    reach = n >= 4
    first, last = 0, n - 1
    middle = jnp.logical_and(has_left, has_right)
    edge = jnp.logical_not(middle)

    def both(a, b):
        return jnp.logical_and(a, b)

    def as_count(flag):
        return flag.astype(jnp.int32)

    barrier = pltpu.get_barrier_semaphore()

    def hello(condition, target):
        @pl.when(condition)
        def _():
            pl.semaphore_signal(barrier, inc=1, device_id={"kv": target}, device_id_type=MESH)

    hello(has_right, right)
    hello(has_left, left)
    pl.semaphore_signal(barrier, inc=1, device_id={"tp": 1 - tp}, device_id_type=MESH)
    greeted = 1 + as_count(has_right) + as_count(has_left)
    if reach:
        hello(me == first, last)
        hello(me == first, 2)
        hello(me == n - 3, last)
        greeted = greeted + 2 * as_count(me == last) + as_count(me == 2)

    def enter():
        pl.semaphore_wait(barrier, greeted)
        if reach:
            @pl.when(me == last)
            def _():
                for target in (first, n - 3):
                    pl.semaphore_signal(
                        far_sem, inc=1, device_id={"kv": target}, device_id_type=MESH
                    )

    def q_copy(source, p, sem, target):
        return pltpu.make_async_remote_copy(
            src_ref=q_all.at[source, p], dst_ref=q_all.at[source, p],
            send_sem=sem, recv_sem=q_recv.at[source, p],
            device_id={"kv": target}, device_id_type=MESH,
        )

    def q_to_right(source, p):
        return q_copy(source, p, q_right.at[source], right)

    def q_to_left(source, p):
        return q_copy(source, p, q_left.at[source], left)

    def q_to_far(p):
        return q_copy(me, p, q_far, last - me)

    size = 2 if pairs % 2 == 0 else 1
    groups = [range(g, g + size) for g in range(0, pairs, size)]

    def part_target(side, owner):
        if side == 0:
            straight = both(owner == last, me == n - 3)
            return jnp.where(straight, last, right) if reach else right
        straight = both(owner == first, me == 2)
        return jnp.where(straight, first, left) if reach else left

    def part_slot(side, owner, target):
        return owner if side == 0 else jnp.where(owner == target, n, owner)

    def mean_copy(side, owner, p):
        means = to_r if side == 0 else to_l
        target = part_target(side, owner)
        return pltpu.make_async_remote_copy(
            src_ref=means.at[owner, p], dst_ref=means.at[owner, p],
            send_sem=m_send.at[owner], recv_sem=m_recv.at[part_slot(side, owner, target), p],
            device_id={"kv": target}, device_id_type=MESH,
        )

    def stat_copy(side, owner, g):
        stats = stat_r if side == 0 else stat_l
        target = part_target(side, owner)
        return pltpu.make_async_remote_copy(
            src_ref=stats.at[owner, g], dst_ref=stats.at[owner, g],
            send_sem=s_send.at[owner], recv_sem=s_recv.at[part_slot(side, owner, target), g],
            device_id={"kv": target}, device_id_type=MESH,
        )

    def near_mean(p):
        return pltpu.make_async_remote_copy(
            src_ref=near.at[p], dst_ref=near.at[p],
            send_sem=m_send.at[n], recv_sem=m_recv.at[n + 1, p],
            device_id={"kv": jnp.where(me == 1, first, last)}, device_id_type=MESH,
        )

    def near_level(g):
        return pltpu.make_async_remote_copy(
            src_ref=near_stat.at[g], dst_ref=near_stat.at[g],
            send_sem=s_send.at[n], recv_sem=s_recv.at[n + 1, g],
            device_id={"kv": jnp.where(me == 1, first, last)}, device_id_type=MESH,
        )

    def await_mean(means, slot, owner, p):
        pltpu.make_async_remote_copy(
            src_ref=means.at[owner, p], dst_ref=means.at[owner, p],
            send_sem=m_send.at[owner], recv_sem=m_recv.at[slot, p],
            device_id={"tp": 1 - tp}, device_id_type=MESH,
        ).wait_recv()

    def await_stat(stats, slot, owner, g):
        pltpu.make_async_remote_copy(
            src_ref=stats.at[owner, g], dst_ref=stats.at[owner, g],
            send_sem=s_send.at[owner], recv_sem=s_recv.at[slot, g],
            device_id={"tp": 1 - tp}, device_id_type=MESH,
        ).wait_recv()

    def all_sent(ref, sem, recv):
        pltpu.make_async_remote_copy(
            src_ref=ref, dst_ref=ref, send_sem=sem, recv_sem=recv,
            device_id={"tp": 1 - tp}, device_id_type=MESH,
        ).wait_send()

    @pl.when(me == last)
    def _():
        enter()

    mark("start")
    c_tok.wait()
    c_gain.wait()
    c_stok.wait()
    mark("tok")
    nrm[pl.ds(0, rows)] = normalize(tok[...], gain[...])
    pad = nrm.shape[0] - rows
    step_norm = normalize(stok[...], gain[...]).astype(F32)
    step_rows = jnp.zeros((pad, nrm.shape[1]), F32)
    for b in range(steps):
        step_rows = jnp.where(iota((pad, nrm.shape[1]), 0) == b, step_norm[b : b + 1], step_rows)
    nrm[pl.ds(rows, pad)] = step_rows.astype(BF16)

    mark("norm")
    def send_queries(which):
        for p in which:
            @pl.when(has_right)
            def _():
                q_to_right(me, p).start()

            @pl.when(has_left)
            def _():
                q_to_left(me, p).start()

    pairs_in_part = part // pair_lanes
    step_q_parts = []
    for c in range(halves):
        c_wq[c].wait()
        mark("wq")
        q_new = jnp.dot(
            nrm[...], wq_v[:, c * part : (c + 1) * part], preferred_element_type=F32
        ).astype(BF16)
        turned = q_new[:rows].T
        for i in range(pairs_in_part):
            q_all[me, c * pairs_in_part + i] = turned[i * pair_lanes : (i + 1) * pair_lanes]
        step_q_parts.append(q_new[rows:].astype(F32))

        @pl.when(has_left)
        def _():
            if c == 0:
                @pl.when(has_right)
                def _():
                    enter()

            send_queries(range(c * pairs_in_part, (c + 1) * pairs_in_part))

    @pl.when(jnp.logical_not(has_left))
    def _():
        enter()
        send_queries(range(pairs))

    if reach:
        @pl.when(me == last)
        def _():
            for p in range(pairs):
                q_to_far(p).start()

    step_q = jnp.concatenate(step_q_parts, axis=1)

    mark("qsent")
    c_gw.wait()
    c_gb.wait()
    logits = lax.dot_general(gate_w[...], nrm[...], NT, preferred_element_type=F32)
    logits = logits + to_column(gate_b[...], gate_w.shape[0])
    lg[...] = jnp.minimum(logits, 0.0) - jnp.log1p(jnp.exp(-jnp.abs(logits)))
    own_lg = lg[pl.ds(pl.multiple_of(tp * heads, heads), heads), :]
    piece_lg = own_lg[:, :rows]
    own_sum = jnp.broadcast_to(jnp.sum(piece_lg, axis=1, keepdims=True), gate_out.shape)

    g_copy = pltpu.make_async_remote_copy(
        src_ref=gate_out, dst_ref=gate_in, send_sem=g_send, recv_sem=g_recv,
        device_id={"kv": right}, device_id_type=MESH,
    )

    @pl.when(jnp.logical_not(has_left))
    def _():
        gate_in[...] = jnp.zeros(gate_in.shape, F32)
        gate_out[...] = own_sum

        @pl.when(has_right)
        def _():
            g_copy.start()

        if reach:
            pl.semaphore_wait(far_sem, 1)
            for p in range(pairs):
                q_to_far(p).start()

    mark("gates")
    c_wk.wait()
    c_wv.wait()
    c_cv.wait()
    c_td.wait()
    c_cd.wait()
    c_ck.wait()
    k_new = jnp.dot(nrm[...], wk_v[...], preferred_element_type=F32).astype(BF16)
    k_all[pl.ds(cache_len, rows)] = k_new[:rows]
    step_nk = k_new[rows:].astype(F32)
    v_new = jnp.dot(nrm[...], wv_v[...], preferred_element_type=F32).astype(BF16)
    v_turned[:, pl.ds(cache_len, rows)] = v_new[:rows].T
    step_nv = v_new[rows:].astype(F32)
    v_turned[:, pl.ds(0, cache_len)] = cv_v[...].T

    upto = (iota((rows, rows), 0) <= iota((rows, rows), 1)).astype(F32)
    running = jnp.dot(
        piece_lg, upto, preferred_element_type=F32, precision=lax.Precision.HIGHEST
    )

    def bias_terms(bias):
        high = bias.astype(BF16).astype(F32)
        rest = bias - high
        middle = rest.astype(BF16).astype(F32)
        low = rest - middle
        blank = jnp.zeros((128 - 3 * heads, bias.shape[1]), F32)
        return jnp.concatenate([high, middle, low, blank], axis=0).T.astype(BF16)

    lg_start = to_column(total_decay[...], gate_w.shape[0])
    start_rows = jnp.where(tp == 0, lg_start[:heads], lg_start[heads : 2 * heads])
    bias_lanes[pl.ds(0, cache_len)] = bias_terms((start_rows - cache_decay[...]) * root)
    bias_rows[...] = running

    head_of_column = lax.div(iota((128, 2 * rows), 1), rows)
    lane_of_term = iota((128, 2 * rows), 0)
    for p in range(pairs):
        hit = jnp.logical_and(
            lax.rem(lane_of_term, heads) == 2 * p + head_of_column, lane_of_term < 3 * heads
        )
        picks[p] = hit.astype(F32).astype(BF16)

    mark("bias")
    def finish_bias():
        @pl.when(has_left)
        def _():
            g_copy.wait_recv()

            @pl.when(has_right)
            def _():
                gate_out[...] = gate_in[...] + own_sum
                g_copy.start()

        fresh = -(gate_in[:, :1] + bias_rows[...]) * root
        bias_lanes[pl.ds(cache_len, rows)] = bias_terms(fresh)

    mark("fin")
    first_rows = iota((pair_lanes, rows), 0) < width
    causal = lax.rem(iota((rows, 2 * rows), 1), rows) >= iota((rows, 2 * rows), 0)

    def spread(two):
        return jnp.concatenate(
            [
                jnp.broadcast_to(two[0:1], (width, rows)),
                jnp.broadcast_to(two[1:2], (width, rows)),
            ],
            axis=0,
        )

    def scores_of(source, p, used):
        q_pair = q_all[source, p]
        zero = jnp.zeros_like(q_pair)
        rhs = jnp.concatenate(
            [
                jnp.concatenate(
                    [jnp.where(first_rows, q_pair, zero), jnp.where(first_rows, zero, q_pair)],
                    axis=1,
                ),
                picks[p],
            ],
            axis=0,
        )
        lanes = pl.ds(p * pair_lanes, pair_lanes)
        lhs = jnp.concatenate([k_all[pl.ds(0, used), lanes], bias_lanes[pl.ds(0, used)]], axis=1)
        return jnp.dot(lhs, rhs, preferred_element_type=F32)

    def weigh(raw):
        high = jnp.max(raw, axis=0, keepdims=True)
        weight = jnp.exp2((raw - high) * scale)
        mass = jnp.sum(weight, axis=0, keepdims=True)
        return weight.astype(BF16), mass, high * scale + jnp.log2(mass)

    def attend(source, group, used, masked):
        raws = [scores_of(source, p, used) for p in group]
        if masked:
            raws = [
                jnp.concatenate(
                    [raw[:cache_len], jnp.where(causal, raw[cache_len:], negative)], axis=0
                )
                for raw in raws
            ]
        weighed = [weigh(raw) for raw in raws]
        results = []
        for p, (weight, mass, level) in zip(group, weighed):
            values = v_turned[pl.ds(p * pair_lanes, pair_lanes), pl.ds(0, used)]
            mix = jnp.dot(values, weight, preferred_element_type=F32) * (1.0 / mass)
            mean = jnp.concatenate([mix[:width, :rows], mix[width:, rows:]], axis=0)
            levels = jnp.concatenate([level[:, :rows], level[:, rows:]], axis=0)
            results.append((p, mean, levels))
        return results

    def shares_of(levels):
        best = functools.reduce(jnp.maximum, levels)
        shares = [jnp.exp2(level - best) for level in levels]
        total = functools.reduce(jnp.add, shares)
        inverse = 1.0 / total
        return [share * inverse for share in shares], best + jnp.log2(total)

    def blend(shares, means, i):
        return functools.reduce(
            jnp.add,
            [spread(share[2 * i : 2 * i + 2]) * mean for share, mean in zip(shares, means)],
        )

    def stack(results):
        return jnp.concatenate([level for _, _, level in results], axis=0)

    def relay(from_left, k, group):
        if from_left:
            source, make, there, skip = me - k, q_to_right, me >= k, both(me - k == first, me == n - 2)
        else:
            source, make, there, skip = me + k, q_to_left, me + k < n, both(me + k == last, me == 1)

        @pl.when(there)
        def _():
            for p in group:
                make(source, p).wait_recv()
                if reach:
                    @pl.when(jnp.logical_not(skip))
                    def _():
                        make(source, p).start()
                else:
                    make(source, p).start()

    def keep(source, g, results):
        for p, mean, level in results:
            own_mean[source, p] = mean
        own_stat[source, g] = stack(results)

    def keep_near(g, results):
        for p, mean, level in results:
            near[p] = mean.astype(BF16)
        near_stat[g] = stack(results)
        near_level(g).start()
        for p, _, _ in results:
            near_mean(p).start()

    def attend_middle(from_left, k, g):
        source, used, there = (
            (me - k, cache_len, me >= k) if from_left else (me + k, keys, me + k < n)
        )
        relay(from_left, k, groups[g])

        @pl.when(there)
        def _():
            mark("L" if from_left else "R")
            results = attend(source, groups[g], used, False)
            if reach:
                is_near = (
                    both(source == first, k == 1) if from_left else both(source == last, k == 1)
                )

                @pl.when(is_near)
                def _():
                    keep_near(g, results)

                @pl.when(jnp.logical_not(is_near))
                def _():
                    keep(source, g, results)
            else:
                keep(source, g, results)

    def attend_edge(from_left, k, g):
        source, used, side = (me - k, cache_len, 1) if from_left else (me + k, keys, 0)
        means, stats = (to_l, stat_l) if from_left else (to_r, stat_r)
        make = q_to_right if from_left else q_to_left
        for p in groups[g]:
            make(source, p).wait_recv()
        mark("L" if from_left else "R")
        results = attend(source, groups[g], used, False)
        for p, mean, level in results:
            means[source, p] = mean.astype(BF16)
        stats[source, g] = stack(results)
        stat_copy(side, source, g).start()
        for p in groups[g]:
            mean_copy(side, source, p).start()

    def attend_own():
        mark("own")
        results = attend(me, range(pairs), keys, True)
        for p, mean, level in results:
            own_final[p] = mean
        for g, group in enumerate(groups):
            own_final_stat[g] = stack([results[p] for p in group])

    def decode():
        head_mask = lax.div(iota((heads, local), 1), width) == iota((heads, local), 0)
        chunk = 128
        chunks = span // chunk
        later = (iota((chunk, chunk), 0) > iota((chunk, chunk), 1)).astype(F32)
        c_sk.wait()
        c_sv.wait()
        c_sg.wait()
        c_sl.wait()
        step_att = jnp.zeros((pad, local), F32)
        for b in range(steps):
            length = step_len[0, b]
            in_cache = iota((heads, span), 1) < length
            kept = jnp.where(in_cache, step_gates[b], 0.0)
            tail = jnp.zeros((heads, 1), F32)
            parts = [None] * chunks
            for c in reversed(range(chunks)):
                piece = kept[:, c * chunk : (c + 1) * chunk]
                inner = jnp.dot(
                    piece, later, preferred_element_type=F32, precision=lax.Precision.HIGHEST
                )
                parts[c] = inner + tail
                tail = tail + jnp.sum(piece, axis=1, keepdims=True)
            after = jnp.concatenate(parts, axis=1)
            q_row = jnp.where(head_mask, step_q[b : b + 1], 0.0)
            scores = lax.dot_general(
                q_row.astype(BF16), sk_v[pl.ds(b * span, span)], NT, preferred_element_type=F32
            )
            new_lg = own_lg[:, rows + b : rows + b + 1]
            scores = scores * scale + (new_lg + after) * log2e
            scores = jnp.where(in_cache, scores, negative)
            self_score = jnp.sum(q_row * step_nk[b : b + 1], axis=1, keepdims=True) * scale
            high = jnp.maximum(jnp.max(scores, axis=1, keepdims=True), self_score)
            weight = jnp.exp2(scores - high)
            self_weight = jnp.exp2(self_score - high)
            mass = jnp.sum(weight, axis=1, keepdims=True) + self_weight
            mix = jnp.dot(
                weight.astype(BF16), sv_v[pl.ds(b * span, span)], preferred_element_type=F32
            )
            mix = mix + self_weight.astype(BF16).astype(F32) * step_nv[b : b + 1]
            one = jnp.sum(jnp.where(head_mask, mix / mass, 0.0), axis=0, keepdims=True)
            step_att = jnp.where(iota((pad, local), 0) == b, one, step_att)
        done = step_att.astype(BF16)
        for p in range(pairs):
            att[tp * pairs + p, pl.ds(rows, pad)] = done[:, p * pair_lanes : (p + 1) * pair_lanes]

    def in_order(i):
        return jnp.where(i == 1, 1, jnp.where(i == 2, n - 1, i - 1))

    @pl.when(jnp.logical_not(has_left))
    def _():
        finish_bias()

    @pl.when(edge)
    def _():
        def step(i, carry):
            k = in_order(i)
            for g in range(len(groups)):
                @pl.when(has_left)
                def _():
                    attend_edge(True, k, g)

                @pl.when(has_right)
                def _():
                    attend_edge(False, k, g)

            return carry

        lax.fori_loop(1, n, step, 0)

        @pl.when(has_left)
        def _():
            finish_bias()

        attend_own()
        mark("dec")
        decode()

    @pl.when(middle)
    def _():
        @pl.when(me == 1)
        def _():
            finish_bias()

        def step(k, carry):
            for g in range(len(groups)):
                attend_middle(True, k, g)

            @pl.when(both(k == 1, me > 1))
            def _():
                mark("bias")
                finish_bias()

            for g in range(len(groups)):
                attend_middle(False, k, g)

            @pl.when(k == 1)
            def _():
                attend_own()

            return carry

        lax.fori_loop(1, n, step, 0)
        mark("dec")
        decode()

    mark("loop")
    def forward(side, owner):
        means, stats = (to_r, stat_r) if side == 0 else (to_l, stat_l)
        for g, group in enumerate(groups):
            await_stat(stats, owner, owner, g)
            shares, level = shares_of([stats[owner, g], own_stat[owner, g]])
            stats[owner, g] = level
            stat_copy(side, owner, g).start()
            for i, p in enumerate(group):
                await_mean(means, owner, owner, p)
                mark("F")
                mean = blend(shares, [means[owner, p].astype(F32), own_mean[owner, p]], i)
                means[owner, p] = mean.astype(BF16)
                mean_copy(side, owner, p).start()

    def pass_right(r):
        due = both(has_left, r > me)
        if reach:
            due = both(due, jnp.logical_not(both(r == last, me == n - 2)))

        @pl.when(due)
        def _():
            if reach:
                @pl.when(both(r == last, me == n - 3))
                def _():
                    pl.semaphore_wait(far_sem, 1)

            forward(0, r)

    def pass_left(r):
        owner = n - 1 - r
        due = both(has_right, owner < me)
        if reach:
            due = both(due, jnp.logical_not(both(owner == first, me == 1)))

        @pl.when(due)
        def _():
            forward(1, owner)

    def turn(i, carry):
        r = jnp.where(i == 1, n - 1, i - 1)

        @pl.when(2 * me < n)
        def _():
            pass_right(r)
            pass_left(r)

        @pl.when(2 * me >= n)
        def _():
            pass_left(r)
            pass_right(r)

        return carry

    @pl.when(middle)
    def _():
        lax.fori_loop(1, n, turn, 0)

    def swap_copy(core, p):
        slot = core * pairs + p
        return pltpu.make_async_remote_copy(
            src_ref=att.at[slot], dst_ref=att.at[slot],
            send_sem=x_send, recv_sem=x_recv.at[p],
            device_id={"tp": 1 - tp}, device_id_type=MESH,
        )

    def finish(from_left, from_right, from_near):
        for g, group in enumerate(groups):
            levels = [own_final_stat[g]]
            if from_near:
                near_level(g).wait_recv()
                levels.append(near_stat[g])
            if from_left:
                await_stat(stat_r, me, me, g)
                levels.append(stat_r[me, g])
            if from_right:
                await_stat(stat_l, n, me, g)
                levels.append(stat_l[me, g])
            shares, _ = shares_of(levels)
            for i, p in enumerate(group):
                means = [own_final[p]]
                if from_near:
                    near_mean(p).wait_recv()
                    means.append(near[p].astype(F32))
                if from_left:
                    await_mean(to_r, me, me, p)
                    means.append(to_r[me, p].astype(F32))
                if from_right:
                    await_mean(to_l, n, me, p)
                    means.append(to_l[me, p].astype(F32))
                mark("fn")
                att[tp * pairs + p, pl.ds(0, rows)] = blend(shares, means, i).T.astype(BF16)
                swap_copy(tp, p).start()

    @pl.when(middle)
    def _():
        finish(True, True, False)

    @pl.when(both(has_left, jnp.logical_not(has_right)))
    def _():
        finish(True, False, reach)

    @pl.when(both(has_right, jnp.logical_not(has_left)))
    def _():
        finish(False, True, reach)

    mark("fin_sent")
    for p in range(pairs):
        swap_copy(1 - tp, p).wait_recv()
    mark("swapped")
    for i in range(2 * pairs):
        out_att[:, i * pair_lanes : (i + 1) * pair_lanes] = att[i]

    all_sent(att.at[pl.ds(tp * pairs, pairs)], x_send, x_recv.at[0])

    @pl.when(has_right)
    def _():
        g_copy.wait_send()

    if reach:
        @pl.when(edge)
        def _():
            all_sent(q_all.at[me], q_far, q_recv.at[me, 0])

        @pl.when(jnp.logical_or(me == 1, me == n - 2))
        def _():
            all_sent(near, m_send.at[n], m_recv.at[n, 0])
            all_sent(near_stat, s_send.at[n], s_recv.at[n, 0])

    def sent(owner, carry):
        right_sent = both(has_right, owner <= me)
        left_sent = both(has_left, owner >= me)
        part_right = both(has_right, owner > me)
        part_left = both(has_left, owner < me)
        if reach:
            right_sent = both(right_sent, jnp.logical_not(both(owner == first, me == n - 2)))
            left_sent = both(left_sent, jnp.logical_not(both(owner == last, me == 1)))
            part_right = both(part_right, jnp.logical_not(both(owner == last, me == n - 2)))
            part_left = both(part_left, jnp.logical_not(both(owner == first, me == 1)))

        @pl.when(right_sent)
        def _():
            all_sent(q_all.at[owner], q_right.at[owner], q_recv.at[owner, 0])

        @pl.when(left_sent)
        def _():
            all_sent(q_all.at[owner], q_left.at[owner], q_recv.at[owner, 0])

        @pl.when(part_right)
        def _():
            all_sent(to_r.at[owner], m_send.at[owner], m_recv.at[owner, 0])
            all_sent(stat_r.at[owner], s_send.at[owner], s_recv.at[owner, 0])

        @pl.when(part_left)
        def _():
            all_sent(to_l.at[owner], m_send.at[owner], m_recv.at[owner, 0])
            all_sent(stat_l.at[owner], s_send.at[owner], s_recv.at[owner, 0])

        return carry

    lax.fori_loop(0, n, sent, 0)
    mark("sent")


def project(rows, att, weight, out_piece, out_step):
    projected = jnp.dot(att[...], weight[...], preferred_element_type=F32)
    out_piece[...] = projected[:rows].astype(BF16)
    out_step[...] = projected[rows : rows + out_step.shape[0]].astype(BF16)


def per_device(
    piece_tokens, step_tokens, norm_gain, query_weight, key_weight, value_weight,
    gate_weight, gate_bias, out_weight, cache_keys, cache_values, cache_decay,
    decay_total, step_keys, step_values, step_gates, step_lengths,
):
    n = lax.axis_size("kv")
    rows, model = piece_tokens.shape
    steps = step_tokens.shape[0]
    heads = cache_decay.shape[0]
    local = query_weight.shape[1]
    width = local // heads
    pairs = heads // 2
    groups = pairs // 2 if pairs % 2 == 0 else pairs
    cache_len = cache_keys.shape[0]
    keys = cache_len + rows
    span = step_keys.shape[1]
    columns = out_weight.shape[1]
    padded = rows + 16 * (-(-steps // 16))
    all_heads = gate_weight.shape[1]
    vmem = pl.BlockSpec(memory_space=pltpu.VMEM)
    hbm = pl.BlockSpec(memory_space=pltpu.HBM)
    dma = pltpu.SemaphoreType.DMA
    att = pl.pallas_call(
        functools.partial(kernel, n, heads, width),
        out_shape=pltpu.VMEM((padded, out_weight.shape[0]), BF16),
        in_specs=[hbm] * 16,
        out_specs=vmem,
        scratch_shapes=[
            pltpu.VMEM((rows, model), BF16),
            pltpu.VMEM((steps, model), BF16),
            pltpu.VMEM((1, model), F32),
            pltpu.VMEM((all_heads, model), BF16),
            pltpu.VMEM((1, all_heads), F32),
            pltpu.VMEM((1, all_heads), F32),
            pltpu.VMEM(cache_decay.shape, F32),
            pltpu.VMEM(step_gates.shape, F32),
            pltpu.SMEM((1, steps), jnp.int32),
            pltpu.VMEM((padded, model), BF16),
            pltpu.VMEM(query_weight.shape, BF16),
            pltpu.VMEM(key_weight.shape, BF16),
            pltpu.VMEM(value_weight.shape, BF16),
            pltpu.VMEM((keys, local), BF16),
            pltpu.VMEM((cache_len, local), BF16),
            pltpu.VMEM((local, keys), BF16),
            pltpu.VMEM((steps * span, local), BF16),
            pltpu.VMEM((steps * span, local), BF16),
            pltpu.VMEM((n, pairs, 2 * width, rows), BF16),
            pltpu.VMEM((all_heads, padded), F32),
            pltpu.VMEM((heads, 128), F32),
            pltpu.VMEM((heads, 128), F32),
            pltpu.VMEM((heads, rows), F32),
            pltpu.VMEM((keys, 128), BF16),
            pltpu.VMEM((pairs, 128, 2 * rows), BF16),
            pltpu.VMEM((n, pairs, 2 * width, rows), F32),
            pltpu.VMEM((n, groups, heads // groups, rows), F32),
            pltpu.VMEM((n, pairs, 2 * width, rows), BF16),
            pltpu.VMEM((n, pairs, 2 * width, rows), BF16),
            pltpu.VMEM((n, groups, heads // groups, rows), F32),
            pltpu.VMEM((n, groups, heads // groups, rows), F32),
            pltpu.VMEM((pairs, 2 * width, rows), BF16),
            pltpu.VMEM((groups, heads // groups, rows), F32),
            pltpu.VMEM((pairs, 2 * width, rows), F32),
            pltpu.VMEM((groups, heads // groups, rows), F32),
            pltpu.VMEM((2 * pairs, padded, 2 * width), BF16),
            dma((17,)),
            dma((n,)), dma((n,)), dma(()), dma((n, pairs)),
            dma(()), dma(()), pltpu.SemaphoreType.REGULAR,
            dma((n + 1,)), dma((n + 2, pairs)), dma((n + 1,)), dma((n + 2, groups)),
            dma(()), dma((pairs,)),
        ],
        compiler_params=pltpu.CompilerParams(
            collective_id=0, has_side_effects=True, vmem_limit_bytes=56 * 1024 * 1024
        ),
    )(
        piece_tokens, step_tokens, norm_gain.reshape(1, -1), gate_weight.T,
        gate_bias.reshape(1, -1), decay_total.reshape(1, -1), cache_decay, step_gates,
        step_lengths.reshape(1, -1), query_weight, key_weight, value_weight,
        cache_keys, cache_values,
        step_keys.reshape(steps * span, local), step_values.reshape(steps * span, local),
    )
    return pl.pallas_call(
        functools.partial(project, rows),
        out_shape=(
            jax.ShapeDtypeStruct((rows, columns), BF16),
            jax.ShapeDtypeStruct((steps, columns), BF16),
        ),
        in_specs=[vmem, vmem],
        out_specs=(vmem, vmem),
        compiler_params=pltpu.CompilerParams(vmem_limit_bytes=16 * 1024 * 1024),
    )(att, out_weight)


def solution(mesh):
    rows = P(("dp", "kv"), None)
    both = P(("dp", "kv"), "tp")
    cols = P(None, "tp")
    in_specs = (
        rows, rows, P(), cols, cols, cols, P(), P(), cols, both, both,
        P("tp", ("dp", "kv")), P("dp"),
        P(("dp", "kv"), None, "tp"), P(("dp", "kv"), None, "tp"),
        P(("dp", "kv"), "tp", None), P(("dp", "kv")),
    )
    return jax.shard_map(
        per_device, mesh=mesh, in_specs=in_specs, out_specs=(both, both), check_vma=False
    )
```

```python
import functools
import math

import jax
import jax.numpy as jnp
from jax import lax
from jax.experimental import pallas as pl
from jax.experimental.pallas import tpu as pltpu
from jax.sharding import PartitionSpec as P

norm_eps = 1e-06
negative = -1e30
log2e = math.log2(math.e)
MESH = pl.DeviceIdType.MESH
F32 = jnp.float32
BF16 = jnp.bfloat16
NT = (((1,), (1,)), ((), ()))


def fence():
    pl.delay(1)


def iota(shape, dim):
    return lax.broadcasted_iota(jnp.int32, shape, dim)


def normalize(rows, gain):
    wide = rows.astype(F32)
    factor = lax.rsqrt(jnp.mean(wide * wide, axis=-1, keepdims=True) + norm_eps)
    return (wide * factor * gain).astype(BF16)


def to_column(row, count):
    eye = iota((count, count), 0) == iota((count, count), 1)
    return jnp.sum(jnp.where(eye, row, 0.0), axis=1, keepdims=True)


def kernel(
    n, heads, width,
    tok_h, stok_h, gain_h, gate_w_h, gate_b_h, total_h, cache_decay_h, step_gates_h, step_len_h,
    wq, wk, wv, cache_k, cache_v, step_k, step_v,
    out_att,
    tok, stok, gain, gate_w, gate_b, total_decay, cache_decay, step_gates, step_len,
    nrm, wq_v, wk_v, wv_v, k_all, cv_v, v_turned, sk_v, sv_v,
    q_all, lg, gate_in, gate_out, bias_rows, bias_lanes, picks,
    own_mean, own_stat, to_r, to_l, stat_r, stat_l, near, near_stat, own_final, own_final_stat, att,
    local_sem, q_right, q_left, q_far, q_recv, g_send, g_recv, far_sem,
    m_send, m_recv, s_send, s_recv, x_send, x_recv,
):
    me = lax.axis_index("kv")
    tp = lax.axis_index("tp")
    rows = tok.shape[0]
    steps = stok.shape[0]
    cache_len = cache_k.shape[0]
    span = step_k.shape[0] // steps
    local = heads * width
    pair_lanes = 2 * width
    pairs = heads // 2
    keys = cache_len + rows
    root = math.sqrt(width)
    scale = log2e / root

    count = [0]

    def fetch(src, dst):
        copy = pltpu.make_async_copy(src, dst, local_sem.at[count[0]])
        count[0] += 1
        copy.start()
        return copy

    halves = 2 if local % 256 == 0 else 1
    part = local // halves
    c_tok = fetch(tok_h, tok)
    c_gain = fetch(gain_h, gain)
    c_stok = fetch(stok_h, stok)
    c_wq = [
        fetch(wq.at[:, pl.ds(c * part, part)], wq_v.at[:, pl.ds(c * part, part)])
        for c in range(halves)
    ]

    has_right = me < n - 1
    has_left = me > 0
    right = lax.rem(me + 1, n)
    left = lax.rem(me + n - 1, n)

    reach = n == 4
    first, last = 0, n - 1
    middle = jnp.logical_and(has_left, has_right)
    edge = jnp.logical_not(middle)

    def both(a, b):
        return jnp.logical_and(a, b)

    def as_count(flag):
        return flag.astype(jnp.int32)

    barrier = pltpu.get_barrier_semaphore()

    def hello(condition, target):
        @pl.when(condition)
        def _():
            pl.semaphore_signal(barrier, inc=1, device_id={"kv": target}, device_id_type=MESH)

    hello(has_right, right)
    hello(has_left, left)
    pl.semaphore_signal(barrier, inc=1, device_id={"tp": 1 - tp}, device_id_type=MESH)
    greeted = 1 + as_count(has_right) + as_count(has_left)
    if reach:
        hello(me == first, 2)
        hello(me == 2, first)
        hello(me == n - 3, last)
        for each in (first, 2, last):
            greeted = greeted + as_count(me == each)

    def enter():
        pl.semaphore_wait(barrier, greeted)
        if reach:
            @pl.when(me == last)
            def _():
                pl.semaphore_signal(far_sem, inc=1, device_id={"kv": n - 3}, device_id_type=MESH)

    def q_copy(source, p, sem, target):
        return pltpu.make_async_remote_copy(
            src_ref=q_all.at[source, p], dst_ref=q_all.at[source, p],
            send_sem=sem, recv_sem=q_recv.at[source, p],
            device_id={"kv": target}, device_id_type=MESH,
        )

    def q_to_right(source, p):
        return q_copy(source, p, q_right.at[source], right)

    def q_to_left(source, p):
        return q_copy(source, p, q_left.at[source], left)

    def q_to_far(p):
        return q_copy(me, p, q_far, jnp.where(me == first, 2, n - 3))

    size = 2 if pairs % 2 == 0 else 1
    groups = [range(g, g + size) for g in range(0, pairs, size)]

    def part_target(side, owner):
        if side == 0:
            straight = both(owner == last, me == n - 3)
            return jnp.where(straight, last, right) if reach else right
        straight = both(owner == first, me == 2)
        return jnp.where(straight, first, left) if reach else left

    def part_slot(side, owner, target):
        return owner if side == 0 else jnp.where(owner == target, n, owner)

    def mean_copy(side, owner, p):
        means = to_r if side == 0 else to_l
        target = part_target(side, owner)
        return pltpu.make_async_remote_copy(
            src_ref=means.at[owner, p], dst_ref=means.at[owner, p],
            send_sem=m_send.at[owner], recv_sem=m_recv.at[part_slot(side, owner, target), p],
            device_id={"kv": target}, device_id_type=MESH,
        )

    def stat_copy(side, owner, g):
        stats = stat_r if side == 0 else stat_l
        target = part_target(side, owner)
        return pltpu.make_async_remote_copy(
            src_ref=stats.at[owner, g], dst_ref=stats.at[owner, g],
            send_sem=s_send.at[owner], recv_sem=s_recv.at[part_slot(side, owner, target), g],
            device_id={"kv": target}, device_id_type=MESH,
        )

    def near_mean(p):
        return pltpu.make_async_remote_copy(
            src_ref=near.at[p], dst_ref=near.at[p],
            send_sem=m_send.at[n], recv_sem=m_recv.at[n + 1, p],
            device_id={"kv": jnp.where(me == 1, first, last)}, device_id_type=MESH,
        )

    def near_level(g):
        return pltpu.make_async_remote_copy(
            src_ref=near_stat.at[g], dst_ref=near_stat.at[g],
            send_sem=s_send.at[n], recv_sem=s_recv.at[n + 1, g],
            device_id={"kv": jnp.where(me == 1, first, last)}, device_id_type=MESH,
        )

    def await_mean(means, slot, owner, p):
        pltpu.make_async_remote_copy(
            src_ref=means.at[owner, p], dst_ref=means.at[owner, p],
            send_sem=m_send.at[owner], recv_sem=m_recv.at[slot, p],
            device_id={"tp": 1 - tp}, device_id_type=MESH,
        ).wait_recv()

    def await_stat(stats, slot, owner, g):
        pltpu.make_async_remote_copy(
            src_ref=stats.at[owner, g], dst_ref=stats.at[owner, g],
            send_sem=s_send.at[owner], recv_sem=s_recv.at[slot, g],
            device_id={"tp": 1 - tp}, device_id_type=MESH,
        ).wait_recv()

    def all_sent(ref, sem, recv):
        pltpu.make_async_remote_copy(
            src_ref=ref, dst_ref=ref, send_sem=sem, recv_sem=recv,
            device_id={"tp": 1 - tp}, device_id_type=MESH,
        ).wait_send()

    c_tok.wait()
    c_gain.wait()
    c_stok.wait()
    c_gw = fetch(gate_w_h, gate_w)
    c_gb = fetch(gate_b_h, gate_b)
    c_wk = fetch(wk, wk_v)
    c_wv = fetch(wv, wv_v)
    c_cv = fetch(cache_v, cv_v)
    c_ck = fetch(cache_k, k_all.at[pl.ds(0, cache_len)])
    c_td = fetch(total_h, total_decay)
    c_cd = fetch(cache_decay_h, cache_decay)
    c_sk = fetch(step_k, sk_v)
    c_sv = fetch(step_v, sv_v)
    c_sg = fetch(step_gates_h, step_gates)
    c_sl = fetch(step_len_h, step_len)
    nrm[pl.ds(0, rows)] = normalize(tok[...], gain[...])
    pad = nrm.shape[0] - rows
    step_norm = normalize(stok[...], gain[...]).astype(F32)
    step_rows = jnp.zeros((pad, nrm.shape[1]), F32)
    for b in range(steps):
        step_rows = jnp.where(iota((pad, nrm.shape[1]), 0) == b, step_norm[b : b + 1], step_rows)
    nrm[pl.ds(rows, pad)] = step_rows.astype(BF16)

    def send_queries(which):
        for p in which:
            @pl.when(has_right)
            def _():
                q_to_right(me, p).start()

            @pl.when(has_left)
            def _():
                q_to_left(me, p).start()

    pairs_in_part = part // pair_lanes
    step_q_parts = []
    for c in range(halves):
        c_wq[c].wait()
        q_new = jnp.dot(
            nrm[...], wq_v[:, c * part : (c + 1) * part], preferred_element_type=F32
        ).astype(BF16)
        turned = q_new[:rows].T
        for i in range(pairs_in_part):
            q_all[me, c * pairs_in_part + i] = turned[i * pair_lanes : (i + 1) * pair_lanes]
        step_q_parts.append(q_new[rows:].astype(F32))

        chunk = range(c * pairs_in_part, (c + 1) * pairs_in_part)

        @pl.when(has_left)
        def _():
            if c == 0:
                enter()
            if reach:
                @pl.when(has_right)
                def _():
                    send_queries(chunk)

                @pl.when(jnp.logical_not(has_right))
                def _():
                    for p in chunk:
                        q_to_far(p).start()
            else:
                send_queries(chunk)

    if reach:
        @pl.when(jnp.logical_not(has_right))
        def _():
            send_queries(range(pairs))

    step_q = jnp.concatenate(step_q_parts, axis=1)

    c_gw.wait()
    c_gb.wait()
    logits = lax.dot_general(gate_w[...], nrm[...], NT, preferred_element_type=F32)
    logits = logits + to_column(gate_b[...], gate_w.shape[0])
    lg[...] = jnp.minimum(logits, 0.0) - jnp.log1p(jnp.exp(-jnp.abs(logits)))
    own_lg = lg[pl.ds(pl.multiple_of(tp * heads, heads), heads), :]
    piece_lg = own_lg[:, :rows]
    own_sum = jnp.broadcast_to(jnp.sum(piece_lg, axis=1, keepdims=True), gate_out.shape)

    g_copy = pltpu.make_async_remote_copy(
        src_ref=gate_out, dst_ref=gate_in, send_sem=g_send, recv_sem=g_recv,
        device_id={"kv": right}, device_id_type=MESH,
    )

    @pl.when(jnp.logical_not(has_left))
    def _():
        gate_in[...] = jnp.zeros(gate_in.shape, F32)
        gate_out[...] = own_sum

        enter()

        @pl.when(has_right)
        def _():
            g_copy.start()

        if reach:
            for p in range(pairs):
                q_to_far(p).start()
        send_queries(range(pairs))

    c_wk.wait()
    c_wv.wait()
    c_cv.wait()
    c_td.wait()
    c_cd.wait()
    c_ck.wait()
    k_new = jnp.dot(nrm[...], wk_v[...], preferred_element_type=F32).astype(BF16)
    k_all[pl.ds(cache_len, rows)] = k_new[:rows]
    step_nk = k_new[rows:].astype(F32)
    v_new = jnp.dot(nrm[...], wv_v[...], preferred_element_type=F32).astype(BF16)
    v_turned[:, pl.ds(cache_len, rows)] = v_new[:rows].T
    step_nv = v_new[rows:].astype(F32)
    v_turned[:, pl.ds(0, cache_len)] = cv_v[...].T

    upto = (iota((rows, rows), 0) <= iota((rows, rows), 1)).astype(F32)
    running = jnp.dot(
        piece_lg, upto, preferred_element_type=F32, precision=lax.Precision.HIGHEST
    )

    def bias_terms(bias):
        high = bias.astype(BF16).astype(F32)
        rest = bias - high
        middle = rest.astype(BF16).astype(F32)
        low = rest - middle
        blank = jnp.zeros((128 - 3 * heads, bias.shape[1]), F32)
        return jnp.concatenate([high, middle, low, blank], axis=0).T.astype(BF16)

    lg_start = to_column(total_decay[...], gate_w.shape[0])
    start_rows = jnp.where(tp == 0, lg_start[:heads], lg_start[heads : 2 * heads])
    bias_lanes[pl.ds(0, cache_len)] = bias_terms((start_rows - cache_decay[...]) * root)
    bias_rows[...] = running

    head_of_column = lax.div(iota((128, 2 * rows), 1), rows)
    lane_of_term = iota((128, 2 * rows), 0)
    for p in range(pairs):
        hit = jnp.logical_and(
            lax.rem(lane_of_term, heads) == 2 * p + head_of_column, lane_of_term < 3 * heads
        )
        picks[p] = hit.astype(F32).astype(BF16)

    def pass_prefix():
        @pl.when(has_left)
        def _():
            g_copy.wait_recv()

            @pl.when(has_right)
            def _():
                gate_out[...] = gate_in[...] + own_sum
                g_copy.start()

    def finish_bias():
        fresh = -(gate_in[:, :1] + bias_rows[...]) * root
        bias_lanes[pl.ds(cache_len, rows)] = bias_terms(fresh)

    first_rows = iota((pair_lanes, rows), 0) < width
    causal = lax.rem(iota((rows, 2 * rows), 1), rows) >= iota((rows, 2 * rows), 0)

    def spread(two):
        return jnp.concatenate(
            [
                jnp.broadcast_to(two[0:1], (width, rows)),
                jnp.broadcast_to(two[1:2], (width, rows)),
            ],
            axis=0,
        )

    def scores_of(source, p, used):
        q_pair = q_all[source, p]
        zero = jnp.zeros_like(q_pair)
        rhs = jnp.concatenate(
            [
                jnp.concatenate(
                    [jnp.where(first_rows, q_pair, zero), jnp.where(first_rows, zero, q_pair)],
                    axis=1,
                ),
                picks[p],
            ],
            axis=0,
        )
        lhs = jnp.concatenate([k_all[pl.ds(0, used), lanes_of(p)], bias_lanes[pl.ds(0, used)]], axis=1)
        return jnp.dot(lhs, rhs, preferred_element_type=F32)

    def lanes_of(p):
        return pl.ds(pl.multiple_of(p * pair_lanes, pair_lanes), pair_lanes)

    def weigh(raw):
        high = jnp.max(raw, axis=0, keepdims=True)
        weight = jnp.exp2((raw - high) * scale)
        mass = jnp.sum(weight, axis=0, keepdims=True)
        return weight.astype(BF16), mass, high * scale + jnp.log2(mass)

    def attend(source, group, used, masked):
        raws = [scores_of(source, p, used) for p in group]
        if masked:
            raws = [
                jnp.concatenate(
                    [raw[:cache_len], jnp.where(causal, raw[cache_len:], negative)], axis=0
                )
                for raw in raws
            ]
        weighed = [weigh(raw) for raw in raws]
        results = []
        for p, (weight, mass, level) in zip(group, weighed):
            values = v_turned[lanes_of(p), pl.ds(0, used)]
            mix = jnp.dot(values, weight, preferred_element_type=F32) * (1.0 / mass)
            mean = jnp.concatenate([mix[:width, :rows], mix[width:, rows:]], axis=0)
            levels = jnp.concatenate([level[:, :rows], level[:, rows:]], axis=0)
            results.append((p, mean, levels))
        return results

    def shares_of(levels):
        best = functools.reduce(jnp.maximum, levels)
        shares = [jnp.exp2(level - best) for level in levels]
        total = functools.reduce(jnp.add, shares)
        inverse = 1.0 / total
        return [share * inverse for share in shares], best + jnp.log2(total)

    def blend(shares, means, i):
        return functools.reduce(
            jnp.add,
            [spread(share[2 * i : 2 * i + 2]) * mean for share, mean in zip(shares, means)],
        )

    def stack(results):
        return jnp.concatenate([level for _, _, level in results], axis=0)

    def in_group(g):
        return [g * size + i for i in range(size)]

    def arrived(from_left, k, g):
        for p in in_group(g):
            if from_left:
                q_to_right(me - k, p).wait_recv()
            else:
                q_to_left(me + k, p).wait_recv()

    def relay(from_left, k, g):
        for p in in_group(g):
            if from_left:
                q_to_right(me - k, p).start()
            else:
                q_to_left(me + k, p).start()

    def attend_keep(from_left, k, g):
        source, used = (me - k, cache_len) if from_left else (me + k, keys)
        fence()
        results = attend(source, in_group(g), used, False)
        for p, mean, level in results:
            own_mean[source, p] = mean
        own_stat[source, g] = stack(results)

    def attend_near(from_left, g):
        source, used = (me - 1, cache_len) if from_left else (me + 1, keys)
        fence()
        results = attend(source, in_group(g), used, False)
        for p, mean, level in results:
            near[p] = mean.astype(BF16)
        near_stat[g] = stack(results)
        near_level(g).start()
        for p, _, _ in results:
            near_mean(p).start()

    def attend_edge(from_left, k, g):
        source, used, side = (me - k, cache_len, 1) if from_left else (me + k, keys, 0)
        means, stats = (to_l, stat_l) if from_left else (to_r, stat_r)
        arrived(from_left, k, g)
        fence()
        results = attend(source, in_group(g), used, False)
        for p, mean, level in results:
            means[source, p] = mean.astype(BF16)
        stats[source, g] = stack(results)
        stat_copy(side, source, g).start()
        for p in in_group(g):
            mean_copy(side, source, p).start()

    def attend_own():
        fence()
        results = attend(me, range(pairs), keys, True)
        for p, mean, level in results:
            own_final[p] = mean
        for g, group in enumerate(groups):
            own_final_stat[g] = stack([results[p] for p in group])

    def decode():
        head_mask = lax.div(iota((heads, local), 1), width) == iota((heads, local), 0)
        chunk = 128
        chunks = span // chunk
        later = (iota((chunk, chunk), 0) > iota((chunk, chunk), 1)).astype(F32)
        c_sk.wait()
        c_sv.wait()
        c_sg.wait()
        c_sl.wait()
        step_att = jnp.zeros((pad, local), F32)
        for b in range(steps):
            length = step_len[0, b]
            in_cache = iota((heads, span), 1) < length
            kept = jnp.where(in_cache, step_gates[b], 0.0)
            tail = jnp.zeros((heads, 1), F32)
            parts = [None] * chunks
            for c in reversed(range(chunks)):
                piece = kept[:, c * chunk : (c + 1) * chunk]
                inner = jnp.dot(
                    piece, later, preferred_element_type=F32, precision=lax.Precision.HIGHEST
                )
                parts[c] = inner + tail
                tail = tail + jnp.sum(piece, axis=1, keepdims=True)
            after = jnp.concatenate(parts, axis=1)
            q_row = jnp.where(head_mask, step_q[b : b + 1], 0.0)
            scores = lax.dot_general(
                q_row.astype(BF16), sk_v[pl.ds(b * span, span)], NT, preferred_element_type=F32
            )
            new_lg = own_lg[:, rows + b : rows + b + 1]
            scores = scores * scale + (new_lg + after) * log2e
            scores = jnp.where(in_cache, scores, negative)
            self_score = jnp.sum(q_row * step_nk[b : b + 1], axis=1, keepdims=True) * scale
            high = jnp.maximum(jnp.max(scores, axis=1, keepdims=True), self_score)
            weight = jnp.exp2(scores - high)
            self_weight = jnp.exp2(self_score - high)
            mass = jnp.sum(weight, axis=1, keepdims=True) + self_weight
            mix = jnp.dot(
                weight.astype(BF16), sv_v[pl.ds(b * span, span)], preferred_element_type=F32
            )
            mix = mix + self_weight.astype(BF16).astype(F32) * step_nv[b : b + 1]
            one = jnp.sum(jnp.where(head_mask, mix / mass, 0.0), axis=0, keepdims=True)
            step_att = jnp.where(iota((pad, local), 0) == b, one, step_att)
        done = step_att.astype(BF16)
        for p in range(pairs):
            att[tp * pairs + p, pl.ds(rows, pad)] = done[:, p * pair_lanes : (p + 1) * pair_lanes]

    parts = len(groups)

    def each_group(make):
        def body(g, carry):
            make(g)
            return carry

        lax.fori_loop(0, parts, body, 0)

    @pl.when(jnp.logical_not(has_left))
    def _():
        pass_prefix()
        finish_bias()

    @pl.when(edge)
    def _():
        def step(i, carry):
            k = jnp.where(i == 1, 1, jnp.where(i == 2, n - 1, i - 1)) if reach else i

            @pl.when(has_left)
            def _():
                each_group(lambda g: attend_edge(True, k, g))

            @pl.when(has_right)
            def _():
                each_group(lambda g: attend_edge(False, k, g))

            @pl.when(i == 1)
            def _():
                fence()
                decode()

            @pl.when(i == max(1, n - 2))
            def _():
                @pl.when(has_left)
                def _():
                    pass_prefix()
                    finish_bias()

                attend_own()

            return carry

        lax.fori_loop(1, n, step, 0)

    if reach:
        @pl.when(me == n - 3)
        def _():
            pass_prefix()
            finish_bias()

            def turn_one(i, carry):
                k = 2 - i

                def body(g):
                    arrived(False, k, g)
                    relay(False, k, g)
                    attend_keep(False, k, g)

                each_group(body)
                return carry

            lax.fori_loop(0, 2, turn_one, 0)

            def body(g):
                arrived(True, 1, g)
                attend_near(True, g)

            each_group(body)

        @pl.when(me == 2)
        def _():
            def turn_two(i, carry):
                k = 2 - i

                def body(g):
                    arrived(True, k, g)
                    relay(True, k, g)
                    attend_keep(True, k, g)

                    @pl.when(both(i == 0, g == 0))
                    def _():
                        pass_prefix()

                each_group(body)
                return carry

            lax.fori_loop(0, 2, turn_two, 0)
            finish_bias()

            def body(g):
                arrived(False, 1, g)
                attend_near(False, g)

            each_group(body)
    else:
        @pl.when(middle)
        def _():
            pass_prefix()
            finish_bias()

            def step(k, carry):
                for from_left, there in ((True, me >= k), (False, me + k < n)):
                    @pl.when(there)
                    def _():
                        def body(g):
                            arrived(from_left, k, g)
                            relay(from_left, k, g)

                        each_group(body)

                for from_left, there in ((True, me >= k), (False, me + k < n)):
                    @pl.when(there)
                    def _():
                        each_group(lambda g: attend_keep(from_left, k, g))

                return carry

            lax.fori_loop(1, n, step, 0)

    @pl.when(middle)
    def _():
        attend_own()
        fence()
        decode()

    def forward(side, owner):
        means, stats = (to_r, stat_r) if side == 0 else (to_l, stat_l)
        for g, group in enumerate(groups):
            await_stat(stats, owner, owner, g)
            shares, level = shares_of([stats[owner, g], own_stat[owner, g]])
            stats[owner, g] = level
            stat_copy(side, owner, g).start()
            for i, p in enumerate(group):
                await_mean(means, owner, owner, p)
                mean = blend(shares, [means[owner, p].astype(F32), own_mean[owner, p]], i)
                means[owner, p] = mean.astype(BF16)
                mean_copy(side, owner, p).start()

    if reach:
        @pl.when(me == n - 3)
        def _():
            pl.semaphore_wait(far_sem, 1)
            forward(0, last)
            forward(0, 2)

        @pl.when(me == 2)
        def _():
            forward(1, first)
            forward(1, n - 3)
    else:
        def pass_right(r):
            @pl.when(both(has_left, r > me))
            def _():
                forward(0, r)

        def pass_left(r):
            @pl.when(both(has_right, n - 1 - r < me))
            def _():
                forward(1, n - 1 - r)

        def turn(r, carry):
            @pl.when(2 * me < n)
            def _():
                pass_right(r)
                pass_left(r)

            @pl.when(2 * me >= n)
            def _():
                pass_left(r)
                pass_right(r)

            return carry

        @pl.when(middle)
        def _():
            lax.fori_loop(1, n, turn, 0)

    def swap_copy(core, p):
        slot = core * pairs + p
        return pltpu.make_async_remote_copy(
            src_ref=att.at[slot], dst_ref=att.at[slot],
            send_sem=x_send, recv_sem=x_recv.at[p],
            device_id={"tp": 1 - tp}, device_id_type=MESH,
        )

    def finish(from_left, from_right, from_near):
        for g, group in enumerate(groups):
            levels = [own_final_stat[g]]
            if from_near:
                near_level(g).wait_recv()
                levels.append(near_stat[g])
            if from_left:
                await_stat(stat_r, me, me, g)
                levels.append(stat_r[me, g])
            if from_right:
                await_stat(stat_l, n, me, g)
                levels.append(stat_l[me, g])
            shares, _ = shares_of(levels)
            for i, p in enumerate(group):
                means = [own_final[p]]
                if from_near:
                    near_mean(p).wait_recv()
                    means.append(near[p].astype(F32))
                if from_left:
                    await_mean(to_r, me, me, p)
                    means.append(to_r[me, p].astype(F32))
                if from_right:
                    await_mean(to_l, n, me, p)
                    means.append(to_l[me, p].astype(F32))
                att[tp * pairs + p, pl.ds(0, rows)] = blend(shares, means, i).T.astype(BF16)
                swap_copy(tp, p).start()

    @pl.when(middle)
    def _():
        finish(True, True, False)

    @pl.when(both(has_left, jnp.logical_not(has_right)))
    def _():
        finish(True, False, reach)

    @pl.when(both(has_right, jnp.logical_not(has_left)))
    def _():
        finish(False, True, reach)

    for p in range(pairs):
        swap_copy(1 - tp, p).wait_recv()
    for i in range(2 * pairs):
        out_att[:, i * pair_lanes : (i + 1) * pair_lanes] = att[i]

    all_sent(att.at[pl.ds(tp * pairs, pairs)], x_send, x_recv.at[0])

    @pl.when(has_right)
    def _():
        g_copy.wait_send()

    if reach:
        @pl.when(edge)
        def _():
            all_sent(q_all.at[me], q_far, q_recv.at[me, 0])

        @pl.when(jnp.logical_or(me == 1, me == n - 2))
        def _():
            all_sent(near, m_send.at[n], m_recv.at[n, 0])
            all_sent(near_stat, s_send.at[n], s_recv.at[n, 0])

    def sent(owner, carry):
        right_sent = both(has_right, owner <= me)
        left_sent = both(has_left, owner >= me)
        part_right = both(has_right, owner > me)
        part_left = both(has_left, owner < me)
        if reach:
            right_sent = both(right_sent, jnp.logical_not(both(owner == first, me == 1)))
            left_sent = both(left_sent, jnp.logical_not(both(owner == last, me == n - 2)))
            part_right = both(part_right, jnp.logical_not(both(owner == last, me == n - 2)))
            part_left = both(part_left, jnp.logical_not(both(owner == first, me == 1)))

        @pl.when(right_sent)
        def _():
            all_sent(q_all.at[owner], q_right.at[owner], q_recv.at[owner, 0])

        @pl.when(left_sent)
        def _():
            all_sent(q_all.at[owner], q_left.at[owner], q_recv.at[owner, 0])

        @pl.when(part_right)
        def _():
            all_sent(to_r.at[owner], m_send.at[owner], m_recv.at[owner, 0])
            all_sent(stat_r.at[owner], s_send.at[owner], s_recv.at[owner, 0])

        @pl.when(part_left)
        def _():
            all_sent(to_l.at[owner], m_send.at[owner], m_recv.at[owner, 0])
            all_sent(stat_l.at[owner], s_send.at[owner], s_recv.at[owner, 0])

        return carry

    lax.fori_loop(0, n, sent, 0)


def project(rows, att, weight, out_piece, out_step):
    projected = jnp.dot(att[...], weight[...], preferred_element_type=F32)
    out_piece[...] = projected[:rows].astype(BF16)
    out_step[...] = projected[rows : rows + out_step.shape[0]].astype(BF16)


def per_device(
    piece_tokens, step_tokens, norm_gain, query_weight, key_weight, value_weight,
    gate_weight, gate_bias, out_weight, cache_keys, cache_values, cache_decay,
    decay_total, step_keys, step_values, step_gates, step_lengths,
):
    n = lax.axis_size("kv")
    rows, model = piece_tokens.shape
    steps = step_tokens.shape[0]
    heads = cache_decay.shape[0]
    local = query_weight.shape[1]
    width = local // heads
    pairs = heads // 2
    groups = pairs // 2 if pairs % 2 == 0 else pairs
    cache_len = cache_keys.shape[0]
    keys = cache_len + rows
    span = step_keys.shape[1]
    columns = out_weight.shape[1]
    padded = rows + 16 * (-(-steps // 16))
    all_heads = gate_weight.shape[1]
    vmem = pl.BlockSpec(memory_space=pltpu.VMEM)
    hbm = pl.BlockSpec(memory_space=pltpu.HBM)
    dma = pltpu.SemaphoreType.DMA
    att = pl.pallas_call(
        functools.partial(kernel, n, heads, width),
        out_shape=pltpu.VMEM((padded, out_weight.shape[0]), BF16),
        in_specs=[hbm] * 16,
        out_specs=vmem,
        scratch_shapes=[
            pltpu.VMEM((rows, model), BF16),
            pltpu.VMEM((steps, model), BF16),
            pltpu.VMEM((1, model), F32),
            pltpu.VMEM((all_heads, model), BF16),
            pltpu.VMEM((1, all_heads), F32),
            pltpu.VMEM((1, all_heads), F32),
            pltpu.VMEM(cache_decay.shape, F32),
            pltpu.VMEM(step_gates.shape, F32),
            pltpu.SMEM((1, steps), jnp.int32),
            pltpu.VMEM((padded, model), BF16),
            pltpu.VMEM(query_weight.shape, BF16),
            pltpu.VMEM(key_weight.shape, BF16),
            pltpu.VMEM(value_weight.shape, BF16),
            pltpu.VMEM((keys, local), BF16),
            pltpu.VMEM((cache_len, local), BF16),
            pltpu.VMEM((local, keys), BF16),
            pltpu.VMEM((steps * span, local), BF16),
            pltpu.VMEM((steps * span, local), BF16),
            pltpu.VMEM((n, pairs, 2 * width, rows), BF16),
            pltpu.VMEM((all_heads, padded), F32),
            pltpu.VMEM((heads, 128), F32),
            pltpu.VMEM((heads, 128), F32),
            pltpu.VMEM((heads, rows), F32),
            pltpu.VMEM((keys, 128), BF16),
            pltpu.VMEM((pairs, 128, 2 * rows), BF16),
            pltpu.VMEM((n, pairs, 2 * width, rows), F32),
            pltpu.VMEM((n, groups, heads // groups, rows), F32),
            pltpu.VMEM((n, pairs, 2 * width, rows), BF16),
            pltpu.VMEM((n, pairs, 2 * width, rows), BF16),
            pltpu.VMEM((n, groups, heads // groups, rows), F32),
            pltpu.VMEM((n, groups, heads // groups, rows), F32),
            pltpu.VMEM((pairs, 2 * width, rows), BF16),
            pltpu.VMEM((groups, heads // groups, rows), F32),
            pltpu.VMEM((pairs, 2 * width, rows), F32),
            pltpu.VMEM((groups, heads // groups, rows), F32),
            pltpu.VMEM((2 * pairs, padded, 2 * width), BF16),
            dma((17,)),
            dma((n,)), dma((n,)), dma(()), dma((n, pairs)),
            dma(()), dma(()), pltpu.SemaphoreType.REGULAR,
            dma((n + 1,)), dma((n + 2, pairs)), dma((n + 1,)), dma((n + 2, groups)),
            dma(()), dma((pairs,)),
        ],
        compiler_params=pltpu.CompilerParams(
            collective_id=0, has_side_effects=True, vmem_limit_bytes=56 * 1024 * 1024
        ),
    )(
        piece_tokens, step_tokens, norm_gain.reshape(1, -1), gate_weight.T,
        gate_bias.reshape(1, -1), decay_total.reshape(1, -1), cache_decay, step_gates,
        step_lengths.reshape(1, -1), query_weight, key_weight, value_weight,
        cache_keys, cache_values,
        step_keys.reshape(steps * span, local), step_values.reshape(steps * span, local),
    )
    return pl.pallas_call(
        functools.partial(project, rows),
        out_shape=(
            jax.ShapeDtypeStruct((rows, columns), BF16),
            jax.ShapeDtypeStruct((steps, columns), BF16),
        ),
        in_specs=[vmem, vmem],
        out_specs=(vmem, vmem),
        compiler_params=pltpu.CompilerParams(vmem_limit_bytes=16 * 1024 * 1024),
    )(att, out_weight)


def solution(mesh):
    rows = P(("dp", "kv"), None)
    both = P(("dp", "kv"), "tp")
    cols = P(None, "tp")
    in_specs = (
        rows, rows, P(), cols, cols, cols, P(), P(), cols, both, both,
        P("tp", ("dp", "kv")), P("dp"),
        P(("dp", "kv"), None, "tp"), P(("dp", "kv"), None, "tp"),
        P(("dp", "kv"), "tp", None), P(("dp", "kv")),
    )
    return jax.shard_map(
        per_device, mesh=mesh, in_specs=in_specs, out_specs=(both, both), check_vma=False
    )
```

```python
import functools
import math

import jax
import jax.numpy as jnp
from jax import lax
from jax.experimental import pallas as pl
from jax.experimental.pallas import tpu as pltpu
from jax.sharding import PartitionSpec as P

norm_eps = 1e-06
negative = -1e30
log2e = math.log2(math.e)
MESH = pl.DeviceIdType.MESH
F32 = jnp.float32
BF16 = jnp.bfloat16
NT = (((1,), (1,)), ((), ()))


def fence():
    pl.delay(1)


def iota(shape, dim):
    return lax.broadcasted_iota(jnp.int32, shape, dim)


def normalize(rows, gain):
    wide = rows.astype(F32)
    factor = lax.rsqrt(jnp.mean(wide * wide, axis=-1, keepdims=True) + norm_eps)
    return (wide * factor * gain).astype(BF16)


def to_column(row, count):
    eye = iota((count, count), 0) == iota((count, count), 1)
    return jnp.sum(jnp.where(eye, row, 0.0), axis=1, keepdims=True)


def kernel(
    n, heads, width,
    tok_h, stok_h, gain_h, gate_w_h, gate_b_h, total_h, cache_decay_h, step_gates_h, step_len_h,
    wq, wk, wv, cache_k, cache_v, step_k, step_v,
    out_att,
    tok, stok, gain, gate_w, gate_b, total_decay, cache_decay, step_gates, step_len,
    nrm, wq_v, wk_v, wv_v, k_all, cv_v, v_turned, sk_v, sv_v,
    q_all, lg, gate_in, gate_out, bias_rows, bias_lanes, picks,
    own_mean, own_stat, to_r, to_l, stat_r, stat_l, near, near_stat, own_final, own_final_stat, att,
    local_sem, q_right, q_left, q_far, q_recv, g_send, g_recv, far_sem,
    m_send, m_recv, s_send, s_recv, x_send, x_recv,
):
    me = lax.axis_index("kv")
    tp = lax.axis_index("tp")
    rows = tok.shape[0]
    steps = stok.shape[0]
    cache_len = cache_k.shape[0]
    span = step_k.shape[0] // steps
    local = heads * width
    pair_lanes = 2 * width
    pairs = heads // 2
    keys = cache_len + rows
    root = math.sqrt(width)
    scale = log2e / root

    count = [0]

    def fetch(src, dst):
        copy = pltpu.make_async_copy(src, dst, local_sem.at[count[0]])
        count[0] += 1
        copy.start()
        return copy

    halves = 2 if local % 256 == 0 else 1
    part = local // halves
    c_tok = fetch(tok_h, tok)
    c_gain = fetch(gain_h, gain)
    c_stok = fetch(stok_h, stok)
    c_wq = [
        fetch(wq.at[:, pl.ds(c * part, part)], wq_v.at[:, pl.ds(c * part, part)])
        for c in range(halves)
    ]

    has_right = me < n - 1
    has_left = me > 0
    right = lax.rem(me + 1, n)
    left = lax.rem(me + n - 1, n)

    reach = n == 4
    first, last = 0, n - 1
    middle = jnp.logical_and(has_left, has_right)
    edge = jnp.logical_not(middle)

    def both(a, b):
        return jnp.logical_and(a, b)

    def as_count(flag):
        return flag.astype(jnp.int32)

    barrier = pltpu.get_barrier_semaphore()

    def hello(condition, target):
        @pl.when(condition)
        def _():
            pl.semaphore_signal(barrier, inc=1, device_id={"kv": target}, device_id_type=MESH)

    hello(has_right, right)
    hello(has_left, left)
    pl.semaphore_signal(barrier, inc=1, device_id={"tp": 1 - tp}, device_id_type=MESH)
    greeted = 1 + as_count(has_right) + as_count(has_left)
    if reach:
        hello(me == first, 2)
        hello(me == 2, first)
        hello(me == n - 3, last)
        for each in (first, 2, last):
            greeted = greeted + as_count(me == each)

    def enter():
        pl.semaphore_wait(barrier, greeted)
        if reach:
            @pl.when(me == last)
            def _():
                pl.semaphore_signal(far_sem, inc=1, device_id={"kv": n - 3}, device_id_type=MESH)

    def q_copy(source, p, sem, target):
        return pltpu.make_async_remote_copy(
            src_ref=q_all.at[source, p], dst_ref=q_all.at[source, p],
            send_sem=sem, recv_sem=q_recv.at[source, p],
            device_id={"kv": target}, device_id_type=MESH,
        )

    def q_to_right(source, p):
        return q_copy(source, p, q_right.at[source], right)

    def q_to_left(source, p):
        return q_copy(source, p, q_left.at[source], left)

    def q_to_far(p):
        return q_copy(me, p, q_far, jnp.where(me == first, 2, n - 3))

    size = 2 if pairs % 2 == 0 else 1
    groups = [range(g, g + size) for g in range(0, pairs, size)]

    def part_target(side, owner):
        if side == 0:
            straight = both(owner == last, me == n - 3)
            return jnp.where(straight, last, right) if reach else right
        straight = both(owner == first, me == 2)
        return jnp.where(straight, first, left) if reach else left

    def part_slot(side, owner, target):
        return owner if side == 0 else jnp.where(owner == target, n, owner)

    def mean_copy(side, owner, p):
        means = to_r if side == 0 else to_l
        target = part_target(side, owner)
        return pltpu.make_async_remote_copy(
            src_ref=means.at[owner, p], dst_ref=means.at[owner, p],
            send_sem=m_send.at[owner], recv_sem=m_recv.at[part_slot(side, owner, target), p],
            device_id={"kv": target}, device_id_type=MESH,
        )

    def stat_copy(side, owner, g):
        stats = stat_r if side == 0 else stat_l
        target = part_target(side, owner)
        return pltpu.make_async_remote_copy(
            src_ref=stats.at[owner, g], dst_ref=stats.at[owner, g],
            send_sem=s_send.at[owner], recv_sem=s_recv.at[part_slot(side, owner, target), g],
            device_id={"kv": target}, device_id_type=MESH,
        )

    def near_mean(p):
        return pltpu.make_async_remote_copy(
            src_ref=near.at[p], dst_ref=near.at[p],
            send_sem=m_send.at[n], recv_sem=m_recv.at[1, p],
            device_id={"kv": jnp.where(me == 1, first, last)}, device_id_type=MESH,
        )

    def near_level(g):
        return pltpu.make_async_remote_copy(
            src_ref=near_stat.at[g], dst_ref=near_stat.at[g],
            send_sem=s_send.at[n], recv_sem=s_recv.at[1, g],
            device_id={"kv": jnp.where(me == 1, first, last)}, device_id_type=MESH,
        )

    def await_mean(means, slot, owner, p):
        pltpu.make_async_remote_copy(
            src_ref=means.at[owner, p], dst_ref=means.at[owner, p],
            send_sem=m_send.at[owner], recv_sem=m_recv.at[slot, p],
            device_id={"tp": 1 - tp}, device_id_type=MESH,
        ).wait_recv()

    def await_stat(stats, slot, owner, g):
        pltpu.make_async_remote_copy(
            src_ref=stats.at[owner, g], dst_ref=stats.at[owner, g],
            send_sem=s_send.at[owner], recv_sem=s_recv.at[slot, g],
            device_id={"tp": 1 - tp}, device_id_type=MESH,
        ).wait_recv()

    def all_sent(ref, sem, recv):
        pltpu.make_async_remote_copy(
            src_ref=ref, dst_ref=ref, send_sem=sem, recv_sem=recv,
            device_id={"tp": 1 - tp}, device_id_type=MESH,
        ).wait_send()

    c_tok.wait()
    c_gain.wait()
    c_stok.wait()
    c_gw = fetch(gate_w_h, gate_w)
    c_gb = fetch(gate_b_h, gate_b)
    c_wk = fetch(wk, wk_v)
    c_wv = fetch(wv, wv_v)
    c_cv = fetch(cache_v, cv_v)
    c_ck = fetch(cache_k, k_all.at[pl.ds(0, cache_len)])
    c_td = fetch(total_h, total_decay)
    c_cd = fetch(cache_decay_h, cache_decay)
    c_sk = fetch(step_k, sk_v)
    c_sv = fetch(step_v, sv_v)
    c_sg = fetch(step_gates_h, step_gates)
    c_sl = fetch(step_len_h, step_len)
    nrm[pl.ds(0, rows)] = normalize(tok[...], gain[...])
    pad = nrm.shape[0] - rows
    step_norm = normalize(stok[...], gain[...]).astype(F32)
    step_rows = jnp.zeros((pad, nrm.shape[1]), F32)
    for b in range(steps):
        step_rows = jnp.where(iota((pad, nrm.shape[1]), 0) == b, step_norm[b : b + 1], step_rows)
    nrm[pl.ds(rows, pad)] = step_rows.astype(BF16)

    def send_queries(which):
        for p in which:
            @pl.when(has_right)
            def _():
                q_to_right(me, p).start()

            @pl.when(has_left)
            def _():
                q_to_left(me, p).start()

    pairs_in_part = part // pair_lanes
    step_q_parts = []
    for c in range(halves):
        c_wq[c].wait()
        q_new = jnp.dot(
            nrm[...], wq_v[:, c * part : (c + 1) * part], preferred_element_type=F32
        ).astype(BF16)
        turned = q_new[:rows].T
        for i in range(pairs_in_part):
            q_all[me, c * pairs_in_part + i] = turned[i * pair_lanes : (i + 1) * pair_lanes]
        step_q_parts.append(q_new[rows:].astype(F32))

        chunk = range(c * pairs_in_part, (c + 1) * pairs_in_part)

        @pl.when(has_left)
        def _():
            if c == 0:
                enter()
            if reach:
                @pl.when(has_right)
                def _():
                    send_queries(chunk)

                @pl.when(jnp.logical_not(has_right))
                def _():
                    for p in chunk:
                        q_to_far(p).start()
            else:
                send_queries(chunk)

    step_q = jnp.concatenate(step_q_parts, axis=1)

    c_gw.wait()
    c_gb.wait()
    logits = lax.dot_general(gate_w[...], nrm[...], NT, preferred_element_type=F32)
    logits = logits + to_column(gate_b[...], gate_w.shape[0])
    lg[...] = jnp.minimum(logits, 0.0) - jnp.log1p(jnp.exp(-jnp.abs(logits)))
    own_lg = lg[pl.ds(pl.multiple_of(tp * heads, heads), heads), :]
    piece_lg = own_lg[:, :rows]
    own_sum = jnp.broadcast_to(jnp.sum(piece_lg, axis=1, keepdims=True), gate_out.shape)

    g_copy = pltpu.make_async_remote_copy(
        src_ref=gate_out, dst_ref=gate_in, send_sem=g_send, recv_sem=g_recv,
        device_id={"kv": right}, device_id_type=MESH,
    )

    @pl.when(jnp.logical_not(has_left))
    def _():
        gate_in[...] = jnp.zeros(gate_in.shape, F32)
        gate_out[...] = own_sum

        enter()

        @pl.when(has_right)
        def _():
            g_copy.start()

        if reach:
            for p in range(pairs):
                q_to_far(p).start()
        else:
            send_queries(range(pairs))

    c_wk.wait()
    c_wv.wait()
    c_cv.wait()
    c_td.wait()
    c_cd.wait()
    c_ck.wait()
    k_new = jnp.dot(nrm[...], wk_v[...], preferred_element_type=F32).astype(BF16)
    k_all[pl.ds(cache_len, rows)] = k_new[:rows]
    step_nk = k_new[rows:].astype(F32)
    v_new = jnp.dot(nrm[...], wv_v[...], preferred_element_type=F32).astype(BF16)
    v_turned[:, pl.ds(cache_len, rows)] = v_new[:rows].T
    step_nv = v_new[rows:].astype(F32)
    v_turned[:, pl.ds(0, cache_len)] = cv_v[...].T

    upto = (iota((rows, rows), 0) <= iota((rows, rows), 1)).astype(F32)
    running = jnp.dot(
        piece_lg, upto, preferred_element_type=F32, precision=lax.Precision.HIGHEST
    )

    def bias_terms(bias):
        high = bias.astype(BF16).astype(F32)
        rest = bias - high
        middle = rest.astype(BF16).astype(F32)
        low = rest - middle
        blank = jnp.zeros((128 - 3 * heads, bias.shape[1]), F32)
        return jnp.concatenate([high, middle, low, blank], axis=0).T.astype(BF16)

    lg_start = to_column(total_decay[...], gate_w.shape[0])
    start_rows = jnp.where(tp == 0, lg_start[:heads], lg_start[heads : 2 * heads])
    bias_lanes[pl.ds(0, cache_len)] = bias_terms((start_rows - cache_decay[...]) * root)
    bias_rows[...] = running

    head_of_column = lax.div(iota((128, 2 * rows), 1), rows)
    lane_of_term = iota((128, 2 * rows), 0)
    for p in range(pairs):
        hit = jnp.logical_and(
            lax.rem(lane_of_term, heads) == 2 * p + head_of_column, lane_of_term < 3 * heads
        )
        picks[p] = hit.astype(F32).astype(BF16)

    def pass_prefix():
        @pl.when(has_left)
        def _():
            g_copy.wait_recv()

            @pl.when(has_right)
            def _():
                gate_out[...] = gate_in[...] + own_sum
                g_copy.start()

    def finish_bias():
        fresh = -(gate_in[:, :1] + bias_rows[...]) * root
        bias_lanes[pl.ds(cache_len, rows)] = bias_terms(fresh)

    first_rows = iota((pair_lanes, rows), 0) < width
    causal = lax.rem(iota((rows, 2 * rows), 1), rows) >= iota((rows, 2 * rows), 0)

    def spread(two):
        return jnp.concatenate(
            [
                jnp.broadcast_to(two[0:1], (width, rows)),
                jnp.broadcast_to(two[1:2], (width, rows)),
            ],
            axis=0,
        )

    def scores_of(source, p, used):
        q_pair = q_all[source, p]
        zero = jnp.zeros_like(q_pair)
        rhs = jnp.concatenate(
            [
                jnp.concatenate(
                    [jnp.where(first_rows, q_pair, zero), jnp.where(first_rows, zero, q_pair)],
                    axis=1,
                ),
                picks[p],
            ],
            axis=0,
        )
        lhs = jnp.concatenate([k_all[pl.ds(0, used), lanes_of(p)], bias_lanes[pl.ds(0, used)]], axis=1)
        return jnp.dot(lhs, rhs, preferred_element_type=F32)

    def lanes_of(p):
        return pl.ds(pl.multiple_of(p * pair_lanes, pair_lanes), pair_lanes)

    def weigh(raw):
        high = jnp.max(raw, axis=0, keepdims=True)
        weight = jnp.exp2((raw - high) * scale)
        mass = jnp.sum(weight, axis=0, keepdims=True)
        return weight.astype(BF16), mass, high * scale + jnp.log2(mass)

    def attend(source, group, used, masked):
        raws = [scores_of(source, p, used) for p in group]
        if masked:
            raws = [
                jnp.concatenate(
                    [raw[:cache_len], jnp.where(causal, raw[cache_len:], negative)], axis=0
                )
                for raw in raws
            ]
        weighed = [weigh(raw) for raw in raws]
        results = []
        for p, (weight, mass, level) in zip(group, weighed):
            values = v_turned[lanes_of(p), pl.ds(0, used)]
            mix = jnp.dot(values, weight, preferred_element_type=F32) * (1.0 / mass)
            mean = jnp.concatenate([mix[:width, :rows], mix[width:, rows:]], axis=0)
            levels = jnp.concatenate([level[:, :rows], level[:, rows:]], axis=0)
            results.append((p, mean, levels))
        return results

    def shares_of(levels):
        best = functools.reduce(jnp.maximum, levels)
        shares = [jnp.exp2(level - best) for level in levels]
        total = functools.reduce(jnp.add, shares)
        inverse = 1.0 / total
        return [share * inverse for share in shares], best + jnp.log2(total)

    def blend(shares, means, i):
        return functools.reduce(
            jnp.add,
            [spread(share[2 * i : 2 * i + 2]) * mean for share, mean in zip(shares, means)],
        )

    def stack(results):
        return jnp.concatenate([level for _, _, level in results], axis=0)

    def in_group(g):
        return [g * size + i for i in range(size)]

    def arrived(from_left, k, g):
        for p in in_group(g):
            if from_left:
                q_to_right(me - k, p).wait_recv()
            else:
                q_to_left(me + k, p).wait_recv()

    def pass_on(from_left, k, g):
        for p in in_group(g):
            copy = q_to_right(me - k, p) if from_left else q_to_left(me + k, p)
            copy.wait_recv()
            copy.start()

    def attend_keep(from_left, k, g):
        source, used = (me - k, cache_len) if from_left else (me + k, keys)
        fence()
        results = attend(source, in_group(g), used, False)
        for p, mean, level in results:
            own_mean[source, p] = mean
        own_stat[source, g] = stack(results)

    def attend_near(from_left, g):
        source, used = (me - 1, cache_len) if from_left else (me + 1, keys)
        fence()
        results = attend(source, in_group(g), used, False)
        for p, mean, level in results:
            near[p] = mean.astype(BF16)
        near_stat[g] = stack(results)
        near_level(g).start()
        for p, _, _ in results:
            near_mean(p).start()

    def attend_edge(from_left, k, g):
        source, used, side = (me - k, cache_len, 1) if from_left else (me + k, keys, 0)
        means, stats = (to_l, stat_l) if from_left else (to_r, stat_r)
        arrived(from_left, k, g)
        fence()
        results = attend(source, in_group(g), used, False)
        for p, mean, level in results:
            means[source, p] = mean.astype(BF16)
        stats[source, g] = stack(results)
        stat_copy(side, source, g).start()
        for p in in_group(g):
            mean_copy(side, source, p).start()

    def attend_own():
        fence()
        results = attend(me, range(pairs), keys, True)
        for p, mean, level in results:
            own_final[p] = mean
        for g, group in enumerate(groups):
            own_final_stat[g] = stack([results[p] for p in group])

    def decode():
        head_mask = lax.div(iota((heads, local), 1), width) == iota((heads, local), 0)
        chunk = 128
        chunks = span // chunk
        later = (iota((chunk, chunk), 0) > iota((chunk, chunk), 1)).astype(F32)
        c_sk.wait()
        c_sv.wait()
        c_sg.wait()
        c_sl.wait()
        step_att = jnp.zeros((pad, local), F32)
        for b in range(steps):
            length = step_len[0, b]
            in_cache = iota((heads, span), 1) < length
            kept = jnp.where(in_cache, step_gates[b], 0.0)
            tail = jnp.zeros((heads, 1), F32)
            parts = [None] * chunks
            for c in reversed(range(chunks)):
                piece = kept[:, c * chunk : (c + 1) * chunk]
                inner = jnp.dot(
                    piece, later, preferred_element_type=F32, precision=lax.Precision.HIGHEST
                )
                parts[c] = inner + tail
                tail = tail + jnp.sum(piece, axis=1, keepdims=True)
            after = jnp.concatenate(parts, axis=1)
            q_row = jnp.where(head_mask, step_q[b : b + 1], 0.0)
            scores = lax.dot_general(
                q_row.astype(BF16), sk_v[pl.ds(b * span, span)], NT, preferred_element_type=F32
            )
            new_lg = own_lg[:, rows + b : rows + b + 1]
            scores = scores * scale + (new_lg + after) * log2e
            scores = jnp.where(in_cache, scores, negative)
            self_score = jnp.sum(q_row * step_nk[b : b + 1], axis=1, keepdims=True) * scale
            high = jnp.maximum(jnp.max(scores, axis=1, keepdims=True), self_score)
            weight = jnp.exp2(scores - high)
            self_weight = jnp.exp2(self_score - high)
            mass = jnp.sum(weight, axis=1, keepdims=True) + self_weight
            mix = jnp.dot(
                weight.astype(BF16), sv_v[pl.ds(b * span, span)], preferred_element_type=F32
            )
            mix = mix + self_weight.astype(BF16).astype(F32) * step_nv[b : b + 1]
            one = jnp.sum(jnp.where(head_mask, mix / mass, 0.0), axis=0, keepdims=True)
            step_att = jnp.where(iota((pad, local), 0) == b, one, step_att)
        done = step_att.astype(BF16)
        for p in range(pairs):
            att[tp * pairs + p, pl.ds(rows, pad)] = done[:, p * pair_lanes : (p + 1) * pair_lanes]

    parts = len(groups)

    if reach:
        @pl.when(edge)
        def _():
            send_queries(range(pairs))

    def each_group(make):
        def body(g, carry):
            make(g)
            return carry

        lax.fori_loop(0, parts, body, 0)

    @pl.when(jnp.logical_not(has_left))
    def _():
        pass_prefix()
        finish_bias()

    @pl.when(edge)
    def _():
        def step(i, carry):
            k = jnp.where(i == 1, 1, jnp.where(i == 2, n - 1, i - 1)) if reach else i

            @pl.when(has_left)
            def _():
                each_group(lambda g: attend_edge(True, k, g))

            @pl.when(has_right)
            def _():
                each_group(lambda g: attend_edge(False, k, g))

            @pl.when(i == 1)
            def _():
                fence()
                decode()

            return carry

        lax.fori_loop(1, n, step, 0)

        @pl.when(has_left)
        def _():
            pass_prefix()
            finish_bias()

        attend_own()

    if reach:
        @pl.when(me == n - 3)
        def _():
            pass_prefix()
            finish_bias()

            def turn_one(g):
                for k in (2, 1):
                    pass_on(False, k, g)
                    attend_keep(False, k, g)

            each_group(turn_one)

            def body(g):
                arrived(True, 1, g)
                attend_near(True, g)

            each_group(body)

        @pl.when(me == 2)
        def _():
            def turn_two(g):
                for k in (2, 1):
                    pass_on(True, k, g)
                    attend_keep(True, k, g)

                @pl.when(g == 0)
                def _():
                    pass_prefix()

            each_group(turn_two)
            finish_bias()

            def body(g):
                arrived(False, 1, g)
                attend_near(False, g)

            each_group(body)
    else:
        @pl.when(middle)
        def _():
            pass_prefix()
            finish_bias()

            def step(k, carry):
                for from_left, there in ((True, me >= k), (False, me + k < n)):
                    @pl.when(there)
                    def _():
                        def body(g):
                            pass_on(from_left, k, g)

                        each_group(body)

                for from_left, there in ((True, me >= k), (False, me + k < n)):
                    @pl.when(there)
                    def _():
                        each_group(lambda g: attend_keep(from_left, k, g))

                return carry

            lax.fori_loop(1, n, step, 0)

    @pl.when(middle)
    def _():
        attend_own()
        fence()
        decode()

    def forward(side, owner):
        means, stats = (to_r, stat_r) if side == 0 else (to_l, stat_l)
        for g, group in enumerate(groups):
            await_stat(stats, owner, owner, g)
            shares, level = shares_of([stats[owner, g], own_stat[owner, g]])
            stats[owner, g] = level
            stat_copy(side, owner, g).start()
            for i, p in enumerate(group):
                await_mean(means, owner, owner, p)
                mean = blend(shares, [means[owner, p].astype(F32), own_mean[owner, p]], i)
                means[owner, p] = mean.astype(BF16)
                mean_copy(side, owner, p).start()

    if reach:
        @pl.when(me == n - 3)
        def _():
            pl.semaphore_wait(far_sem, 1)
            forward(0, last)
            forward(0, 2)

        @pl.when(me == 2)
        def _():
            forward(1, first)
            forward(1, n - 3)
    else:
        def pass_right(r):
            @pl.when(both(has_left, r > me))
            def _():
                forward(0, r)

        def pass_left(r):
            @pl.when(both(has_right, n - 1 - r < me))
            def _():
                forward(1, n - 1 - r)

        def turn(r, carry):
            @pl.when(2 * me < n)
            def _():
                pass_right(r)
                pass_left(r)

            @pl.when(2 * me >= n)
            def _():
                pass_left(r)
                pass_right(r)

            return carry

        @pl.when(middle)
        def _():
            lax.fori_loop(1, n, turn, 0)

    def swap_copy(core, p):
        slot = core * pairs + p
        return pltpu.make_async_remote_copy(
            src_ref=att.at[slot], dst_ref=att.at[slot],
            send_sem=x_send, recv_sem=x_recv.at[p],
            device_id={"tp": 1 - tp}, device_id_type=MESH,
        )

    def finish(from_left, from_right, from_near):
        for g, group in enumerate(groups):
            levels = [own_final_stat[g]]
            if from_near:
                near_level(g).wait_recv()
                levels.append(near_stat[g])
            if from_left:
                await_stat(stat_r, me, me, g)
                levels.append(stat_r[me, g])
            if from_right:
                await_stat(stat_l, n, me, g)
                levels.append(stat_l[me, g])
            shares, _ = shares_of(levels)
            for i, p in enumerate(group):
                means = [own_final[p]]
                if from_near:
                    near_mean(p).wait_recv()
                    means.append(near[p].astype(F32))
                if from_left:
                    await_mean(to_r, me, me, p)
                    means.append(to_r[me, p].astype(F32))
                if from_right:
                    await_mean(to_l, n, me, p)
                    means.append(to_l[me, p].astype(F32))
                att[tp * pairs + p, pl.ds(0, rows)] = blend(shares, means, i).T.astype(BF16)
                swap_copy(tp, p).start()

    @pl.when(middle)
    def _():
        finish(True, True, False)

    @pl.when(both(has_left, jnp.logical_not(has_right)))
    def _():
        finish(True, False, reach)

    @pl.when(both(has_right, jnp.logical_not(has_left)))
    def _():
        finish(False, True, reach)

    for p in range(pairs):
        swap_copy(1 - tp, p).wait_recv()
    for i in range(2 * pairs):
        out_att[:, i * pair_lanes : (i + 1) * pair_lanes] = att[i]

    all_sent(att.at[pl.ds(tp * pairs, pairs)], x_send, x_recv.at[0])

    @pl.when(has_right)
    def _():
        g_copy.wait_send()

    if reach:
        @pl.when(edge)
        def _():
            all_sent(q_all.at[me], q_far, q_recv.at[me, 0])

        @pl.when(jnp.logical_or(me == 1, me == n - 2))
        def _():
            all_sent(near, m_send.at[n], m_recv.at[n, 0])
            all_sent(near_stat, s_send.at[n], s_recv.at[n, 0])

    def sent(owner, carry):
        right_sent = both(has_right, owner <= me)
        left_sent = both(has_left, owner >= me)
        part_right = both(has_right, owner > me)
        part_left = both(has_left, owner < me)
        if reach:
            right_sent = both(right_sent, jnp.logical_not(both(owner == first, me == 1)))
            left_sent = both(left_sent, jnp.logical_not(both(owner == last, me == n - 2)))
            part_right = both(part_right, jnp.logical_not(both(owner == last, me == n - 2)))
            part_left = both(part_left, jnp.logical_not(both(owner == first, me == 1)))

        @pl.when(right_sent)
        def _():
            all_sent(q_all.at[owner], q_right.at[owner], q_recv.at[owner, 0])

        @pl.when(left_sent)
        def _():
            all_sent(q_all.at[owner], q_left.at[owner], q_recv.at[owner, 0])

        @pl.when(part_right)
        def _():
            all_sent(to_r.at[owner], m_send.at[owner], m_recv.at[owner, 0])
            all_sent(stat_r.at[owner], s_send.at[owner], s_recv.at[owner, 0])

        @pl.when(part_left)
        def _():
            all_sent(to_l.at[owner], m_send.at[owner], m_recv.at[owner, 0])
            all_sent(stat_l.at[owner], s_send.at[owner], s_recv.at[owner, 0])

        return carry

    lax.fori_loop(0, n, sent, 0)


def project(rows, att, weight, out_piece, out_step):
    projected = jnp.dot(att[...], weight[...], preferred_element_type=F32)
    out_piece[...] = projected[:rows].astype(BF16)
    out_step[...] = projected[rows : rows + out_step.shape[0]].astype(BF16)


def per_device(
    piece_tokens, step_tokens, norm_gain, query_weight, key_weight, value_weight,
    gate_weight, gate_bias, out_weight, cache_keys, cache_values, cache_decay,
    decay_total, step_keys, step_values, step_gates, step_lengths,
):
    n = lax.axis_size("kv")
    rows, model = piece_tokens.shape
    steps = step_tokens.shape[0]
    heads = cache_decay.shape[0]
    local = query_weight.shape[1]
    width = local // heads
    pairs = heads // 2
    groups = pairs // 2 if pairs % 2 == 0 else pairs
    cache_len = cache_keys.shape[0]
    keys = cache_len + rows
    span = step_keys.shape[1]
    columns = out_weight.shape[1]
    padded = rows + 16 * (-(-steps // 16))
    all_heads = gate_weight.shape[1]
    vmem = pl.BlockSpec(memory_space=pltpu.VMEM)
    hbm = pl.BlockSpec(memory_space=pltpu.HBM)
    dma = pltpu.SemaphoreType.DMA
    att = pl.pallas_call(
        functools.partial(kernel, n, heads, width),
        out_shape=pltpu.VMEM((padded, out_weight.shape[0]), BF16),
        in_specs=[hbm] * 16,
        out_specs=vmem,
        scratch_shapes=[
            pltpu.VMEM((rows, model), BF16),
            pltpu.VMEM((steps, model), BF16),
            pltpu.VMEM((1, model), F32),
            pltpu.VMEM((all_heads, model), BF16),
            pltpu.VMEM((1, all_heads), F32),
            pltpu.VMEM((1, all_heads), F32),
            pltpu.VMEM(cache_decay.shape, F32),
            pltpu.VMEM(step_gates.shape, F32),
            pltpu.SMEM((1, steps), jnp.int32),
            pltpu.VMEM((padded, model), BF16),
            pltpu.VMEM(query_weight.shape, BF16),
            pltpu.VMEM(key_weight.shape, BF16),
            pltpu.VMEM(value_weight.shape, BF16),
            pltpu.VMEM((keys, local), BF16),
            pltpu.VMEM((cache_len, local), BF16),
            pltpu.VMEM((local, keys), BF16),
            pltpu.VMEM((steps * span, local), BF16),
            pltpu.VMEM((steps * span, local), BF16),
            pltpu.VMEM((n, pairs, 2 * width, rows), BF16),
            pltpu.VMEM((all_heads, padded), F32),
            pltpu.VMEM((heads, 128), F32),
            pltpu.VMEM((heads, 128), F32),
            pltpu.VMEM((heads, rows), F32),
            pltpu.VMEM((keys, 128), BF16),
            pltpu.VMEM((pairs, 128, 2 * rows), BF16),
            pltpu.VMEM((n, pairs, 2 * width, rows), F32),
            pltpu.VMEM((n, groups, heads // groups, rows), F32),
            pltpu.VMEM((n, pairs, 2 * width, rows), BF16),
            pltpu.VMEM((n, pairs, 2 * width, rows), BF16),
            pltpu.VMEM((n, groups, heads // groups, rows), F32),
            pltpu.VMEM((n, groups, heads // groups, rows), F32),
            pltpu.VMEM((pairs, 2 * width, rows), BF16),
            pltpu.VMEM((groups, heads // groups, rows), F32),
            pltpu.VMEM((pairs, 2 * width, rows), F32),
            pltpu.VMEM((groups, heads // groups, rows), F32),
            pltpu.VMEM((2 * pairs, padded, 2 * width), BF16),
            dma((17,)),
            dma((n,)), dma((n,)), dma(()), dma((n, pairs)),
            dma(()), dma(()), pltpu.SemaphoreType.REGULAR,
            dma((n + 1,)), dma((n + 1, pairs)), dma((n + 1,)), dma((n + 1, groups)),
            dma(()), dma((pairs,)),
        ],
        compiler_params=pltpu.CompilerParams(
            collective_id=0, has_side_effects=True, vmem_limit_bytes=56 * 1024 * 1024
        ),
    )(
        piece_tokens, step_tokens, norm_gain.reshape(1, -1), gate_weight.T,
        gate_bias.reshape(1, -1), decay_total.reshape(1, -1), cache_decay, step_gates,
        step_lengths.reshape(1, -1), query_weight, key_weight, value_weight,
        cache_keys, cache_values,
        step_keys.reshape(steps * span, local), step_values.reshape(steps * span, local),
    )
    return pl.pallas_call(
        functools.partial(project, rows),
        out_shape=(
            jax.ShapeDtypeStruct((rows, columns), BF16),
            jax.ShapeDtypeStruct((steps, columns), BF16),
        ),
        in_specs=[vmem, vmem],
        out_specs=(vmem, vmem),
        compiler_params=pltpu.CompilerParams(vmem_limit_bytes=16 * 1024 * 1024),
    )(att, out_weight)


def solution(mesh):
    rows = P(("dp", "kv"), None)
    both = P(("dp", "kv"), "tp")
    cols = P(None, "tp")
    in_specs = (
        rows, rows, P(), cols, cols, cols, P(), P(), cols, both, both,
        P("tp", ("dp", "kv")), P("dp"),
        P(("dp", "kv"), None, "tp"), P(("dp", "kv"), None, "tp"),
        P(("dp", "kv"), "tp", None), P(("dp", "kv")),
    )
    return jax.shard_map(
        per_device, mesh=mesh, in_specs=in_specs, out_specs=(both, both), check_vma=False
    )
```

```python
import functools
import math

import jax
import jax.numpy as jnp
from jax import lax
from jax.experimental import pallas as pl
from jax.experimental.pallas import tpu as pltpu
from jax.sharding import PartitionSpec as P

norm_eps = 1e-06
negative = -1e30
log2e = math.log2(math.e)
MESH = pl.DeviceIdType.MESH
F32 = jnp.float32
BF16 = jnp.bfloat16
NT = (((1,), (1,)), ((), ()))


def fence():
    pl.delay(1)


def iota(shape, dim):
    return lax.broadcasted_iota(jnp.int32, shape, dim)


def normalize(rows, gain):
    wide = rows.astype(F32)
    factor = lax.rsqrt(jnp.mean(wide * wide, axis=-1, keepdims=True) + norm_eps)
    return (wide * factor * gain).astype(BF16)


def to_column(row, count):
    eye = iota((count, count), 0) == iota((count, count), 1)
    return jnp.sum(jnp.where(eye, row, 0.0), axis=1, keepdims=True)


def kernel(
    n, heads, width,
    tok_h, stok_h, gain_h, gate_w_h, gate_b_h, total_h, cache_decay_h, step_gates_h, step_len_h,
    wq, wk, wv, cache_k, cache_v, step_k, step_v,
    out_att,
    tok, stok, gain, gate_w, gate_b, total_decay, cache_decay, step_gates, step_len,
    nrm, wq_v, wk_v, wv_v, k_all, cv_v, v_turned, sk_v, sv_v,
    q_all, lg, gate_in, gate_out, bias_rows, bias_lanes, picks,
    own_mean, own_stat, to_r, to_l, stat_r, stat_l, near, near_stat, own_final, own_final_stat, att,
    local_sem, q_right, q_left, q_far, q_recv, g_send, g_recv, far_sem,
    m_send, m_recv, s_send, s_recv, x_send, x_recv,
):
    me = lax.axis_index("kv")
    tp = lax.axis_index("tp")
    rows = tok.shape[0]
    steps = stok.shape[0]
    cache_len = cache_k.shape[0]
    span = step_k.shape[0] // steps
    local = heads * width
    pair_lanes = 2 * width
    pairs = heads // 2
    keys = cache_len + rows
    root = math.sqrt(width)
    scale = log2e / root

    count = [0]

    def fetch(src, dst):
        copy = pltpu.make_async_copy(src, dst, local_sem.at[count[0]])
        count[0] += 1
        copy.start()
        return copy

    halves = 2 if local % 256 == 0 else 1
    part = local // halves
    c_tok = fetch(tok_h, tok)
    c_gain = fetch(gain_h, gain)
    c_stok = fetch(stok_h, stok)
    c_wq = [
        fetch(wq.at[:, pl.ds(c * part, part)], wq_v.at[:, pl.ds(c * part, part)])
        for c in range(halves)
    ]

    has_right = me < n - 1
    has_left = me > 0
    right = lax.rem(me + 1, n)
    left = lax.rem(me + n - 1, n)

    reach = n == 4
    first, last = 0, n - 1
    middle = jnp.logical_and(has_left, has_right)
    edge = jnp.logical_not(middle)

    def both(a, b):
        return jnp.logical_and(a, b)

    def as_count(flag):
        return flag.astype(jnp.int32)

    barrier = pltpu.get_barrier_semaphore()

    def hello(condition, target):
        @pl.when(condition)
        def _():
            pl.semaphore_signal(barrier, inc=1, device_id={"kv": target}, device_id_type=MESH)

    hello(has_right, right)
    hello(has_left, left)
    pl.semaphore_signal(barrier, inc=1, device_id={"tp": 1 - tp}, device_id_type=MESH)
    greeted = 1 + as_count(has_right) + as_count(has_left)
    if reach:
        hello(me == first, 2)
        hello(me == 2, first)
        hello(me == n - 3, last)
        for each in (first, 2, last):
            greeted = greeted + as_count(me == each)

    def enter():
        pl.semaphore_wait(barrier, greeted)
        if reach:
            @pl.when(me == last)
            def _():
                pl.semaphore_signal(far_sem, inc=1, device_id={"kv": n - 3}, device_id_type=MESH)

    def q_copy(source, p, sem, target):
        return pltpu.make_async_remote_copy(
            src_ref=q_all.at[source, p], dst_ref=q_all.at[source, p],
            send_sem=sem, recv_sem=q_recv.at[source, p],
            device_id={"kv": target}, device_id_type=MESH,
        )

    def q_to_right(source, p):
        return q_copy(source, p, q_right.at[source], right)

    def q_to_left(source, p):
        return q_copy(source, p, q_left.at[source], left)

    def q_to_far(p):
        return q_copy(me, p, q_far, jnp.where(me == first, 2, n - 3))

    size = 2 if pairs % 2 == 0 else 1
    groups = [range(g, g + size) for g in range(0, pairs, size)]

    def part_target(side, owner):
        if side == 0:
            straight = both(owner == last, me == n - 3)
            return jnp.where(straight, last, right) if reach else right
        straight = both(owner == first, me == 2)
        return jnp.where(straight, first, left) if reach else left

    def part_slot(side, owner, target):
        return owner if side == 0 else jnp.where(owner == target, n, owner)

    def mean_copy(side, owner, p):
        means = to_r if side == 0 else to_l
        target = part_target(side, owner)
        return pltpu.make_async_remote_copy(
            src_ref=means.at[owner, p], dst_ref=means.at[owner, p],
            send_sem=m_send.at[owner], recv_sem=m_recv.at[part_slot(side, owner, target), p],
            device_id={"kv": target}, device_id_type=MESH,
        )

    def stat_copy(side, owner, g):
        stats = stat_r if side == 0 else stat_l
        target = part_target(side, owner)
        return pltpu.make_async_remote_copy(
            src_ref=stats.at[owner, g], dst_ref=stats.at[owner, g],
            send_sem=s_send.at[owner], recv_sem=s_recv.at[part_slot(side, owner, target), g],
            device_id={"kv": target}, device_id_type=MESH,
        )

    def near_mean(p):
        return pltpu.make_async_remote_copy(
            src_ref=near.at[p], dst_ref=near.at[p],
            send_sem=m_send.at[n], recv_sem=m_recv.at[1, p],
            device_id={"kv": jnp.where(me == 1, first, last)}, device_id_type=MESH,
        )

    def near_level(g):
        return pltpu.make_async_remote_copy(
            src_ref=near_stat.at[g], dst_ref=near_stat.at[g],
            send_sem=s_send.at[n], recv_sem=s_recv.at[1, g],
            device_id={"kv": jnp.where(me == 1, first, last)}, device_id_type=MESH,
        )

    def await_mean(means, slot, owner, p):
        pltpu.make_async_remote_copy(
            src_ref=means.at[owner, p], dst_ref=means.at[owner, p],
            send_sem=m_send.at[owner], recv_sem=m_recv.at[slot, p],
            device_id={"tp": 1 - tp}, device_id_type=MESH,
        ).wait_recv()

    def await_stat(stats, slot, owner, g):
        pltpu.make_async_remote_copy(
            src_ref=stats.at[owner, g], dst_ref=stats.at[owner, g],
            send_sem=s_send.at[owner], recv_sem=s_recv.at[slot, g],
            device_id={"tp": 1 - tp}, device_id_type=MESH,
        ).wait_recv()

    def all_sent(ref, sem, recv):
        pltpu.make_async_remote_copy(
            src_ref=ref, dst_ref=ref, send_sem=sem, recv_sem=recv,
            device_id={"tp": 1 - tp}, device_id_type=MESH,
        ).wait_send()

    c_tok.wait()
    c_gain.wait()
    c_stok.wait()
    c_gw = fetch(gate_w_h, gate_w)
    c_gb = fetch(gate_b_h, gate_b)
    c_wk = fetch(wk, wk_v)
    c_wv = fetch(wv, wv_v)
    c_cv = fetch(cache_v, cv_v)
    c_ck = fetch(cache_k, k_all.at[pl.ds(0, cache_len)])
    c_td = fetch(total_h, total_decay)
    c_cd = fetch(cache_decay_h, cache_decay)
    c_sk = fetch(step_k, sk_v)
    c_sv = fetch(step_v, sv_v)
    c_sg = fetch(step_gates_h, step_gates)
    c_sl = fetch(step_len_h, step_len)
    nrm[pl.ds(0, rows)] = normalize(tok[...], gain[...])
    pad = nrm.shape[0] - rows
    step_norm = normalize(stok[...], gain[...]).astype(F32)
    step_rows = jnp.zeros((pad, nrm.shape[1]), F32)
    for b in range(steps):
        step_rows = jnp.where(iota((pad, nrm.shape[1]), 0) == b, step_norm[b : b + 1], step_rows)
    nrm[pl.ds(rows, pad)] = step_rows.astype(BF16)

    def send_queries(which):
        for p in which:
            @pl.when(has_right)
            def _():
                q_to_right(me, p).start()

            @pl.when(has_left)
            def _():
                q_to_left(me, p).start()

    pairs_in_part = part // pair_lanes
    step_q_parts = []
    for c in range(halves):
        c_wq[c].wait()
        q_new = jnp.dot(
            nrm[...], wq_v[:, c * part : (c + 1) * part], preferred_element_type=F32
        ).astype(BF16)
        turned = q_new[:rows].T
        for i in range(pairs_in_part):
            q_all[me, c * pairs_in_part + i] = turned[i * pair_lanes : (i + 1) * pair_lanes]
        step_q_parts.append(q_new[rows:].astype(F32))

        chunk = range(c * pairs_in_part, (c + 1) * pairs_in_part)

        @pl.when(has_left)
        def _():
            if c == 0:
                enter()
            if reach:
                @pl.when(has_right)
                def _():
                    send_queries(chunk)

                @pl.when(jnp.logical_not(has_right))
                def _():
                    for p in chunk:
                        q_to_far(p).start()
            else:
                send_queries(chunk)

    step_q = jnp.concatenate(step_q_parts, axis=1)

    c_gw.wait()
    c_gb.wait()
    logits = lax.dot_general(gate_w[...], nrm[...], NT, preferred_element_type=F32)
    logits = logits + to_column(gate_b[...], gate_w.shape[0])
    lg[...] = jnp.minimum(logits, 0.0) - jnp.log1p(jnp.exp(-jnp.abs(logits)))
    own_lg = lg[pl.ds(pl.multiple_of(tp * heads, heads), heads), :]
    piece_lg = own_lg[:, :rows]
    own_sum = jnp.broadcast_to(jnp.sum(piece_lg, axis=1, keepdims=True), gate_out.shape)

    g_copy = pltpu.make_async_remote_copy(
        src_ref=gate_out, dst_ref=gate_in, send_sem=g_send, recv_sem=g_recv,
        device_id={"kv": right}, device_id_type=MESH,
    )

    @pl.when(jnp.logical_not(has_left))
    def _():
        gate_in[...] = jnp.zeros(gate_in.shape, F32)
        gate_out[...] = own_sum

        enter()

        @pl.when(has_right)
        def _():
            g_copy.start()

        if reach:
            for p in range(pairs):
                q_to_far(p).start()
        else:
            send_queries(range(pairs))

    c_wk.wait()
    c_wv.wait()
    c_cv.wait()
    c_td.wait()
    c_cd.wait()
    c_ck.wait()
    k_new = jnp.dot(nrm[...], wk_v[...], preferred_element_type=F32).astype(BF16)
    k_all[pl.ds(cache_len, rows)] = k_new[:rows]
    step_nk = k_new[rows:].astype(F32)
    v_new = jnp.dot(nrm[...], wv_v[...], preferred_element_type=F32).astype(BF16)
    v_turned[:, pl.ds(cache_len, rows)] = v_new[:rows].T
    step_nv = v_new[rows:].astype(F32)
    v_turned[:, pl.ds(0, cache_len)] = cv_v[...].T

    upto = (iota((rows, rows), 0) <= iota((rows, rows), 1)).astype(F32)
    running = jnp.dot(
        piece_lg, upto, preferred_element_type=F32, precision=lax.Precision.HIGHEST
    )

    def bias_terms(bias):
        high = bias.astype(BF16).astype(F32)
        rest = bias - high
        middle = rest.astype(BF16).astype(F32)
        low = rest - middle
        blank = jnp.zeros((128 - 3 * heads, bias.shape[1]), F32)
        return jnp.concatenate([high, middle, low, blank], axis=0).T.astype(BF16)

    lg_start = to_column(total_decay[...], gate_w.shape[0])
    start_rows = jnp.where(tp == 0, lg_start[:heads], lg_start[heads : 2 * heads])
    bias_lanes[pl.ds(0, cache_len)] = bias_terms((start_rows - cache_decay[...]) * root)
    bias_rows[...] = running

    head_of_column = lax.div(iota((128, 2 * rows), 1), rows)
    lane_of_term = iota((128, 2 * rows), 0)
    for p in range(pairs):
        hit = jnp.logical_and(
            lax.rem(lane_of_term, heads) == 2 * p + head_of_column, lane_of_term < 3 * heads
        )
        picks[p] = hit.astype(F32).astype(BF16)

    def pass_prefix():
        @pl.when(has_left)
        def _():
            g_copy.wait_recv()

            @pl.when(has_right)
            def _():
                gate_out[...] = gate_in[...] + own_sum
                g_copy.start()

    def finish_bias():
        fresh = -(gate_in[:, :1] + bias_rows[...]) * root
        bias_lanes[pl.ds(cache_len, rows)] = bias_terms(fresh)

    first_rows = iota((pair_lanes, rows), 0) < width
    causal = lax.rem(iota((rows, 2 * rows), 1), rows) >= iota((rows, 2 * rows), 0)

    def spread(two):
        return jnp.concatenate(
            [
                jnp.broadcast_to(two[0:1], (width, rows)),
                jnp.broadcast_to(two[1:2], (width, rows)),
            ],
            axis=0,
        )

    def scores_of(source, p, used):
        q_pair = q_all[source, p]
        zero = jnp.zeros_like(q_pair)
        rhs = jnp.concatenate(
            [
                jnp.concatenate(
                    [jnp.where(first_rows, q_pair, zero), jnp.where(first_rows, zero, q_pair)],
                    axis=1,
                ),
                picks[p],
            ],
            axis=0,
        )
        lhs = jnp.concatenate([k_all[pl.ds(0, used), lanes_of(p)], bias_lanes[pl.ds(0, used)]], axis=1)
        return jnp.dot(lhs, rhs, preferred_element_type=F32)

    def lanes_of(p):
        return pl.ds(pl.multiple_of(p * pair_lanes, pair_lanes), pair_lanes)

    def weigh(raw):
        high = jnp.max(raw, axis=0, keepdims=True)
        weight = jnp.exp2((raw - high) * scale)
        mass = jnp.sum(weight, axis=0, keepdims=True)
        return weight.astype(BF16), mass, high * scale + jnp.log2(mass)

    def attend(source, group, used, masked):
        raws = [scores_of(source, p, used) for p in group]
        if masked:
            raws = [
                jnp.concatenate(
                    [raw[:cache_len], jnp.where(causal, raw[cache_len:], negative)], axis=0
                )
                for raw in raws
            ]
        weighed = [weigh(raw) for raw in raws]
        results = []
        for p, (weight, mass, level) in zip(group, weighed):
            values = v_turned[lanes_of(p), pl.ds(0, used)]
            mix = jnp.dot(values, weight, preferred_element_type=F32) * (1.0 / mass)
            mean = jnp.concatenate([mix[:width, :rows], mix[width:, rows:]], axis=0)
            levels = jnp.concatenate([level[:, :rows], level[:, rows:]], axis=0)
            results.append((p, mean, levels))
        return results

    def shares_of(levels):
        best = functools.reduce(jnp.maximum, levels)
        shares = [jnp.exp2(level - best) for level in levels]
        total = functools.reduce(jnp.add, shares)
        inverse = 1.0 / total
        return [share * inverse for share in shares], best + jnp.log2(total)

    def blend(shares, means, i):
        return functools.reduce(
            jnp.add,
            [spread(share[2 * i : 2 * i + 2]) * mean for share, mean in zip(shares, means)],
        )

    def stack(results):
        return jnp.concatenate([level for _, _, level in results], axis=0)

    def in_group(g):
        return [g * size + i for i in range(size)]

    def arrived(from_left, k, g):
        for p in in_group(g):
            if from_left:
                q_to_right(me - k, p).wait_recv()
            else:
                q_to_left(me + k, p).wait_recv()

    def pass_on(from_left, k, g):
        for p in in_group(g):
            copy = q_to_right(me - k, p) if from_left else q_to_left(me + k, p)
            copy.wait_recv()
            copy.start()

    def attend_keep(from_left, k, g):
        source, used = (me - k, cache_len) if from_left else (me + k, keys)
        fence()
        results = attend(source, in_group(g), used, False)
        for p, mean, level in results:
            own_mean[source, p] = mean
        own_stat[source, g] = stack(results)

    def attend_near(from_left, g):
        source, used = (me - 1, cache_len) if from_left else (me + 1, keys)
        fence()
        results = attend(source, in_group(g), used, False)
        for p, mean, level in results:
            near[p] = mean.astype(BF16)
        near_stat[g] = stack(results)
        near_level(g).start()
        for p, _, _ in results:
            near_mean(p).start()

    def attend_edge(from_left, k, g):
        source, used, side = (me - k, cache_len, 1) if from_left else (me + k, keys, 0)
        means, stats = (to_l, stat_l) if from_left else (to_r, stat_r)
        arrived(from_left, k, g)
        fence()
        results = attend(source, in_group(g), used, False)
        for p, mean, level in results:
            means[source, p] = mean.astype(BF16)
        stats[source, g] = stack(results)
        stat_copy(side, source, g).start()
        for p in in_group(g):
            mean_copy(side, source, p).start()

    def attend_own():
        fence()
        results = attend(me, range(pairs), keys, True)
        for p, mean, level in results:
            own_final[p] = mean
        for g, group in enumerate(groups):
            own_final_stat[g] = stack([results[p] for p in group])

    def decode():
        head_mask = lax.div(iota((heads, local), 1), width) == iota((heads, local), 0)
        chunk = 128
        chunks = span // chunk
        later = (iota((chunk, chunk), 0) > iota((chunk, chunk), 1)).astype(F32)
        c_sk.wait()
        c_sv.wait()
        c_sg.wait()
        c_sl.wait()
        step_att = jnp.zeros((pad, local), F32)
        for b in range(steps):
            length = step_len[0, b]
            in_cache = iota((heads, span), 1) < length
            kept = jnp.where(in_cache, step_gates[b], 0.0)
            tail = jnp.zeros((heads, 1), F32)
            parts = [None] * chunks
            for c in reversed(range(chunks)):
                piece = kept[:, c * chunk : (c + 1) * chunk]
                inner = jnp.dot(
                    piece, later, preferred_element_type=F32, precision=lax.Precision.HIGHEST
                )
                parts[c] = inner + tail
                tail = tail + jnp.sum(piece, axis=1, keepdims=True)
            after = jnp.concatenate(parts, axis=1)
            q_row = jnp.where(head_mask, step_q[b : b + 1], 0.0)
            scores = lax.dot_general(
                q_row.astype(BF16), sk_v[pl.ds(b * span, span)], NT, preferred_element_type=F32
            )
            new_lg = own_lg[:, rows + b : rows + b + 1]
            scores = scores * scale + (new_lg + after) * log2e
            scores = jnp.where(in_cache, scores, negative)
            self_score = jnp.sum(q_row * step_nk[b : b + 1], axis=1, keepdims=True) * scale
            high = jnp.maximum(jnp.max(scores, axis=1, keepdims=True), self_score)
            weight = jnp.exp2(scores - high)
            self_weight = jnp.exp2(self_score - high)
            mass = jnp.sum(weight, axis=1, keepdims=True) + self_weight
            mix = jnp.dot(
                weight.astype(BF16), sv_v[pl.ds(b * span, span)], preferred_element_type=F32
            )
            mix = mix + self_weight.astype(BF16).astype(F32) * step_nv[b : b + 1]
            one = jnp.sum(jnp.where(head_mask, mix / mass, 0.0), axis=0, keepdims=True)
            step_att = jnp.where(iota((pad, local), 0) == b, one, step_att)
        done = step_att.astype(BF16)
        for p in range(pairs):
            att[tp * pairs + p, pl.ds(rows, pad)] = done[:, p * pair_lanes : (p + 1) * pair_lanes]

    parts = len(groups)

    if reach:
        @pl.when(edge)
        def _():
            send_queries(range(pairs))

    @pl.when(middle)
    def _():
        decode()

    def each_group(make):
        def body(g, carry):
            make(g)
            return carry

        lax.fori_loop(0, parts, body, 0)

    @pl.when(jnp.logical_not(has_left))
    def _():
        pass_prefix()
        finish_bias()

    @pl.when(edge)
    def _():
        def step(i, carry):
            k = jnp.where(i == 1, 1, jnp.where(i == 2, n - 1, i - 1)) if reach else i

            @pl.when(has_left)
            def _():
                each_group(lambda g: attend_edge(True, k, g))

            @pl.when(has_right)
            def _():
                each_group(lambda g: attend_edge(False, k, g))

            @pl.when(i == 1)
            def _():
                fence()
                decode()

            return carry

        lax.fori_loop(1, n, step, 0)

        @pl.when(has_left)
        def _():
            pass_prefix()
            finish_bias()

        attend_own()

    if reach:
        @pl.when(me == n - 3)
        def _():
            pass_prefix()
            finish_bias()

            def turn_one(g):
                for k in (2, 1):
                    pass_on(False, k, g)
                    attend_keep(False, k, g)

            each_group(turn_one)

            def body(g):
                arrived(True, 1, g)
                attend_near(True, g)

            each_group(body)

        @pl.when(me == 2)
        def _():
            def turn_two(g):
                for k in (2, 1):
                    pass_on(True, k, g)
                    attend_keep(True, k, g)

                @pl.when(g == 0)
                def _():
                    pass_prefix()

            each_group(turn_two)
            finish_bias()

            def body(g):
                arrived(False, 1, g)
                attend_near(False, g)

            each_group(body)
    else:
        @pl.when(middle)
        def _():
            pass_prefix()
            finish_bias()

            def step(k, carry):
                for from_left, there in ((True, me >= k), (False, me + k < n)):
                    @pl.when(there)
                    def _():
                        def body(g):
                            pass_on(from_left, k, g)

                        each_group(body)

                for from_left, there in ((True, me >= k), (False, me + k < n)):
                    @pl.when(there)
                    def _():
                        each_group(lambda g: attend_keep(from_left, k, g))

                return carry

            lax.fori_loop(1, n, step, 0)

    @pl.when(middle)
    def _():
        attend_own()

    def forward(side, owner):
        means, stats = (to_r, stat_r) if side == 0 else (to_l, stat_l)
        for g, group in enumerate(groups):
            await_stat(stats, owner, owner, g)
            shares, level = shares_of([stats[owner, g], own_stat[owner, g]])
            stats[owner, g] = level
            stat_copy(side, owner, g).start()
            for i, p in enumerate(group):
                await_mean(means, owner, owner, p)
                mean = blend(shares, [means[owner, p].astype(F32), own_mean[owner, p]], i)
                means[owner, p] = mean.astype(BF16)
                mean_copy(side, owner, p).start()

    if reach:
        @pl.when(me == n - 3)
        def _():
            pl.semaphore_wait(far_sem, 1)
            forward(0, last)
            forward(0, 2)

        @pl.when(me == 2)
        def _():
            forward(1, first)
            forward(1, n - 3)
    else:
        def pass_right(r):
            @pl.when(both(has_left, r > me))
            def _():
                forward(0, r)

        def pass_left(r):
            @pl.when(both(has_right, n - 1 - r < me))
            def _():
                forward(1, n - 1 - r)

        def turn(r, carry):
            @pl.when(2 * me < n)
            def _():
                pass_right(r)
                pass_left(r)

            @pl.when(2 * me >= n)
            def _():
                pass_left(r)
                pass_right(r)

            return carry

        @pl.when(middle)
        def _():
            lax.fori_loop(1, n, turn, 0)

    def swap_copy(core, p):
        slot = core * pairs + p
        return pltpu.make_async_remote_copy(
            src_ref=att.at[slot], dst_ref=att.at[slot],
            send_sem=x_send, recv_sem=x_recv.at[p],
            device_id={"tp": 1 - tp}, device_id_type=MESH,
        )

    def finish(from_left, from_right, from_near):
        for g, group in enumerate(groups):
            levels = [own_final_stat[g]]
            if from_near:
                near_level(g).wait_recv()
                levels.append(near_stat[g])
            if from_left:
                await_stat(stat_r, me, me, g)
                levels.append(stat_r[me, g])
            if from_right:
                await_stat(stat_l, n, me, g)
                levels.append(stat_l[me, g])
            shares, _ = shares_of(levels)
            for i, p in enumerate(group):
                means = [own_final[p]]
                if from_near:
                    near_mean(p).wait_recv()
                    means.append(near[p].astype(F32))
                if from_left:
                    await_mean(to_r, me, me, p)
                    means.append(to_r[me, p].astype(F32))
                if from_right:
                    await_mean(to_l, n, me, p)
                    means.append(to_l[me, p].astype(F32))
                att[tp * pairs + p, pl.ds(0, rows)] = blend(shares, means, i).T.astype(BF16)
                swap_copy(tp, p).start()

    @pl.when(middle)
    def _():
        finish(True, True, False)

    @pl.when(both(has_left, jnp.logical_not(has_right)))
    def _():
        finish(True, False, reach)

    @pl.when(both(has_right, jnp.logical_not(has_left)))
    def _():
        finish(False, True, reach)

    for p in range(pairs):
        swap_copy(1 - tp, p).wait_recv()
    for i in range(2 * pairs):
        out_att[:, i * pair_lanes : (i + 1) * pair_lanes] = att[i]

    all_sent(att.at[pl.ds(tp * pairs, pairs)], x_send, x_recv.at[0])

    @pl.when(has_right)
    def _():
        g_copy.wait_send()

    if reach:
        @pl.when(edge)
        def _():
            all_sent(q_all.at[me], q_far, q_recv.at[me, 0])

        @pl.when(jnp.logical_or(me == 1, me == n - 2))
        def _():
            all_sent(near, m_send.at[n], m_recv.at[n, 0])
            all_sent(near_stat, s_send.at[n], s_recv.at[n, 0])

    def sent(owner, carry):
        right_sent = both(has_right, owner <= me)
        left_sent = both(has_left, owner >= me)
        part_right = both(has_right, owner > me)
        part_left = both(has_left, owner < me)
        if reach:
            right_sent = both(right_sent, jnp.logical_not(both(owner == first, me == 1)))
            left_sent = both(left_sent, jnp.logical_not(both(owner == last, me == n - 2)))
            part_right = both(part_right, jnp.logical_not(both(owner == last, me == n - 2)))
            part_left = both(part_left, jnp.logical_not(both(owner == first, me == 1)))

        @pl.when(right_sent)
        def _():
            all_sent(q_all.at[owner], q_right.at[owner], q_recv.at[owner, 0])

        @pl.when(left_sent)
        def _():
            all_sent(q_all.at[owner], q_left.at[owner], q_recv.at[owner, 0])

        @pl.when(part_right)
        def _():
            all_sent(to_r.at[owner], m_send.at[owner], m_recv.at[owner, 0])
            all_sent(stat_r.at[owner], s_send.at[owner], s_recv.at[owner, 0])

        @pl.when(part_left)
        def _():
            all_sent(to_l.at[owner], m_send.at[owner], m_recv.at[owner, 0])
            all_sent(stat_l.at[owner], s_send.at[owner], s_recv.at[owner, 0])

        return carry

    lax.fori_loop(0, n, sent, 0)


def project(rows, att, weight, out_piece, out_step):
    projected = jnp.dot(att[...], weight[...], preferred_element_type=F32)
    out_piece[...] = projected[:rows].astype(BF16)
    out_step[...] = projected[rows : rows + out_step.shape[0]].astype(BF16)


def per_device(
    piece_tokens, step_tokens, norm_gain, query_weight, key_weight, value_weight,
    gate_weight, gate_bias, out_weight, cache_keys, cache_values, cache_decay,
    decay_total, step_keys, step_values, step_gates, step_lengths,
):
    n = lax.axis_size("kv")
    rows, model = piece_tokens.shape
    steps = step_tokens.shape[0]
    heads = cache_decay.shape[0]
    local = query_weight.shape[1]
    width = local // heads
    pairs = heads // 2
    groups = pairs // 2 if pairs % 2 == 0 else pairs
    cache_len = cache_keys.shape[0]
    keys = cache_len + rows
    span = step_keys.shape[1]
    columns = out_weight.shape[1]
    padded = rows + 16 * (-(-steps // 16))
    all_heads = gate_weight.shape[1]
    vmem = pl.BlockSpec(memory_space=pltpu.VMEM)
    hbm = pl.BlockSpec(memory_space=pltpu.HBM)
    dma = pltpu.SemaphoreType.DMA
    att = pl.pallas_call(
        functools.partial(kernel, n, heads, width),
        out_shape=pltpu.VMEM((padded, out_weight.shape[0]), BF16),
        in_specs=[hbm] * 16,
        out_specs=vmem,
        scratch_shapes=[
            pltpu.VMEM((rows, model), BF16),
            pltpu.VMEM((steps, model), BF16),
            pltpu.VMEM((1, model), F32),
            pltpu.VMEM((all_heads, model), BF16),
            pltpu.VMEM((1, all_heads), F32),
            pltpu.VMEM((1, all_heads), F32),
            pltpu.VMEM(cache_decay.shape, F32),
            pltpu.VMEM(step_gates.shape, F32),
            pltpu.SMEM((1, steps), jnp.int32),
            pltpu.VMEM((padded, model), BF16),
            pltpu.VMEM(query_weight.shape, BF16),
            pltpu.VMEM(key_weight.shape, BF16),
            pltpu.VMEM(value_weight.shape, BF16),
            pltpu.VMEM((keys, local), BF16),
            pltpu.VMEM((cache_len, local), BF16),
            pltpu.VMEM((local, keys), BF16),
            pltpu.VMEM((steps * span, local), BF16),
            pltpu.VMEM((steps * span, local), BF16),
            pltpu.VMEM((n, pairs, 2 * width, rows), BF16),
            pltpu.VMEM((all_heads, padded), F32),
            pltpu.VMEM((heads, 128), F32),
            pltpu.VMEM((heads, 128), F32),
            pltpu.VMEM((heads, rows), F32),
            pltpu.VMEM((keys, 128), BF16),
            pltpu.VMEM((pairs, 128, 2 * rows), BF16),
            pltpu.VMEM((n, pairs, 2 * width, rows), F32),
            pltpu.VMEM((n, groups, heads // groups, rows), F32),
            pltpu.VMEM((n, pairs, 2 * width, rows), BF16),
            pltpu.VMEM((n, pairs, 2 * width, rows), BF16),
            pltpu.VMEM((n, groups, heads // groups, rows), F32),
            pltpu.VMEM((n, groups, heads // groups, rows), F32),
            pltpu.VMEM((pairs, 2 * width, rows), BF16),
            pltpu.VMEM((groups, heads // groups, rows), F32),
            pltpu.VMEM((pairs, 2 * width, rows), F32),
            pltpu.VMEM((groups, heads // groups, rows), F32),
            pltpu.VMEM((2 * pairs, padded, 2 * width), BF16),
            dma((17,)),
            dma((n,)), dma((n,)), dma(()), dma((n, pairs)),
            dma(()), dma(()), pltpu.SemaphoreType.REGULAR,
            dma((n + 1,)), dma((n + 1, pairs)), dma((n + 1,)), dma((n + 1, groups)),
            dma(()), dma((pairs,)),
        ],
        compiler_params=pltpu.CompilerParams(
            collective_id=0, has_side_effects=True, vmem_limit_bytes=56 * 1024 * 1024
        ),
    )(
        piece_tokens, step_tokens, norm_gain.reshape(1, -1), gate_weight.T,
        gate_bias.reshape(1, -1), decay_total.reshape(1, -1), cache_decay, step_gates,
        step_lengths.reshape(1, -1), query_weight, key_weight, value_weight,
        cache_keys, cache_values,
        step_keys.reshape(steps * span, local), step_values.reshape(steps * span, local),
    )
    return pl.pallas_call(
        functools.partial(project, rows),
        out_shape=(
            jax.ShapeDtypeStruct((rows, columns), BF16),
            jax.ShapeDtypeStruct((steps, columns), BF16),
        ),
        in_specs=[vmem, vmem],
        out_specs=(vmem, vmem),
        compiler_params=pltpu.CompilerParams(vmem_limit_bytes=16 * 1024 * 1024),
    )(att, out_weight)


def solution(mesh):
    rows = P(("dp", "kv"), None)
    both = P(("dp", "kv"), "tp")
    cols = P(None, "tp")
    in_specs = (
        rows, rows, P(), cols, cols, cols, P(), P(), cols, both, both,
        P("tp", ("dp", "kv")), P("dp"),
        P(("dp", "kv"), None, "tp"), P(("dp", "kv"), None, "tp"),
        P(("dp", "kv"), "tp", None), P(("dp", "kv")),
    )
    return jax.shard_map(
        per_device, mesh=mesh, in_specs=in_specs, out_specs=(both, both), check_vma=False
    )
```

```python
import functools
import math

import jax
import jax.numpy as jnp
from jax import lax
from jax.experimental import pallas as pl
from jax.experimental.pallas import tpu as pltpu
from jax.sharding import PartitionSpec as P

norm_eps = 1e-06
negative = -1e30
log2e = math.log2(math.e)
MESH = pl.DeviceIdType.MESH
F32 = jnp.float32
BF16 = jnp.bfloat16
NT = (((1,), (1,)), ((), ()))


def fence():
    pl.delay(1)


def iota(shape, dim):
    return lax.broadcasted_iota(jnp.int32, shape, dim)


def normalize(rows, gain):
    wide = rows.astype(F32)
    factor = lax.rsqrt(jnp.mean(wide * wide, axis=-1, keepdims=True) + norm_eps)
    return (wide * factor * gain).astype(BF16)


def to_column(row, count):
    eye = iota((count, count), 0) == iota((count, count), 1)
    return jnp.sum(jnp.where(eye, row, 0.0), axis=1, keepdims=True)


def kernel(
    n, heads, width,
    tok_h, stok_h, gain_h, gate_w_h, gate_b_h, total_h, cache_decay_h, step_gates_h, step_len_h,
    wq, wk, wv, cache_k, cache_v, step_k, step_v,
    out_att,
    tok, stok, gain, gate_w, gate_b, total_decay, cache_decay, step_gates, step_len,
    nrm, wq_v, wk_v, wv_v, k_all, cv_v, v_turned, sk_v, sv_v,
    q_all, lg, gate_in, gate_out, bias_rows, bias_lanes, picks,
    own_mean, own_stat, to_r, to_l, stat_r, stat_l, near, near_stat, own_final, own_final_stat, att,
    local_sem, q_right, q_left, q_far, q_recv, g_send, g_recv, far_sem,
    m_send, m_recv, s_send, s_recv, x_send, x_recv,
):
    me = lax.axis_index("kv")
    tp = lax.axis_index("tp")
    rows = tok.shape[0]
    steps = stok.shape[0]
    cache_len = cache_k.shape[0]
    span = step_k.shape[0] // steps
    local = heads * width
    pair_lanes = 2 * width
    pairs = heads // 2
    keys = cache_len + rows
    root = math.sqrt(width)
    scale = log2e / root

    count = [0]

    def fetch(src, dst):
        copy = pltpu.make_async_copy(src, dst, local_sem.at[count[0]])
        count[0] += 1
        copy.start()
        return copy

    halves = 2 if local % 256 == 0 else 1
    part = local // halves
    c_tok = fetch(tok_h, tok)
    c_gain = fetch(gain_h, gain)
    c_stok = fetch(stok_h, stok)
    c_wq = [
        fetch(wq.at[:, pl.ds(c * part, part)], wq_v.at[:, pl.ds(c * part, part)])
        for c in range(halves)
    ]

    has_right = me < n - 1
    has_left = me > 0
    right = lax.rem(me + 1, n)
    left = lax.rem(me + n - 1, n)

    reach = n == 4
    first, last = 0, n - 1
    middle = jnp.logical_and(has_left, has_right)
    edge = jnp.logical_not(middle)

    def both(a, b):
        return jnp.logical_and(a, b)

    def as_count(flag):
        return flag.astype(jnp.int32)

    barrier = pltpu.get_barrier_semaphore()

    def hello(condition, target):
        @pl.when(condition)
        def _():
            pl.semaphore_signal(barrier, inc=1, device_id={"kv": target}, device_id_type=MESH)

    hello(has_right, right)
    hello(has_left, left)
    pl.semaphore_signal(barrier, inc=1, device_id={"tp": 1 - tp}, device_id_type=MESH)
    greeted = 1 + as_count(has_right) + as_count(has_left)
    if reach:
        hello(me == first, 2)
        hello(me == 2, first)
        hello(me == n - 3, last)
        for each in (first, 2, last):
            greeted = greeted + as_count(me == each)

    def enter():
        pl.semaphore_wait(barrier, greeted)
        if reach:
            @pl.when(me == last)
            def _():
                pl.semaphore_signal(far_sem, inc=1, device_id={"kv": n - 3}, device_id_type=MESH)

    def q_copy(source, p, sem, target):
        return pltpu.make_async_remote_copy(
            src_ref=q_all.at[source, p], dst_ref=q_all.at[source, p],
            send_sem=sem, recv_sem=q_recv.at[source, p],
            device_id={"kv": target}, device_id_type=MESH,
        )

    def q_to_right(source, p):
        return q_copy(source, p, q_right.at[source], right)

    def q_to_left(source, p):
        return q_copy(source, p, q_left.at[source], left)

    def q_to_far(p):
        return q_copy(me, p, q_far, jnp.where(me == first, 2, n - 3))

    size = 2 if pairs % 2 == 0 else 1
    groups = [range(g, g + size) for g in range(0, pairs, size)]

    def part_target(side, owner):
        if side == 0:
            straight = both(owner == last, me == n - 3)
            return jnp.where(straight, last, right) if reach else right
        straight = both(owner == first, me == 2)
        return jnp.where(straight, first, left) if reach else left

    def part_slot(side, owner, target):
        return owner if side == 0 else jnp.where(owner == target, n, owner)

    def mean_copy(side, owner, p):
        means = to_r if side == 0 else to_l
        target = part_target(side, owner)
        return pltpu.make_async_remote_copy(
            src_ref=means.at[owner, p], dst_ref=means.at[owner, p],
            send_sem=m_send.at[owner], recv_sem=m_recv.at[part_slot(side, owner, target), p],
            device_id={"kv": target}, device_id_type=MESH,
        )

    def stat_copy(side, owner, g):
        stats = stat_r if side == 0 else stat_l
        target = part_target(side, owner)
        return pltpu.make_async_remote_copy(
            src_ref=stats.at[owner, g], dst_ref=stats.at[owner, g],
            send_sem=s_send.at[owner], recv_sem=s_recv.at[part_slot(side, owner, target), g],
            device_id={"kv": target}, device_id_type=MESH,
        )

    def near_mean(p):
        return pltpu.make_async_remote_copy(
            src_ref=near.at[p], dst_ref=near.at[p],
            send_sem=m_send.at[n], recv_sem=m_recv.at[1, p],
            device_id={"kv": jnp.where(me == 1, first, last)}, device_id_type=MESH,
        )

    def near_level(g):
        return pltpu.make_async_remote_copy(
            src_ref=near_stat.at[g], dst_ref=near_stat.at[g],
            send_sem=s_send.at[n], recv_sem=s_recv.at[1, g],
            device_id={"kv": jnp.where(me == 1, first, last)}, device_id_type=MESH,
        )

    def await_mean(means, slot, owner, p):
        pltpu.make_async_remote_copy(
            src_ref=means.at[owner, p], dst_ref=means.at[owner, p],
            send_sem=m_send.at[owner], recv_sem=m_recv.at[slot, p],
            device_id={"tp": 1 - tp}, device_id_type=MESH,
        ).wait_recv()

    def await_stat(stats, slot, owner, g):
        pltpu.make_async_remote_copy(
            src_ref=stats.at[owner, g], dst_ref=stats.at[owner, g],
            send_sem=s_send.at[owner], recv_sem=s_recv.at[slot, g],
            device_id={"tp": 1 - tp}, device_id_type=MESH,
        ).wait_recv()

    def all_sent(ref, sem, recv):
        pltpu.make_async_remote_copy(
            src_ref=ref, dst_ref=ref, send_sem=sem, recv_sem=recv,
            device_id={"tp": 1 - tp}, device_id_type=MESH,
        ).wait_send()

    c_tok.wait()
    c_gain.wait()
    c_stok.wait()
    c_gw = fetch(gate_w_h, gate_w)
    c_gb = fetch(gate_b_h, gate_b)
    c_wk = fetch(wk, wk_v)
    c_wv = fetch(wv, wv_v)
    c_cv = fetch(cache_v, cv_v)
    c_ck = fetch(cache_k, k_all.at[pl.ds(0, cache_len)])
    c_td = fetch(total_h, total_decay)
    c_cd = fetch(cache_decay_h, cache_decay)
    c_sk = fetch(step_k, sk_v)
    c_sv = fetch(step_v, sv_v)
    c_sg = fetch(step_gates_h, step_gates)
    c_sl = fetch(step_len_h, step_len)
    nrm[pl.ds(0, rows)] = normalize(tok[...], gain[...])
    pad = nrm.shape[0] - rows
    step_norm = normalize(stok[...], gain[...]).astype(F32)
    step_rows = jnp.zeros((pad, nrm.shape[1]), F32)
    for b in range(steps):
        step_rows = jnp.where(iota((pad, nrm.shape[1]), 0) == b, step_norm[b : b + 1], step_rows)
    nrm[pl.ds(rows, pad)] = step_rows.astype(BF16)

    def send_queries(which):
        for p in which:
            @pl.when(has_right)
            def _():
                q_to_right(me, p).start()

            @pl.when(has_left)
            def _():
                q_to_left(me, p).start()

    def send_outward(which):
        for p in which:
            @pl.when(me == 1)
            def _():
                q_to_left(me, p).start()

            @pl.when(me == n - 2)
            def _():
                q_to_right(me, p).start()

    def send_inward(which):
        for p in which:
            @pl.when(me == 1)
            def _():
                q_to_right(me, p).start()

            @pl.when(me == n - 2)
            def _():
                q_to_left(me, p).start()

    pairs_in_part = part // pair_lanes
    step_q_parts = []
    for c in range(halves):
        c_wq[c].wait()
        q_new = jnp.dot(
            nrm[...], wq_v[:, c * part : (c + 1) * part], preferred_element_type=F32
        ).astype(BF16)
        turned = q_new[:rows].T
        for i in range(pairs_in_part):
            q_all[me, c * pairs_in_part + i] = turned[i * pair_lanes : (i + 1) * pair_lanes]
        step_q_parts.append(q_new[rows:].astype(F32))

        chunk = range(c * pairs_in_part, (c + 1) * pairs_in_part)

        @pl.when(has_left)
        def _():
            if c == 0:
                enter()
            if reach:
                @pl.when(has_right)
                def _():
                    if c == 0 and halves > 1:
                        send_queries(chunk)
                    else:
                        send_outward(chunk)

                @pl.when(jnp.logical_not(has_right))
                def _():
                    for p in chunk:
                        q_to_far(p).start()
            else:
                send_queries(chunk)

    step_q = jnp.concatenate(step_q_parts, axis=1)
    if reach:
        @pl.when(jnp.logical_not(has_left))
        def _():
            enter()
            for p in range(pairs_in_part):
                q_to_far(p).start()


    c_gw.wait()
    c_gb.wait()
    logits = lax.dot_general(gate_w[...], nrm[...], NT, preferred_element_type=F32)
    logits = logits + to_column(gate_b[...], gate_w.shape[0])
    lg[...] = jnp.minimum(logits, 0.0) - jnp.log1p(jnp.exp(-jnp.abs(logits)))
    own_lg = lg[pl.ds(pl.multiple_of(tp * heads, heads), heads), :]
    piece_lg = own_lg[:, :rows]
    own_sum = jnp.broadcast_to(jnp.sum(piece_lg, axis=1, keepdims=True), gate_out.shape)

    g_copy = pltpu.make_async_remote_copy(
        src_ref=gate_out, dst_ref=gate_in, send_sem=g_send, recv_sem=g_recv,
        device_id={"kv": right}, device_id_type=MESH,
    )

    @pl.when(jnp.logical_not(has_left))
    def _():
        gate_in[...] = jnp.zeros(gate_in.shape, F32)
        gate_out[...] = own_sum

        if not reach:
            enter()

        @pl.when(has_right)
        def _():
            g_copy.start()

        if reach:
            for p in range(pairs_in_part, pairs):
                q_to_far(p).start()
        else:
            send_queries(range(pairs))

    c_wk.wait()
    c_wv.wait()
    c_cv.wait()
    c_td.wait()
    c_cd.wait()
    c_ck.wait()
    k_new = jnp.dot(nrm[...], wk_v[...], preferred_element_type=F32).astype(BF16)
    k_all[pl.ds(cache_len, rows)] = k_new[:rows]
    step_nk = k_new[rows:].astype(F32)
    v_new = jnp.dot(nrm[...], wv_v[...], preferred_element_type=F32).astype(BF16)
    v_turned[:, pl.ds(cache_len, rows)] = v_new[:rows].T
    step_nv = v_new[rows:].astype(F32)
    v_turned[:, pl.ds(0, cache_len)] = cv_v[...].T

    upto = (iota((rows, rows), 0) <= iota((rows, rows), 1)).astype(F32)
    running = jnp.dot(
        piece_lg, upto, preferred_element_type=F32, precision=lax.Precision.HIGHEST
    )

    def bias_terms(bias):
        high = bias.astype(BF16).astype(F32)
        rest = bias - high
        middle = rest.astype(BF16).astype(F32)
        low = rest - middle
        blank = jnp.zeros((128 - 3 * heads, bias.shape[1]), F32)
        return jnp.concatenate([high, middle, low, blank], axis=0).T.astype(BF16)

    lg_start = to_column(total_decay[...], gate_w.shape[0])
    start_rows = jnp.where(tp == 0, lg_start[:heads], lg_start[heads : 2 * heads])
    bias_lanes[pl.ds(0, cache_len)] = bias_terms((start_rows - cache_decay[...]) * root)
    bias_rows[...] = running

    head_of_column = lax.div(iota((128, 2 * rows), 1), rows)
    lane_of_term = iota((128, 2 * rows), 0)
    for p in range(pairs):
        hit = jnp.logical_and(
            lax.rem(lane_of_term, heads) == 2 * p + head_of_column, lane_of_term < 3 * heads
        )
        picks[p] = hit.astype(F32).astype(BF16)

    def pass_prefix():
        @pl.when(has_left)
        def _():
            g_copy.wait_recv()

            @pl.when(has_right)
            def _():
                gate_out[...] = gate_in[...] + own_sum
                g_copy.start()

    def finish_bias():
        fresh = -(gate_in[:, :1] + bias_rows[...]) * root
        bias_lanes[pl.ds(cache_len, rows)] = bias_terms(fresh)

    first_rows = iota((pair_lanes, rows), 0) < width
    causal = lax.rem(iota((rows, 2 * rows), 1), rows) >= iota((rows, 2 * rows), 0)

    def spread(two):
        return jnp.concatenate(
            [
                jnp.broadcast_to(two[0:1], (width, rows)),
                jnp.broadcast_to(two[1:2], (width, rows)),
            ],
            axis=0,
        )

    def scores_of(source, p, used):
        q_pair = q_all[source, p]
        zero = jnp.zeros_like(q_pair)
        rhs = jnp.concatenate(
            [
                jnp.concatenate(
                    [jnp.where(first_rows, q_pair, zero), jnp.where(first_rows, zero, q_pair)],
                    axis=1,
                ),
                picks[p],
            ],
            axis=0,
        )
        lhs = jnp.concatenate([k_all[pl.ds(0, used), lanes_of(p)], bias_lanes[pl.ds(0, used)]], axis=1)
        return jnp.dot(lhs, rhs, preferred_element_type=F32)

    def lanes_of(p):
        return pl.ds(pl.multiple_of(p * pair_lanes, pair_lanes), pair_lanes)

    def weigh(raw):
        high = jnp.max(raw, axis=0, keepdims=True)
        weight = jnp.exp2((raw - high) * scale)
        mass = jnp.sum(weight, axis=0, keepdims=True)
        return weight.astype(BF16), mass, high * scale + jnp.log2(mass)

    def attend(source, group, used, masked):
        raws = [scores_of(source, p, used) for p in group]
        if masked:
            raws = [
                jnp.concatenate(
                    [raw[:cache_len], jnp.where(causal, raw[cache_len:], negative)], axis=0
                )
                for raw in raws
            ]
        weighed = [weigh(raw) for raw in raws]
        results = []
        for p, (weight, mass, level) in zip(group, weighed):
            values = v_turned[lanes_of(p), pl.ds(0, used)]
            mix = jnp.dot(values, weight, preferred_element_type=F32) * (1.0 / mass)
            mean = jnp.concatenate([mix[:width, :rows], mix[width:, rows:]], axis=0)
            levels = jnp.concatenate([level[:, :rows], level[:, rows:]], axis=0)
            results.append((p, mean, levels))
        return results

    def shares_of(levels):
        best = functools.reduce(jnp.maximum, levels)
        shares = [jnp.exp2(level - best) for level in levels]
        total = functools.reduce(jnp.add, shares)
        inverse = 1.0 / total
        return [share * inverse for share in shares], best + jnp.log2(total)

    def blend(shares, means, i):
        return functools.reduce(
            jnp.add,
            [spread(share[2 * i : 2 * i + 2]) * mean for share, mean in zip(shares, means)],
        )

    def stack(results):
        return jnp.concatenate([level for _, _, level in results], axis=0)

    def in_group(g):
        return [g * size + i for i in range(size)]

    def arrived(from_left, k, g):
        for p in in_group(g):
            if from_left:
                q_to_right(me - k, p).wait_recv()
            else:
                q_to_left(me + k, p).wait_recv()

    def pass_on(from_left, k, g):
        for p in in_group(g):
            copy = q_to_right(me - k, p) if from_left else q_to_left(me + k, p)
            copy.wait_recv()
            copy.start()

    def attend_keep(from_left, k, g):
        source, used = (me - k, cache_len) if from_left else (me + k, keys)
        fence()
        results = attend(source, in_group(g), used, False)
        for p, mean, level in results:
            own_mean[source, p] = mean
        own_stat[source, g] = stack(results)

    def attend_near(from_left, g):
        source, used = (me - 1, cache_len) if from_left else (me + 1, keys)
        fence()
        results = attend(source, in_group(g), used, False)
        for p, mean, level in results:
            near[p] = mean.astype(BF16)
        near_stat[g] = stack(results)
        near_level(g).start()
        for p, _, _ in results:
            near_mean(p).start()

    def attend_edge(from_left, k, g):
        source, used, side = (me - k, cache_len, 1) if from_left else (me + k, keys, 0)
        means, stats = (to_l, stat_l) if from_left else (to_r, stat_r)
        arrived(from_left, k, g)
        fence()
        results = attend(source, in_group(g), used, False)
        for p, mean, level in results:
            means[source, p] = mean.astype(BF16)
        stats[source, g] = stack(results)
        stat_copy(side, source, g).start()
        for p in in_group(g):
            mean_copy(side, source, p).start()

    def attend_own():
        fence()
        results = attend(me, range(pairs), keys, True)
        for p, mean, level in results:
            own_final[p] = mean
        for g, group in enumerate(groups):
            own_final_stat[g] = stack([results[p] for p in group])

    def decode():
        head_mask = lax.div(iota((heads, local), 1), width) == iota((heads, local), 0)
        chunk = 128
        chunks = span // chunk
        later = (iota((chunk, chunk), 0) > iota((chunk, chunk), 1)).astype(F32)
        c_sk.wait()
        c_sv.wait()
        c_sg.wait()
        c_sl.wait()
        step_att = jnp.zeros((pad, local), F32)
        for b in range(steps):
            length = step_len[0, b]
            in_cache = iota((heads, span), 1) < length
            kept = jnp.where(in_cache, step_gates[b], 0.0)
            tail = jnp.zeros((heads, 1), F32)
            parts = [None] * chunks
            for c in reversed(range(chunks)):
                piece = kept[:, c * chunk : (c + 1) * chunk]
                inner = jnp.dot(
                    piece, later, preferred_element_type=F32, precision=lax.Precision.HIGHEST
                )
                parts[c] = inner + tail
                tail = tail + jnp.sum(piece, axis=1, keepdims=True)
            after = jnp.concatenate(parts, axis=1)
            q_row = jnp.where(head_mask, step_q[b : b + 1], 0.0)
            scores = lax.dot_general(
                q_row.astype(BF16), sk_v[pl.ds(b * span, span)], NT, preferred_element_type=F32
            )
            new_lg = own_lg[:, rows + b : rows + b + 1]
            scores = scores * scale + (new_lg + after) * log2e
            scores = jnp.where(in_cache, scores, negative)
            self_score = jnp.sum(q_row * step_nk[b : b + 1], axis=1, keepdims=True) * scale
            high = jnp.maximum(jnp.max(scores, axis=1, keepdims=True), self_score)
            weight = jnp.exp2(scores - high)
            self_weight = jnp.exp2(self_score - high)
            mass = jnp.sum(weight, axis=1, keepdims=True) + self_weight
            mix = jnp.dot(
                weight.astype(BF16), sv_v[pl.ds(b * span, span)], preferred_element_type=F32
            )
            mix = mix + self_weight.astype(BF16).astype(F32) * step_nv[b : b + 1]
            one = jnp.sum(jnp.where(head_mask, mix / mass, 0.0), axis=0, keepdims=True)
            step_att = jnp.where(iota((pad, local), 0) == b, one, step_att)
        done = step_att.astype(BF16)
        for p in range(pairs):
            att[tp * pairs + p, pl.ds(rows, pad)] = done[:, p * pair_lanes : (p + 1) * pair_lanes]

    parts = len(groups)

    if reach:
        @pl.when(edge)
        def _():
            send_queries(range(pairs))

        @pl.when(middle)
        def _():
            send_inward(range(pairs_in_part if halves > 1 else 0, pairs))

    @pl.when(middle)
    def _():
        decode()

    def each_group(make):
        def body(g, carry):
            make(g)
            return carry

        lax.fori_loop(0, parts, body, 0)

    @pl.when(jnp.logical_not(has_left))
    def _():
        pass_prefix()
        finish_bias()

    @pl.when(edge)
    def _():
        def step(i, carry):
            k = jnp.where(i == 1, 1, jnp.where(i == 2, n - 1, i - 1)) if reach else i

            @pl.when(has_left)
            def _():
                each_group(lambda g: attend_edge(True, k, g))

            @pl.when(has_right)
            def _():
                each_group(lambda g: attend_edge(False, k, g))

            @pl.when(i == 1)
            def _():
                fence()
                decode()

            return carry

        lax.fori_loop(1, n, step, 0)

        @pl.when(has_left)
        def _():
            pass_prefix()
            finish_bias()

        attend_own()

    if reach:
        @pl.when(me == n - 3)
        def _():
            pass_prefix()
            finish_bias()

            def turn_one(g):
                for k in (2, 1):
                    pass_on(False, k, g)
                    attend_keep(False, k, g)

            each_group(turn_one)

            def body(g):
                arrived(True, 1, g)
                attend_near(True, g)

            each_group(body)

        @pl.when(me == 2)
        def _():
            def turn_two(g):
                for k in (2, 1):
                    pass_on(True, k, g)
                    attend_keep(True, k, g)

                @pl.when(g == 0)
                def _():
                    pass_prefix()

            each_group(turn_two)
            finish_bias()

            def body(g):
                arrived(False, 1, g)
                attend_near(False, g)

            each_group(body)
    else:
        @pl.when(middle)
        def _():
            pass_prefix()
            finish_bias()

            def step(k, carry):
                for from_left, there in ((True, me >= k), (False, me + k < n)):
                    @pl.when(there)
                    def _():
                        def body(g):
                            pass_on(from_left, k, g)

                        each_group(body)

                for from_left, there in ((True, me >= k), (False, me + k < n)):
                    @pl.when(there)
                    def _():
                        each_group(lambda g: attend_keep(from_left, k, g))

                return carry

            lax.fori_loop(1, n, step, 0)

    @pl.when(middle)
    def _():
        attend_own()

    def forward(side, owner):
        means, stats = (to_r, stat_r) if side == 0 else (to_l, stat_l)
        for g, group in enumerate(groups):
            await_stat(stats, owner, owner, g)
            shares, level = shares_of([stats[owner, g], own_stat[owner, g]])
            stats[owner, g] = level
            stat_copy(side, owner, g).start()
            for i, p in enumerate(group):
                await_mean(means, owner, owner, p)
                mean = blend(shares, [means[owner, p].astype(F32), own_mean[owner, p]], i)
                means[owner, p] = mean.astype(BF16)
                mean_copy(side, owner, p).start()

    if reach:
        @pl.when(me == n - 3)
        def _():
            pl.semaphore_wait(far_sem, 1)
            forward(0, last)
            forward(0, 2)

        @pl.when(me == 2)
        def _():
            forward(1, first)
            forward(1, n - 3)
    else:
        def pass_right(r):
            @pl.when(both(has_left, r > me))
            def _():
                forward(0, r)

        def pass_left(r):
            @pl.when(both(has_right, n - 1 - r < me))
            def _():
                forward(1, n - 1 - r)

        def turn(r, carry):
            @pl.when(2 * me < n)
            def _():
                pass_right(r)
                pass_left(r)

            @pl.when(2 * me >= n)
            def _():
                pass_left(r)
                pass_right(r)

            return carry

        @pl.when(middle)
        def _():
            lax.fori_loop(1, n, turn, 0)

    def swap_copy(core, p):
        slot = core * pairs + p
        return pltpu.make_async_remote_copy(
            src_ref=att.at[slot], dst_ref=att.at[slot],
            send_sem=x_send, recv_sem=x_recv.at[p],
            device_id={"tp": 1 - tp}, device_id_type=MESH,
        )

    def finish(from_left, from_right, from_near):
        for g, group in enumerate(groups):
            levels = [own_final_stat[g]]
            if from_near:
                near_level(g).wait_recv()
                levels.append(near_stat[g])
            if from_left:
                await_stat(stat_r, me, me, g)
                levels.append(stat_r[me, g])
            if from_right:
                await_stat(stat_l, n, me, g)
                levels.append(stat_l[me, g])
            shares, _ = shares_of(levels)
            for i, p in enumerate(group):
                means = [own_final[p]]
                if from_near:
                    near_mean(p).wait_recv()
                    means.append(near[p].astype(F32))
                if from_left:
                    await_mean(to_r, me, me, p)
                    means.append(to_r[me, p].astype(F32))
                if from_right:
                    await_mean(to_l, n, me, p)
                    means.append(to_l[me, p].astype(F32))
                att[tp * pairs + p, pl.ds(0, rows)] = blend(shares, means, i).T.astype(BF16)
                swap_copy(tp, p).start()

    @pl.when(middle)
    def _():
        finish(True, True, False)

    @pl.when(both(has_left, jnp.logical_not(has_right)))
    def _():
        finish(True, False, reach)

    @pl.when(both(has_right, jnp.logical_not(has_left)))
    def _():
        finish(False, True, reach)

    for p in range(pairs):
        swap_copy(1 - tp, p).wait_recv()
    for i in range(2 * pairs):
        out_att[:, i * pair_lanes : (i + 1) * pair_lanes] = att[i]

    all_sent(att.at[pl.ds(tp * pairs, pairs)], x_send, x_recv.at[0])

    @pl.when(has_right)
    def _():
        g_copy.wait_send()

    if reach:
        @pl.when(edge)
        def _():
            all_sent(q_all.at[me], q_far, q_recv.at[me, 0])

        @pl.when(jnp.logical_or(me == 1, me == n - 2))
        def _():
            all_sent(near, m_send.at[n], m_recv.at[n, 0])
            all_sent(near_stat, s_send.at[n], s_recv.at[n, 0])

    def sent(owner, carry):
        right_sent = both(has_right, owner <= me)
        left_sent = both(has_left, owner >= me)
        part_right = both(has_right, owner > me)
        part_left = both(has_left, owner < me)
        if reach:
            right_sent = both(right_sent, jnp.logical_not(both(owner == first, me == 1)))
            left_sent = both(left_sent, jnp.logical_not(both(owner == last, me == n - 2)))
            part_right = both(part_right, jnp.logical_not(both(owner == last, me == n - 2)))
            part_left = both(part_left, jnp.logical_not(both(owner == first, me == 1)))

        @pl.when(right_sent)
        def _():
            all_sent(q_all.at[owner], q_right.at[owner], q_recv.at[owner, 0])

        @pl.when(left_sent)
        def _():
            all_sent(q_all.at[owner], q_left.at[owner], q_recv.at[owner, 0])

        @pl.when(part_right)
        def _():
            all_sent(to_r.at[owner], m_send.at[owner], m_recv.at[owner, 0])
            all_sent(stat_r.at[owner], s_send.at[owner], s_recv.at[owner, 0])

        @pl.when(part_left)
        def _():
            all_sent(to_l.at[owner], m_send.at[owner], m_recv.at[owner, 0])
            all_sent(stat_l.at[owner], s_send.at[owner], s_recv.at[owner, 0])

        return carry

    lax.fori_loop(0, n, sent, 0)


def project(rows, att, weight, out_piece, out_step):
    projected = jnp.dot(att[...], weight[...], preferred_element_type=F32)
    out_piece[...] = projected[:rows].astype(BF16)
    out_step[...] = projected[rows : rows + out_step.shape[0]].astype(BF16)


def per_device(
    piece_tokens, step_tokens, norm_gain, query_weight, key_weight, value_weight,
    gate_weight, gate_bias, out_weight, cache_keys, cache_values, cache_decay,
    decay_total, step_keys, step_values, step_gates, step_lengths,
):
    n = lax.axis_size("kv")
    rows, model = piece_tokens.shape
    steps = step_tokens.shape[0]
    heads = cache_decay.shape[0]
    local = query_weight.shape[1]
    width = local // heads
    pairs = heads // 2
    groups = pairs // 2 if pairs % 2 == 0 else pairs
    cache_len = cache_keys.shape[0]
    keys = cache_len + rows
    span = step_keys.shape[1]
    columns = out_weight.shape[1]
    padded = rows + 16 * (-(-steps // 16))
    all_heads = gate_weight.shape[1]
    vmem = pl.BlockSpec(memory_space=pltpu.VMEM)
    hbm = pl.BlockSpec(memory_space=pltpu.HBM)
    dma = pltpu.SemaphoreType.DMA
    att = pl.pallas_call(
        functools.partial(kernel, n, heads, width),
        out_shape=pltpu.VMEM((padded, out_weight.shape[0]), BF16),
        in_specs=[hbm] * 16,
        out_specs=vmem,
        scratch_shapes=[
            pltpu.VMEM((rows, model), BF16),
            pltpu.VMEM((steps, model), BF16),
            pltpu.VMEM((1, model), F32),
            pltpu.VMEM((all_heads, model), BF16),
            pltpu.VMEM((1, all_heads), F32),
            pltpu.VMEM((1, all_heads), F32),
            pltpu.VMEM(cache_decay.shape, F32),
            pltpu.VMEM(step_gates.shape, F32),
            pltpu.SMEM((1, steps), jnp.int32),
            pltpu.VMEM((padded, model), BF16),
            pltpu.VMEM(query_weight.shape, BF16),
            pltpu.VMEM(key_weight.shape, BF16),
            pltpu.VMEM(value_weight.shape, BF16),
            pltpu.VMEM((keys, local), BF16),
            pltpu.VMEM((cache_len, local), BF16),
            pltpu.VMEM((local, keys), BF16),
            pltpu.VMEM((steps * span, local), BF16),
            pltpu.VMEM((steps * span, local), BF16),
            pltpu.VMEM((n, pairs, 2 * width, rows), BF16),
            pltpu.VMEM((all_heads, padded), F32),
            pltpu.VMEM((heads, 128), F32),
            pltpu.VMEM((heads, 128), F32),
            pltpu.VMEM((heads, rows), F32),
            pltpu.VMEM((keys, 128), BF16),
            pltpu.VMEM((pairs, 128, 2 * rows), BF16),
            pltpu.VMEM((n, pairs, 2 * width, rows), F32),
            pltpu.VMEM((n, groups, heads // groups, rows), F32),
            pltpu.VMEM((n, pairs, 2 * width, rows), BF16),
            pltpu.VMEM((n, pairs, 2 * width, rows), BF16),
            pltpu.VMEM((n, groups, heads // groups, rows), F32),
            pltpu.VMEM((n, groups, heads // groups, rows), F32),
            pltpu.VMEM((pairs, 2 * width, rows), BF16),
            pltpu.VMEM((groups, heads // groups, rows), F32),
            pltpu.VMEM((pairs, 2 * width, rows), F32),
            pltpu.VMEM((groups, heads // groups, rows), F32),
            pltpu.VMEM((2 * pairs, padded, 2 * width), BF16),
            dma((17,)),
            dma((n,)), dma((n,)), dma(()), dma((n, pairs)),
            dma(()), dma(()), pltpu.SemaphoreType.REGULAR,
            dma((n + 1,)), dma((n + 1, pairs)), dma((n + 1,)), dma((n + 1, groups)),
            dma(()), dma((pairs,)),
        ],
        compiler_params=pltpu.CompilerParams(
            collective_id=0, has_side_effects=True, vmem_limit_bytes=56 * 1024 * 1024
        ),
    )(
        piece_tokens, step_tokens, norm_gain.reshape(1, -1), gate_weight.T,
        gate_bias.reshape(1, -1), decay_total.reshape(1, -1), cache_decay, step_gates,
        step_lengths.reshape(1, -1), query_weight, key_weight, value_weight,
        cache_keys, cache_values,
        step_keys.reshape(steps * span, local), step_values.reshape(steps * span, local),
    )
    return pl.pallas_call(
        functools.partial(project, rows),
        out_shape=(
            jax.ShapeDtypeStruct((rows, columns), BF16),
            jax.ShapeDtypeStruct((steps, columns), BF16),
        ),
        in_specs=[vmem, vmem],
        out_specs=(vmem, vmem),
        compiler_params=pltpu.CompilerParams(vmem_limit_bytes=16 * 1024 * 1024),
    )(att, out_weight)


def solution(mesh):
    rows = P(("dp", "kv"), None)
    both = P(("dp", "kv"), "tp")
    cols = P(None, "tp")
    in_specs = (
        rows, rows, P(), cols, cols, cols, P(), P(), cols, both, both,
        P("tp", ("dp", "kv")), P("dp"),
        P(("dp", "kv"), None, "tp"), P(("dp", "kv"), None, "tp"),
        P(("dp", "kv"), "tp", None), P(("dp", "kv")),
    )
    return jax.shard_map(
        per_device, mesh=mesh, in_specs=in_specs, out_specs=(both, both), check_vma=False
    )
```
